256 devices in a mesh: sp: 32 (over z, y), tp: 8 (over x, core).
Axes of the slice: x: 4, y: 4, z: 8, core: 2. Of those that a mesh axis runs over, the one named last changes fastest.
Arguments:
- skip_stream: bfloat16 [24576, 2048], P(('sp', 'tp')), may hold values from -24 to 24
- acceptance_signal: bfloat16 [24576, 2048], P('sp', 'tp'), may hold values from -6 to 6
- lookup_mapped: bfloat16 [24576, 2048], P('sp', 'tp'), may hold values from -12 to 12
- payload_mapped: bfloat16 [24576, 2048], P('sp', 'tp'), may hold values from -6 to 6
- result_switch: bfloat16 [24576, 2048], P('sp', 'tp'), may hold values from -6 to 6
- forget_dynamic_share: bfloat16 [24576, 2048], P('sp', 'tp'), may hold values from -4 to 4
- additive_forget_logarithm: float32 [24576, 32], P('sp', 'tp'), may hold values from -1 to 0
- forget_feature_offset: float32 [2048], P('tp'), may hold values from -11 to -3
- substitution_dynamic_share: bfloat16 [24576, 2048], P('sp', 'tp'), may hold values from -6 to 6
- substitution_feature_offset: float32 [2048], P('tp'), may hold values from -6.5 to 2.5
- diagonal_reward_scales: float32 [2048], P('tp'), may hold values from -0.9 to 0.9
- result_matrix: bfloat16 [2048, 2048], P('tp'), may hold values from -0.125 to 0.125
- mlp_rescaler: float32 [2048], replicated, may hold values from 0.1 to 1.9
- switch_matrix: bfloat16 [2048, 5120], P('sp', 'tp'), may hold values from -0.125 to 0.125
- expand_matrix: bfloat16 [2048, 5120], P('sp', 'tp'), may hold values from -0.125 to 0.125
- contract_matrix: bfloat16 [2048, 5120], P('sp', 'tp'), may hold values from -0.25 to 0.25
Outputs:
- mixed_out: bfloat16 [24576, 2048], P(('sp', 'tp'))
The draws below stay inside these ranges and needn't reach their ends.
All inputs are finite; a program needn't handle non-finite values.
Results may differ from the reference program's by a relative error of at most 0.015.
Values may be sent and summed in bfloat16 or wider, within the bound.
A program may use at most 128 MiB of HBM per device.

```python
import jax
import jax.numpy as jnp
from jax import lax

EMBED_DIMENSION = 2048
PER_GROUP_DIMS = 64
FF = 5120
TOK_DEV = 768
TOKENS = 24576
N_TP = 8


def draw_skip_stream(key, part):
    entries = jnp.clip(jax.random.normal(jax.random.fold_in(key, 11), (TOKENS, EMBED_DIMENSION), jnp.float32), -4.0, 4.0)
    column_scale = jnp.exp(jnp.linspace(jnp.log(0.3), jnp.log(3.0), EMBED_DIMENSION))
    row_scale = jnp.exp(jax.random.uniform(jax.random.fold_in(key, 12), (TOKENS, 1), jnp.float32, jnp.log(0.5), jnp.log(2.0)))
    return (entries * column_scale[None, :] * row_scale).astype(jnp.bfloat16)


def draw_lookup_mapped(key, part):
    attention_groups = EMBED_DIMENSION // PER_GROUP_DIMS
    direction = jnp.clip(jax.random.normal(jax.random.fold_in(key, 51), (attention_groups, PER_GROUP_DIMS), jnp.float32), -4.0, 4.0)
    noise = jnp.clip(jax.random.normal(jax.random.fold_in(key, 52), (TOKENS, attention_groups, PER_GROUP_DIMS), jnp.float32), -4.0, 4.0)
    weight = 2.0 * jnp.ones((attention_groups, 1), jnp.float32)
    shared = weight * direction
    return (noise + shared[None, :, :]).reshape(TOKENS, EMBED_DIMENSION).astype(jnp.bfloat16)


def draw_forget_dynamic_share(key, part):
    blocks = TOKENS // TOK_DEV
    offset = jax.random.uniform(jax.random.fold_in(key, 21), (blocks, 1, 1), jnp.float32, -0.7, 0.7)
    noise = jnp.clip(jax.random.normal(jax.random.fold_in(key, 22), (blocks, TOK_DEV, EMBED_DIMENSION), jnp.float32), -3.0, 3.0)
    return (noise + offset).reshape(TOKENS, EMBED_DIMENSION).astype(jnp.bfloat16)


def draw_additive_forget_logarithm(key, part):
    spots = jax.random.randint(jax.random.fold_in(key, 31), (4,), 0, TOKENS)
    struck = jnp.any(jnp.arange(TOKENS)[:, None] == spots[None, :], axis=1)
    losses = jnp.log(jax.random.uniform(jax.random.fold_in(key, 32), (TOKENS, EMBED_DIMENSION // PER_GROUP_DIMS), jnp.float32, 0.5, 0.8))
    return jnp.where(struck[:, None], losses, 0.0).astype(jnp.float32)


def draw_forget_feature_offset(key, part):
    attention_groups = EMBED_DIMENSION // PER_GROUP_DIMS
    fast_share = 0.5
    quick_heads = jax.random.uniform(jax.random.fold_in(key, 41), (attention_groups, 1), jnp.float32) < fast_share
    quick = jax.random.uniform(jax.random.fold_in(key, 42), (attention_groups, PER_GROUP_DIMS), jnp.float32, -4.5, -3.0)
    patient = jax.random.uniform(jax.random.fold_in(key, 43), (attention_groups, PER_GROUP_DIMS), jnp.float32, -11.0, -9.0)
    return jnp.where(quick_heads, quick, patient).reshape(EMBED_DIMENSION).astype(jnp.float32)


def draw_substitution_feature_offset(key, part):
    attention_groups = EMBED_DIMENSION // PER_GROUP_DIMS
    order = jax.random.permutation(jax.random.fold_in(key, 61), attention_groups)
    levels = jnp.linspace(-6.0, 2.2, attention_groups)
    jitter = jax.random.uniform(jax.random.fold_in(key, 62), (attention_groups, PER_GROUP_DIMS), jnp.float32, -0.3, 0.3)
    return (levels[order][:, None] + jitter).reshape(EMBED_DIMENSION).astype(jnp.float32)


def steps_of(key, dims, split, least, top_value):
    gain = 1.0
    for dim, shards_of in split:
        steps = jax.random.uniform(jax.random.fold_in(jax.random.fold_in(key, 6), dim), (shards_of,), jnp.float32, least / len(split), top_value / len(split))
        gain = gain * jnp.repeat(jnp.exp(steps), dims[dim] // shards_of).reshape((-1,) + (1,) * (len(dims) - 1 - dim))
    return gain


def scatter_about(key, dims, scale, limit, cuts=(), kind=jnp.bfloat16):
    values = scale * jax.random.normal(key, dims, jnp.float32)
    if cuts:
        values = values * steps_of(key, dims, cuts, -0.22, 0.18)
    return jnp.clip(values, -limit, limit).astype(kind)


def setup_inputs(seed: int = 0) -> dict:
    seeds = jax.random.split(jax.random.key(seed), 17)
    skip_stream = draw_skip_stream(jax.random.fold_in(seeds[16], 71), 0)
    acceptance_signal = scatter_about(seeds[1], (TOKENS, EMBED_DIMENSION), 1.0, 6.0, ((0, 32), (1, 8)))
    lookup_mapped = draw_lookup_mapped(jax.random.fold_in(seeds[16], 71), 0)
    payload_mapped = scatter_about(seeds[3], (TOKENS, EMBED_DIMENSION), 1.0, 6.0, ((0, 32), (1, 8)))
    result_switch = scatter_about(seeds[4], (TOKENS, EMBED_DIMENSION), 1.0, 6.0, ((0, 32), (1, 8)))
    forget_dynamic_share = draw_forget_dynamic_share(jax.random.fold_in(seeds[16], 71), 0)
    additive_forget_logarithm = draw_additive_forget_logarithm(jax.random.fold_in(seeds[16], 71), 0)
    forget_feature_offset = draw_forget_feature_offset(jax.random.fold_in(seeds[16], 71), 0)
    substitution_dynamic_share = scatter_about(seeds[8], (TOKENS, EMBED_DIMENSION), 1.0, 6.0, ((0, 32), (1, 8)))
    substitution_feature_offset = draw_substitution_feature_offset(jax.random.fold_in(seeds[16], 71), 0)
    diagonal_reward_scales = scatter_about(seeds[10], (EMBED_DIMENSION,), 0.15, 0.9, ((0, 8),), jnp.float32)
    result_matrix = scatter_about(seeds[11], (EMBED_DIMENSION, EMBED_DIMENSION), EMBED_DIMENSION ** -0.5, 0.125, ((0, 8),))
    mlp_rescaler = jnp.clip(1.0 + 0.18 * jax.random.normal(seeds[12], (EMBED_DIMENSION,), jnp.float32), 0.1, 1.9)
    switch_matrix = scatter_about(seeds[13], (EMBED_DIMENSION, FF), EMBED_DIMENSION ** -0.5, 0.125, ((0, 32), (1, 8)))
    expand_matrix = scatter_about(seeds[14], (EMBED_DIMENSION, FF), EMBED_DIMENSION ** -0.5, 0.125, ((0, 32), (1, 8)))
    contract_matrix = scatter_about(seeds[15], (EMBED_DIMENSION, FF), (FF // 8) ** -0.5, 0.25, ((0, 32), (1, 8)))
    return dict(skip_stream=skip_stream, acceptance_signal=acceptance_signal, lookup_mapped=lookup_mapped, payload_mapped=payload_mapped, result_switch=result_switch, forget_dynamic_share=forget_dynamic_share, additive_forget_logarithm=additive_forget_logarithm, forget_feature_offset=forget_feature_offset, substitution_dynamic_share=substitution_dynamic_share, substitution_feature_offset=substitution_feature_offset, diagonal_reward_scales=diagonal_reward_scales, result_matrix=result_matrix, mlp_rescaler=mlp_rescaler, switch_matrix=switch_matrix, expand_matrix=expand_matrix, contract_matrix=contract_matrix)


norm_eps = 1e-06
group_eps = 0.00064
half_step = 0.5

def group_sum(left, right, groups):
    span = left.shape[1] // groups

    def add_group(total, index):
        first = (index * span).astype(jnp.int32)
        left_part = lax.dynamic_slice_in_dim(left, first, span, 1)
        right_part = lax.dynamic_slice_in_dim(right, first, span, 0)
        partial_prod = jnp.dot(left_part, right_part, preferred_element_type=jnp.float32)
        partial_prod = lax.optimization_barrier(partial_prod.astype(jnp.bfloat16)).astype(jnp.float32)
        return (total + partial_prod, None)
    start_total = jnp.zeros((left.shape[0], right.shape[1]), jnp.float32)
    total, _ = lax.scan(add_group, start_total, jnp.arange(groups, dtype=jnp.int32))
    return total.astype(jnp.bfloat16)

def advance(memory, inputs):
    read_now, decay_now, key_now, value_now, unit_now, rate_now = inputs
    recall = lax.optimization_barrier(jnp.sum(memory * unit_now[:, None, :], axis=-1))
    memory = memory * decay_now[:, None, :] - recall[:, :, None] * (unit_now * rate_now)[:, None, :] + value_now[:, :, None] * key_now[:, None, :]
    return (memory, lax.optimization_barrier(jnp.sum(memory * read_now[:, None, :], axis=-1)))

def reference(skip_stream, acceptance_signal, lookup_mapped, payload_mapped, result_switch, forget_dynamic_share, additive_forget_logarithm, forget_feature_offset, substitution_dynamic_share, substitution_feature_offset, diagonal_reward_scales, result_matrix, mlp_rescaler, switch_matrix, expand_matrix, contract_matrix):
    sequence_span = skip_stream.shape[0]
    attention_groups = EMBED_DIMENSION // PER_GROUP_DIMS

    def by_head(values):
        return values.astype(jnp.float32).reshape(sequence_span, attention_groups, PER_GROUP_DIMS)
    acceptance_lines = by_head(acceptance_signal)
    lookup_vectors = by_head(lookup_mapped)
    payload_vectors = by_head(payload_mapped)
    log_decay_rate = -jax.nn.softplus(-(forget_feature_offset[None, :] + forget_dynamic_share.astype(jnp.float32))) - 0.5
    decay_factor_step = jnp.exp(-jnp.exp(log_decay_rate).reshape(sequence_span, attention_groups, PER_GROUP_DIMS) + additive_forget_logarithm[:, :, None])
    replace_rate = jax.nn.sigmoid(substitution_feature_offset[None, :] + substitution_dynamic_share.astype(jnp.float32))
    replace_rate = replace_rate.reshape(sequence_span, attention_groups, PER_GROUP_DIMS)
    unit_key = lookup_vectors * lax.rsqrt(lax.optimization_barrier(jnp.sum(lookup_vectors * lookup_vectors, axis=-1, keepdims=True)) + norm_eps)
    start_memory = jnp.zeros((attention_groups, PER_GROUP_DIMS, PER_GROUP_DIMS), jnp.float32)
    _, outcome = lax.scan(advance, start_memory, (acceptance_lines, decay_factor_step, lookup_vectors, payload_vectors, unit_key, replace_rate))
    centre = lax.optimization_barrier(jnp.mean(outcome, axis=-1, keepdims=True))
    spread = lax.optimization_barrier(jnp.mean(jnp.square(outcome - centre), axis=-1, keepdims=True))
    rescaled_attention = (outcome - centre) * lax.rsqrt(spread + group_eps)
    diagonal_reward_summand = lax.optimization_barrier(jnp.sum(acceptance_lines * lookup_vectors * diagonal_reward_scales.reshape(attention_groups, PER_GROUP_DIMS), axis=-1, keepdims=True)) * payload_vectors
    merged_attention = ((rescaled_attention + diagonal_reward_summand).reshape(sequence_span, EMBED_DIMENSION) * result_switch.astype(jnp.float32)).astype(jnp.bfloat16)
    projected = group_sum(merged_attention, result_matrix, N_TP)
    stream = skip_stream.astype(jnp.float32) + projected.astype(jnp.float32)
    scale_rows = lax.rsqrt(lax.optimization_barrier(jnp.mean(stream * stream, axis=-1, keepdims=True)) + norm_eps)
    normed_rows = (stream * scale_rows * mlp_rescaler[None, :]).astype(jnp.bfloat16)
    gate_act = jnp.dot(normed_rows, switch_matrix, preferred_element_type=jnp.float32)
    up_act = jnp.dot(normed_rows, expand_matrix, preferred_element_type=jnp.float32)
    hidden = (jax.nn.silu(gate_act) * up_act).astype(jnp.bfloat16)
    ffn_out = group_sum(hidden, contract_matrix.T, N_TP)
    return (stream + half_step * ffn_out.astype(jnp.float32)).astype(jnp.bfloat16)
```

```python
import functools

import jax
import jax.numpy as jnp
from jax import lax
from jax.experimental import pallas as pl
from jax.experimental.pallas import tpu as pltpu
from jax.sharding import Mesh
from jax.sharding import PartitionSpec as P

PER_GROUP_DIMS = 64
SP = ("sp_0", "sp_1")
SP_TP = ("sp_0", "sp_1", "tp")
MESH = pl.DeviceIdType.MESH

norm_eps = 1e-06
group_eps = 0.00064
half_step = 0.5
EXP_HALF = 0.6065306597126334

C = 64
TOGETHER = 2
LEVELS = (2, 4, 8, 16, 32)
F32 = jnp.float32
BF16 = jnp.bfloat16


def dot_nn(a, b):
    return lax.dot_general(a, b, (((1,), (0,)), ((), ())), preferred_element_type=F32)


def dot_nt(a, b):
    return lax.dot_general(a, b, (((1,), (1,)), ((), ())), preferred_element_type=F32)


def dot_tn(a, b):
    return lax.dot_general(a, b, (((0,), (0,)), ((), ())), preferred_element_type=F32)


def two_parts(x):
    high = x.astype(BF16)
    return high, (x - high.astype(F32)).astype(BF16)


def mixing_kernel(
    n_z,
    n_y,
    r_ref,
    k_ref,
    v_ref,
    gate_ref,
    fd_ref,
    afl_ref,
    foff_ref,
    sd_ref,
    soff_ref,
    scale_ref,
    out_ref,
    mask_ref,
    level_ref,
    local_ref,
    coef_ref,
    extra_ref,
    sm_ref,
    packet_y,
    recv_y,
    packet_z,
    recv_z,
    s_ref,
    send_y_sem,
    recv_y_sem,
    send_z_sem,
    recv_z_sem,
):
    length, width = r_ref.shape
    heads = width // C
    place_z = lax.axis_index("sp_0")
    place_y = lax.axis_index("sp_1")

    barrier = pltpu.get_barrier_semaphore()
    for d in range(1, n_y):
        pl.semaphore_signal(
            barrier, inc=1, device_id={"sp_1": lax.rem(place_y + d, n_y)}, device_id_type=MESH
        )
    for d in range(1, n_z):
        pl.semaphore_signal(
            barrier, inc=1, device_id={"sp_0": lax.rem(place_z + d, n_z)}, device_id_type=MESH
        )

    big_row = lax.broadcasted_iota(jnp.int32, (width, width), 0)
    big_col = lax.broadcasted_iota(jnp.int32, (width, width), 1)
    same_head = (big_row // C) == (big_col // C)
    mask_ref[...] = jnp.where(same_head, 1.0, 0.0).astype(BF16)

    t_idx = lax.broadcasted_iota(jnp.int32, (C, width), 0)
    lane = lax.broadcasted_iota(jnp.int32, (C, width), 1)
    j_idx = lane % C
    strict = j_idx < t_idx
    inclusive = j_idx <= t_idx
    eye = jnp.where(j_idx == t_idx, 1.0, 0.0).astype(F32)
    for n, b in enumerate(LEVELS):
        rb = (big_row % C) // b
        cb = (big_col % C) // b
        level_ref[n] = jnp.where(
            same_head & (rb % 2 == 1) & (cb == rb - 1), 1.0, 0.0
        ).astype(BF16)
    first_level = (t_idx % 2 == 1) & (j_idx == t_idx - 1)

    tri = jnp.where(
        (lax.broadcasted_iota(jnp.int32, (C, 2 * C), 1) % C)
        <= lax.broadcasted_iota(jnp.int32, (C, 2 * C), 0),
        1.0,
        0.0,
    ).astype(BF16)

    def tiled(x):
        return jnp.concatenate([x.astype(BF16)] * heads, axis=0)

    def bd(x):
        return tiled(x) * mask_ref[...]

    def diagonal_of(full):
        out = full[0:C]
        for h in range(1, heads):
            out = jnp.where(lane >= h * C, full[h * C : (h + 1) * C], out)
        return out

    sm_ref[0:C, :] = jnp.zeros((C, width), F32)
    sm_ref[C:, :] = eye

    def chunk(c, result):
        rows = pl.ds(pl.multiple_of(c * C, C), C)
        r = r_ref[rows, :].astype(F32)
        k = k_ref[rows, :].astype(F32)
        vb = v_ref[rows, :]
        v = vb.astype(F32)
        afl = afl_ref[rows, :]
        added = jnp.broadcast_to(afl[:, 0:1], (C, width))
        for h in range(1, heads):
            added = jnp.where(lane >= h * C, afl[:, h : h + 1], added)
        log_step = added - EXP_HALF * jax.nn.sigmoid(foff_ref[...] + fd_ref[rows, :].astype(F32))
        rate = jax.nn.sigmoid(soff_ref[...] + sd_ref[rows, :].astype(F32))
        k_hi, k_lo = two_parts(k * k)
        d_hi, d_lo = two_parts(r * k * scale_ref[...])
        sums = dot_nn(jnp.concatenate([k_hi, k_lo, d_hi, d_lo], axis=0), mask_ref[...])
        l_hi, l_lo = two_parts(log_step)
        cum = dot_nn(tri, jnp.concatenate([l_hi, l_lo], axis=0))
        yield
        unit = k * lax.rsqrt(sums[0:C] + sums[C : 2 * C] + norm_eps)
        extra_ref[rows, :] = (sums[2 * C : 3 * C] + sums[3 * C :]) * v
        mid = cum[C // 2 - 1 : C // 2]
        end = cum[C - 1 : C]
        rel = cum - mid
        grow = jnp.exp(rel)
        shrink = jnp.exp(-rel)
        before_unit = jnp.exp(rel - log_step) * unit
        read_fwd = r * grow
        key_back = k * shrink
        erase_back = unit * rate * shrink
        grow_mid = jnp.exp(mid)
        grow_rest = jnp.exp(end - mid)
        grow_end = jnp.exp(end)
        left = jnp.concatenate([before_unit, read_fwd], axis=0).astype(BF16)
        by_key = dot_nt(left, bd(key_back))
        by_erase = dot_nt(left, bd(erase_back))
        yield
        key_both = jnp.concatenate(
            [jnp.where(strict, by_key[0:C], 0.0), jnp.where(inclusive, by_key[C:], 0.0)], axis=0
        ).astype(BF16)
        erase_past = jnp.where(strict, by_erase[0:C], 0.0)
        erase_read = jnp.where(inclusive, by_erase[C:], 0.0).astype(BF16)
        by_value = dot_nn(key_both, bd(vb))
        erase_tiled = tiled(erase_past)
        inv = eye - jnp.where(first_level, erase_past, 0.0)
        for n in range(len(LEVELS)):
            half = dot_nn(inv.astype(BF16), erase_tiled * level_ref[n])
            yield
            inv = inv - dot_nn(half.astype(BF16), bd(inv))
            yield
        inv_b = inv.astype(BF16)
        recalled = dot_nn(inv_b, bd(by_value[0:C]))
        carried_map = dot_nn(inv_b, bd(before_unit * grow_mid))
        yield
        recalled_b = recalled.astype(BF16)
        carried_b = carried_map.astype(BF16)
        local = by_value[C:] - dot_nn(erase_read, bd(recalled_b))
        from_start = (read_fwd * grow_mid - dot_nn(erase_read, bd(carried_b))).astype(BF16)
        key_end = (key_back * grow_rest).astype(BF16)
        erase_end = (erase_back * grow_rest).astype(BF16)
        gain = dot_tn(
            jnp.concatenate([vb, -recalled_b], axis=0),
            jnp.concatenate([key_end, erase_end], axis=0),
        )
        loss = dot_tn(carried_b, erase_end)
        yield
        result.append(
            (rows, local, from_start, diagonal_of(gain), loss.astype(BF16) * mask_ref[...], grow_end)
        )

    def group(g, _):
        results = [[] for _ in range(TOGETHER)]
        running = [chunk(g * TOGETHER + n, results[n]) for n in range(TOGETHER)]
        while running:
            left_over = []
            for one in running:
                try:
                    next(one)
                    left_over.append(one)
                except StopIteration:
                    pass
            running = left_over
        sm = sm_ref[...]
        for n in range(TOGETHER):
            rows, local, from_start, gain, loss, grow_end = results[n][0]
            sm_b = sm.astype(BF16)
            local_ref[rows, :] = local + dot_nt(from_start, bd(sm_b[0:C]))
            coef_ref[rows, :] = dot_nt(from_start, bd(sm_b[C:])).astype(BF16)
            sm = sm * grow_end - dot_nn(sm_b, loss)
            sm = jnp.concatenate([sm[0:C] + gain, sm[C:]], axis=0)
        sm_ref[...] = sm
        return 0

    lax.fori_loop(0, length // (C * TOGETHER), group, 0)

    def followed_by(sm, packet):
        prod = dot_nn(sm.astype(BF16), bd(packet[C:]))
        return jnp.concatenate([prod[0:C] + packet[0:C].astype(F32), prod[C:]], axis=0)

    own = sm_ref[...].astype(BF16)
    packet_y[...] = own
    recv_y[place_y] = own
    pl.semaphore_wait(barrier, n_y - 1 + n_z - 1)

    def copy_y(to, slot):
        return pltpu.make_async_remote_copy(
            src_ref=packet_y,
            dst_ref=recv_y.at[slot],
            send_sem=send_y_sem.at[to],
            recv_sem=recv_y_sem.at[slot],
            device_id={"sp_1": to},
            device_id_type=MESH,
        )

    for d in range(1, n_y):
        copy_y(lax.rem(place_y + d, n_y), place_y).start()
    for d in range(1, n_y):
        peer = lax.rem(place_y + n_y - d, n_y)
        copy_y(peer, peer).wait_recv()
    total = recv_y[0].astype(F32)
    inside = jnp.concatenate([jnp.zeros((C, width), F32), eye], axis=0)
    for m in range(1, n_y):
        inside = jnp.where(place_y == m, total, inside)
        total = followed_by(total, recv_y[m])
    packet_z[...] = total.astype(BF16)

    def copy_z(to, slot):
        return pltpu.make_async_remote_copy(
            src_ref=packet_z,
            dst_ref=recv_z.at[slot],
            send_sem=send_z_sem.at[to],
            recv_sem=recv_z_sem.at[slot],
            device_id={"sp_0": to},
            device_id_type=MESH,
        )

    for d in range(1, n_z):

        @pl.when(place_z + d < n_z)
        def _():
            copy_z(place_z + d, place_z).start()

    s_ref[...] = jnp.zeros((C, width), F32)
    for m in range(n_z - 1):

        @pl.when(m < place_z)
        def _():
            copy_z(m, m).wait_recv()
            arrived = recv_z[m]
            s_ref[...] = (
                dot_nn(s_ref[...].astype(BF16), bd(arrived[C:])) + arrived[0:C].astype(F32)
            )

    incoming = dot_nn(s_ref[...].astype(BF16), bd(inside[C:])) + inside[0:C]
    incoming_bd = bd(incoming)

    span = 4 * C
    for start in range(0, length, span):
        rows = pl.ds(start, span)
        outcome = local_ref[rows, :] + dot_nt(coef_ref[rows, :], incoming_bd)
        o_hi, o_lo = two_parts(outcome)
        centre = dot_nn(jnp.concatenate([o_hi, o_lo], axis=0), mask_ref[...])
        away = outcome - (centre[0:span] + centre[span:]) * (1.0 / C)
        a_hi, a_lo = two_parts(away * away)
        spread = dot_nn(jnp.concatenate([a_hi, a_lo], axis=0), mask_ref[...])
        spread = (spread[0:span] + spread[span:]) * (1.0 / C)
        normed = away * lax.rsqrt(spread + group_eps)
        out_ref[rows, :] = ((normed + extra_ref[rows, :]) * gate_ref[rows, :].astype(F32)).astype(
            BF16
        )

    for d in range(1, n_y):
        to = lax.rem(place_y + d, n_y)
        copy_y(to, to).wait_send()
    for d in range(1, n_z):

        @pl.when(place_z + d < n_z)
        def _():
            copy_z(place_z + d, place_z).wait_send()


def mixed_heads_of(r, k, v, gate, fd, afl, foff, sd, soff, scale):
    n_z, n_y = lax.axis_size("sp_0"), lax.axis_size("sp_1")
    length, width = r.shape
    vmem = pl.BlockSpec(memory_space=pltpu.VMEM)
    return pl.pallas_call(
        functools.partial(mixing_kernel, n_z, n_y),
        out_shape=jax.ShapeDtypeStruct((length, width), BF16),
        in_specs=[vmem] * 10,
        out_specs=vmem,
        scratch_shapes=[
            pltpu.VMEM((width, width), BF16),
            pltpu.VMEM((len(LEVELS), width, width), BF16),
            pltpu.VMEM((length, width), F32),
            pltpu.VMEM((length, width), BF16),
            pltpu.VMEM((length, width), F32),
            pltpu.VMEM((2 * C, width), F32),
            pltpu.VMEM((2 * C, width), BF16),
            pltpu.VMEM((n_y, 2 * C, width), BF16),
            pltpu.VMEM((2 * C, width), BF16),
            pltpu.VMEM((n_z, 2 * C, width), BF16),
            pltpu.VMEM((C, width), F32),
            pltpu.SemaphoreType.DMA((n_y,)),
            pltpu.SemaphoreType.DMA((n_y,)),
            pltpu.SemaphoreType.DMA((n_z,)),
            pltpu.SemaphoreType.DMA((n_z,)),
        ],
        compiler_params=pltpu.CompilerParams(
            collective_id=0, has_side_effects=True, vmem_limit_bytes=40 * 1024 * 1024
        ),
        cost_estimate=pl.CostEstimate(
            flops=40_000_000_000, bytes_accessed=3_000_000, transcendentals=0
        ),
        name="mixing",
    )(r, k, v, gate, fd, afl, foff[None, :], sd, soff[None, :], scale[None, :])


def sent_and_summed(shard, axis, dim):
    peers = lax.axis_size(axis)
    parts = lax.all_to_all(
        shard.reshape(peers, shard.shape[0] // peers, shard.shape[1]), axis, 0, 0, tiled=True
    )
    return jnp.sum(parts.astype(jnp.float32), axis=0)


def per_device(
    skip_stream,
    acceptance_signal,
    lookup_mapped,
    payload_mapped,
    result_switch,
    forget_dynamic_share,
    additive_forget_logarithm,
    forget_feature_offset,
    substitution_dynamic_share,
    substitution_feature_offset,
    diagonal_reward_scales,
    result_matrix,
    mlp_rescaler,
    switch_matrix,
    expand_matrix,
    contract_matrix,
):
    weights = jnp.concatenate([switch_matrix, expand_matrix, contract_matrix], axis=1)
    whole = lax.all_gather(weights, SP, axis=0, tiled=True)
    ff = switch_matrix.shape[1]
    gate_whole, up_whole, down_whole = whole[:, :ff], whole[:, ff : 2 * ff], whole[:, 2 * ff :]

    merged_attention = mixed_heads_of(
        acceptance_signal,
        lookup_mapped,
        payload_mapped,
        result_switch,
        forget_dynamic_share,
        additive_forget_logarithm,
        forget_feature_offset,
        substitution_dynamic_share,
        substitution_feature_offset,
        diagonal_reward_scales,
    )
    projected = sent_and_summed(
        jnp.dot(merged_attention, result_matrix, preferred_element_type=jnp.float32).astype(
            jnp.bfloat16
        ),
        "tp",
        0,
    ).astype(jnp.bfloat16)
    stream = skip_stream.astype(jnp.float32) + lax.optimization_barrier(projected).astype(
        jnp.float32
    )
    scale_rows = lax.rsqrt(jnp.mean(stream * stream, axis=-1, keepdims=True) + norm_eps)
    normed_rows = (stream * scale_rows * mlp_rescaler[None, :]).astype(jnp.bfloat16)
    whole_rows = lax.all_gather(normed_rows, "tp", axis=0, tiled=True)
    gate_act = jnp.dot(whole_rows, gate_whole, preferred_element_type=jnp.float32)
    up_act = jnp.dot(whole_rows, up_whole, preferred_element_type=jnp.float32)
    hidden = (jax.nn.silu(gate_act) * up_act).astype(jnp.bfloat16)
    ffn_out = lax.psum_scatter(
        lax.dot_general(
            hidden, down_whole, (((1,), (1,)), ((), ())), preferred_element_type=jnp.float32
        ).astype(jnp.bfloat16),
        "tp",
        scatter_dimension=0,
        tiled=True,
    )
    return (stream + half_step * lax.optimization_barrier(ffn_out).astype(jnp.float32)).astype(
        jnp.bfloat16
    )


def solution(mesh):
    torus = Mesh(mesh.devices.reshape(8, 4, mesh.shape["tp"]), ("sp_0", "sp_1", "tp"))
    in_specs = (
        P(SP_TP, None),
        P(SP, "tp"),
        P(SP, "tp"),
        P(SP, "tp"),
        P(SP, "tp"),
        P(SP, "tp"),
        P(SP, "tp"),
        P("tp"),
        P(SP, "tp"),
        P("tp"),
        P("tp"),
        P("tp", None),
        P(),
        P(SP, "tp"),
        P(SP, "tp"),
        P(SP, "tp"),
    )
    out_specs = P(SP_TP, None)
    return jax.shard_map(
        per_device, mesh=torus, in_specs=in_specs, out_specs=out_specs, check_vma=False
    )
```

```python
import functools

import jax
import jax.numpy as jnp
from jax import lax
from jax.experimental import pallas as pl
from jax.experimental.pallas import tpu as pltpu
from jax.sharding import Mesh
from jax.sharding import PartitionSpec as P

PER_GROUP_DIMS = 64
SP = ("sp_0", "sp_1")
SP_TP = ("sp_0", "sp_1", "tp")
MESH = pl.DeviceIdType.MESH

norm_eps = 1e-06
group_eps = 0.00064
half_step = 0.5
EXP_HALF = 0.6065306597126334

C = 64
TOGETHER = 2
LEVELS = (2, 4, 8, 16, 32)
F32 = jnp.float32
BF16 = jnp.bfloat16


def dot_nn(a, b):
    return lax.dot_general(a, b, (((1,), (0,)), ((), ())), preferred_element_type=F32)


def dot_nt(a, b):
    return lax.dot_general(a, b, (((1,), (1,)), ((), ())), preferred_element_type=F32)


def dot_tn(a, b):
    return lax.dot_general(a, b, (((0,), (0,)), ((), ())), preferred_element_type=F32)


def two_parts(x):
    high = x.astype(BF16)
    return high, (x - high.astype(F32)).astype(BF16)


ROWS = 96
HALF = 1024


def ring_places():
    tp = lax.axis_index("tp")
    chip, core = tp // 2, tp % 2
    right = lax.rem(chip + 1, 4) * 2 + core
    left = lax.rem(chip + 3, 4) * 2 + core
    sibling = chip * 2 + 1 - core
    return chip, core, right, left, sibling


def remote(src, dst, send_sem, recv_sem, to):
    return pltpu.make_async_remote_copy(
        src_ref=src,
        dst_ref=dst,
        send_sem=send_sem,
        recv_sem=recv_sem,
        device_id={"tp": to},
        device_id_type=MESH,
    )


class RingSum:
    def __init__(self, part, sib, pair, relay, arrived, sems):
        self.part, self.sib, self.pair, self.relay, self.arrived = part, sib, pair, relay, arrived
        self.sib_send, self.sib_recv, self.send, self.recv = sems
        self.chip, self.core, self.right, self.left, self.sibling = ring_places()
        self.own = pl.ds(pl.multiple_of(self.core * ROWS, ROWS), ROWS)
        self.other = pl.ds(pl.multiple_of((1 - self.core) * ROWS, ROWS), ROWS)

    def to_sibling(self, d):
        return remote(
            self.part.at[d, :, self.other, :],
            self.sib.at[d],
            self.sib_send.at[d],
            self.sib_recv.at[d],
            self.sibling,
        )

    def hop(self, n):
        src, dst, to = (
            (self.pair.at[2, 0], self.relay.at[0], self.right),
            (self.pair.at[2, 1], self.relay.at[1], self.left),
            (self.pair.at[1, 1], self.arrived.at[0, 1], self.right),
            (self.pair.at[3, 0], self.arrived.at[1, 0], self.left),
            (self.pair.at[1, 0], self.arrived.at[0, 0], self.right),
            (self.pair.at[3, 1], self.arrived.at[1, 1], self.left),
        )[n]
        return remote(src, dst, self.send.at[n], self.recv.at[n], to)

    def produced(self, d):
        self.to_sibling(d).start()

    def summed(self, d, h):
        return self.part[d, h, self.own, :].astype(F32) + self.sib[d, h].astype(F32)

    def pass_on(self, d):
        self.to_sibling(d).wait_recv()
        if d == 2:
            self.pair[2, 0] = self.summed(2, 0).astype(BF16)
            self.hop(0).start()
            self.pair[2, 1] = self.summed(2, 1).astype(BF16)
            self.hop(1).start()
        if d == 1:
            self.pair[1, 1] = self.summed(1, 1).astype(BF16)
            self.hop(2).start()
        if d == 3:
            self.pair[3, 0] = self.summed(3, 0).astype(BF16)
            self.hop(3).start()

    def pass_relayed(self):
        self.hop(0).wait_recv()
        self.pair[1, 0] = (self.summed(1, 0) + self.relay[0].astype(F32)).astype(BF16)
        self.hop(4).start()
        self.hop(1).wait_recv()
        self.pair[3, 1] = (self.summed(3, 1) + self.relay[1].astype(F32)).astype(BF16)
        self.hop(5).start()

    def arrive(self):
        for n in (2, 3, 4, 5):
            self.hop(n).wait_recv()

    def result(self, h):
        return (
            self.summed(0, h)
            + self.arrived[0, h].astype(F32)
            + self.arrived[1, h].astype(F32)
        )

    def drain(self):
        for d in range(4):
            self.to_sibling(d).wait_send()
        for n in range(6):
            self.hop(n).wait_send()


RING_SUM_SCRATCH = [
    pltpu.VMEM((4, 2, 2 * ROWS, HALF), BF16),
    pltpu.VMEM((4, 2, ROWS, HALF), BF16),
    pltpu.VMEM((4, 2, ROWS, HALF), BF16),
    pltpu.VMEM((2, ROWS, HALF), BF16),
    pltpu.VMEM((2, 2, ROWS, HALF), BF16),
    pltpu.SemaphoreType.DMA((4,)),
    pltpu.SemaphoreType.DMA((4,)),
    pltpu.SemaphoreType.DMA((6,)),
    pltpu.SemaphoreType.DMA((6,)),
]


def greet_ring(barrier):
    _, _, right, left, sibling = ring_places()
    for to in (right, left, sibling):
        pl.semaphore_signal(barrier, inc=1, device_id={"tp": to}, device_id_type=MESH)


def feed_forward_kernel(
    rows_in_ref,
    stream_ref,
    gate_up_hbm,
    down_hbm,
    out_ref,
    gate_up_ref,
    down_ref,
    rows_ref,
    hidden_ref,
    part_ref,
    sib_ref,
    pair_ref,
    relay_ref,
    arrived_ref,
    sib_send,
    sib_recv,
    hop_send,
    hop_recv,
    load_sem,
    row_send,
    row_recv,
    side_send,
    side_recv,
):
    barrier = pltpu.get_barrier_semaphore()
    greet_ring(barrier)
    chip, core, right, left, sibling = ring_places()
    load_gate_up = pltpu.make_async_copy(gate_up_hbm, gate_up_ref, load_sem.at[0])
    load_down = pltpu.make_async_copy(down_hbm, down_ref, load_sem.at[1])
    load_gate_up.start()
    load_down.start()
    here = pl.ds(pl.multiple_of(core * ROWS, ROWS), ROWS)
    there = pl.ds(pl.multiple_of((1 - core) * ROWS, ROWS), ROWS)

    def chip_at(d):
        return lax.rem(chip + d, 4)

    rows_ref[chip, :, here, :] = rows_in_ref[...]
    pl.semaphore_wait(barrier, 3)

    def hop(n):
        d, h, to = (
            (0, 0, right),
            (0, 1, left),
            (0, 1, right),
            (0, 0, left),
            (3, 0, right),
            (1, 1, left),
        )[n]
        block = rows_ref.at[chip_at(d), h, here, :]
        return remote(block, block, row_send.at[n], row_recv.at[n], to)

    def arrival(n):
        d, h = ((3, 0), (1, 1), (3, 1), (1, 0), (2, 0), (2, 1))[n]
        block = rows_ref.at[chip_at(d), h, here, :]
        return remote(block, block, row_send.at[n], row_recv.at[n], sibling)

    def side(n):
        d, h = ((0, 0), (0, 1), (1, 0), (1, 1), (3, 0), (3, 1), (2, 0), (2, 1))[n]
        block = rows_ref.at[chip_at(d), h, here, :]
        return remote(block, block, side_send.at[n], side_recv.at[n], sibling)

    def side_arrival(n):
        d, h = ((0, 0), (0, 1), (1, 0), (1, 1), (3, 0), (3, 1), (2, 0), (2, 1))[n]
        block = rows_ref.at[chip_at(d), h, there, :]
        return remote(block, block, side_send.at[n], side_recv.at[n], sibling)

    for n in range(4):
        hop(n).start()
    side(0).start()
    side(1).start()

    ring = RingSum(
        part_ref,
        sib_ref,
        pair_ref,
        relay_ref,
        arrived_ref,
        (sib_send, sib_recv, hop_send, hop_recv),
    )
    ff_half = hidden_ref.shape[1]

    def produce(d):
        block = chip_at(d)
        x = [rows_ref[block, 0], rows_ref[block, 1]]
        for n in range(ff_half // 128):
            cols = pl.ds(256 * n, 256)
            both = dot_nn(x[0], gate_up_ref[0:HALF, cols]) + dot_nn(x[1], gate_up_ref[HALF:, cols])
            gate_act, up_act = both[:, :128], both[:, 128:]
            hidden_ref[:, pl.ds(128 * n, 128)] = (
                gate_act * jax.nn.sigmoid(gate_act) * up_act
            ).astype(BF16)
        hidden = hidden_ref[...]
        for h in range(2):
            for n in range(HALF // 256):
                part_ref[d, h, :, pl.ds(256 * n, 256)] = dot_nt(
                    hidden, down_ref[pl.ds(h * HALF + 256 * n, 256), :]
                ).astype(BF16)
        ring.produced(d)

    side_arrival(0).wait_recv()
    side_arrival(1).wait_recv()
    load_gate_up.wait()
    load_down.wait()
    produce(0)
    arrival(0).wait_recv()
    hop(4).start()
    side(4).start()
    arrival(1).wait_recv()
    hop(5).start()
    side(3).start()
    arrival(2).wait_recv()
    side(5).start()
    arrival(3).wait_recv()
    side(2).start()
    side_arrival(4).wait_recv()
    side_arrival(5).wait_recv()
    produce(3)
    side_arrival(2).wait_recv()
    side_arrival(3).wait_recv()
    arrival(4).wait_recv()
    side(6).start()
    arrival(5).wait_recv()
    side(7).start()
    ring.pass_on(3)
    produce(1)
    ring.pass_on(1)
    side_arrival(6).wait_recv()
    side_arrival(7).wait_recv()
    produce(2)
    ring.pass_on(2)
    ring.pass_relayed()
    ring.to_sibling(0).wait_recv()
    ring.arrive()
    for h in range(2):
        out_ref[:, pl.ds(h * HALF, HALF)] = (
            stream_ref[:, pl.ds(h * HALF, HALF)] + half_step * ring.result(h)
        ).astype(BF16)
    ring.drain()
    for n in range(6):
        hop(n).wait_send()
    for n in range(8):
        side(n).wait_send()


def feed_forward(rows, stream, gate_up, down):
    vmem = pl.BlockSpec(memory_space=pltpu.VMEM)
    hbm = pl.BlockSpec(memory_space=pl.ANY)
    ff = down.shape[1]
    return pl.pallas_call(
        feed_forward_kernel,
        out_shape=jax.ShapeDtypeStruct((ROWS, 2 * HALF), BF16),
        in_specs=[vmem, vmem, hbm, hbm],
        out_specs=vmem,
        scratch_shapes=[
            pltpu.VMEM(gate_up.shape, BF16),
            pltpu.VMEM(down.shape, BF16),
            pltpu.VMEM((4, 2, 2 * ROWS, HALF), BF16),
            pltpu.VMEM((2 * ROWS, ff), BF16),
        ]
        + RING_SUM_SCRATCH
        + [
            pltpu.SemaphoreType.DMA((2,)),
            pltpu.SemaphoreType.DMA((6,)),
            pltpu.SemaphoreType.DMA((6,)),
            pltpu.SemaphoreType.DMA((8,)),
            pltpu.SemaphoreType.DMA((8,)),
        ],
        compiler_params=pltpu.CompilerParams(
            collective_id=1, has_side_effects=True, vmem_limit_bytes=56 * 1024 * 1024
        ),
        cost_estimate=pl.CostEstimate(
            flops=20_000_000_000, bytes_accessed=8_000_000, transcendentals=0
        ),
        name="feed_forward",
    )(rows, stream, gate_up, down)


def mixing_kernel(
    n_z,
    n_y,
    r_hbm,
    k_hbm,
    v_hbm,
    gate_hbm,
    fd_hbm,
    afl_ref,
    foff_ref,
    sd_hbm,
    soff_ref,
    scale_ref,
    skip_ref,
    matrix_hbm,
    gain_ref,
    rows_out_ref,
    stream_ref,
    r_ref,
    k_ref,
    v_ref,
    gate_ref,
    fd_ref,
    sd_ref,
    matrix_ref,
    load_sem,
    mask_ref,
    level_ref,
    local_ref,
    coef_ref,
    extra_ref,
    sm_ref,
    packet_y,
    recv_y,
    packet_z,
    recv_z,
    s_ref,
    send_y_sem,
    recv_y_sem,
    send_z_sem,
    recv_z_sem,
    *ring_refs,
):
    length, width = r_ref.shape
    heads = width // C
    place_z = lax.axis_index("sp_0")
    place_y = lax.axis_index("sp_1")

    loads = [
        pltpu.make_async_copy(src, dst, load_sem.at[n])
        for n, (src, dst) in enumerate(
            (
                (r_hbm, r_ref),
                (k_hbm, k_ref),
                (v_hbm, v_ref),
                (fd_hbm, fd_ref),
                (sd_hbm, sd_ref),
                (gate_hbm, gate_ref),
                (matrix_hbm, matrix_ref),
            )
        )
    ]
    for load in loads:
        load.start()
    barrier = pltpu.get_barrier_semaphore()
    greet_ring(barrier)
    for d in range(1, n_y):
        pl.semaphore_signal(
            barrier, inc=1, device_id={"sp_1": lax.rem(place_y + d, n_y)}, device_id_type=MESH
        )
    for d in range(1, n_z):
        pl.semaphore_signal(
            barrier, inc=1, device_id={"sp_0": lax.rem(place_z + d, n_z)}, device_id_type=MESH
        )

    big_row = lax.broadcasted_iota(jnp.int32, (width, width), 0)
    big_col = lax.broadcasted_iota(jnp.int32, (width, width), 1)
    same_head = (big_row // C) == (big_col // C)
    mask_ref[...] = jnp.where(same_head, 1.0, 0.0).astype(BF16)

    t_idx = lax.broadcasted_iota(jnp.int32, (C, width), 0)
    lane = lax.broadcasted_iota(jnp.int32, (C, width), 1)
    j_idx = lane % C
    strict = j_idx < t_idx
    inclusive = j_idx <= t_idx
    eye = jnp.where(j_idx == t_idx, 1.0, 0.0).astype(F32)
    for n, b in enumerate(LEVELS):
        rb = (big_row % C) // b
        cb = (big_col % C) // b
        level_ref[n] = jnp.where(
            same_head & (rb % 2 == 1) & (cb == rb - 1), 1.0, 0.0
        ).astype(BF16)
    first_level = (t_idx % 2 == 1) & (j_idx == t_idx - 1)

    tri = jnp.where(
        (lax.broadcasted_iota(jnp.int32, (C, 2 * C), 1) % C)
        <= lax.broadcasted_iota(jnp.int32, (C, 2 * C), 0),
        1.0,
        0.0,
    ).astype(BF16)

    def tiled(x):
        return jnp.concatenate([x.astype(BF16)] * heads, axis=0)

    def bd(x):
        return tiled(x) * mask_ref[...]

    def diagonal_of(full):
        out = full[0:C]
        for h in range(1, heads):
            out = jnp.where(lane >= h * C, full[h * C : (h + 1) * C], out)
        return out

    sm_ref[0:C, :] = jnp.zeros((C, width), F32)
    sm_ref[C:, :] = eye

    def chunk(c, result):
        rows = pl.ds(pl.multiple_of(c * C, C), C)
        r = r_ref[rows, :].astype(F32)
        k = k_ref[rows, :].astype(F32)
        vb = v_ref[rows, :]
        v = vb.astype(F32)
        afl = afl_ref[rows, :]
        added = jnp.broadcast_to(afl[:, 0:1], (C, width))
        for h in range(1, heads):
            added = jnp.where(lane >= h * C, afl[:, h : h + 1], added)
        log_step = added - EXP_HALF * jax.nn.sigmoid(foff_ref[...] + fd_ref[rows, :].astype(F32))
        rate = jax.nn.sigmoid(soff_ref[...] + sd_ref[rows, :].astype(F32))
        k_hi, k_lo = two_parts(k * k)
        d_hi, d_lo = two_parts(r * k * scale_ref[...])
        sums = dot_nn(jnp.concatenate([k_hi, k_lo, d_hi, d_lo], axis=0), mask_ref[...])
        l_hi, l_lo = two_parts(log_step)
        cum = dot_nn(tri, jnp.concatenate([l_hi, l_lo], axis=0))
        yield
        unit = k * lax.rsqrt(sums[0:C] + sums[C : 2 * C] + norm_eps)
        extra_ref[rows, :] = (sums[2 * C : 3 * C] + sums[3 * C :]) * v
        mid = cum[C // 2 - 1 : C // 2]
        end = cum[C - 1 : C]
        rel = cum - mid
        grow = jnp.exp(rel)
        shrink = jnp.exp(-rel)
        before_unit = jnp.exp(rel - log_step) * unit
        read_fwd = r * grow
        key_back = k * shrink
        erase_back = unit * rate * shrink
        grow_mid = jnp.exp(mid)
        grow_rest = jnp.exp(end - mid)
        grow_end = jnp.exp(end)
        left = jnp.concatenate([before_unit, read_fwd], axis=0).astype(BF16)
        by_key = dot_nt(left, bd(key_back))
        by_erase = dot_nt(left, bd(erase_back))
        yield
        key_both = jnp.concatenate(
            [jnp.where(strict, by_key[0:C], 0.0), jnp.where(inclusive, by_key[C:], 0.0)], axis=0
        ).astype(BF16)
        erase_past = jnp.where(strict, by_erase[0:C], 0.0)
        erase_read = jnp.where(inclusive, by_erase[C:], 0.0).astype(BF16)
        by_value = dot_nn(key_both, bd(vb))
        erase_tiled = tiled(erase_past)
        inv = eye - jnp.where(first_level, erase_past, 0.0)
        for n in range(len(LEVELS)):
            half = dot_nn(inv.astype(BF16), erase_tiled * level_ref[n])
            yield
            inv = inv - dot_nn(half.astype(BF16), bd(inv))
            yield
        inv_b = inv.astype(BF16)
        recalled = dot_nn(inv_b, bd(by_value[0:C]))
        carried_map = dot_nn(inv_b, bd(before_unit * grow_mid))
        yield
        recalled_b = recalled.astype(BF16)
        carried_b = carried_map.astype(BF16)
        local = by_value[C:] - dot_nn(erase_read, bd(recalled_b))
        from_start = (read_fwd * grow_mid - dot_nn(erase_read, bd(carried_b))).astype(BF16)
        key_end = (key_back * grow_rest).astype(BF16)
        erase_end = (erase_back * grow_rest).astype(BF16)
        gain = dot_tn(
            jnp.concatenate([vb, -recalled_b], axis=0),
            jnp.concatenate([key_end, erase_end], axis=0),
        )
        loss = dot_tn(carried_b, erase_end)
        yield
        result.append(
            (rows, local, from_start, diagonal_of(gain), loss.astype(BF16) * mask_ref[...], grow_end)
        )

    def group(g, _):
        results = [[] for _ in range(TOGETHER)]
        running = [chunk(g * TOGETHER + n, results[n]) for n in range(TOGETHER)]
        while running:
            left_over = []
            for one in running:
                try:
                    next(one)
                    left_over.append(one)
                except StopIteration:
                    pass
            running = left_over
        sm = sm_ref[...]
        for n in range(TOGETHER):
            rows, local, from_start, gain, loss, grow_end = results[n][0]
            sm_b = sm.astype(BF16)
            local_ref[rows, :] = local + dot_nt(from_start, bd(sm_b[0:C]))
            coef_ref[rows, :] = dot_nt(from_start, bd(sm_b[C:])).astype(BF16)
            sm = sm * grow_end - dot_nn(sm_b, loss)
            sm = jnp.concatenate([sm[0:C] + gain, sm[C:]], axis=0)
        sm_ref[...] = sm
        return 0

    for load in loads[:5]:
        load.wait()
    lax.fori_loop(0, length // (C * TOGETHER), group, 0)

    def followed_by(sm, packet):
        prod = dot_nn(sm.astype(BF16), bd(packet[C:]))
        return jnp.concatenate([prod[0:C] + packet[0:C].astype(F32), prod[C:]], axis=0)

    own = sm_ref[...].astype(BF16)
    packet_y[...] = own
    recv_y[place_y] = own
    pl.semaphore_wait(barrier, n_y - 1 + n_z - 1 + 3)

    def copy_y(to, slot):
        return pltpu.make_async_remote_copy(
            src_ref=packet_y,
            dst_ref=recv_y.at[slot],
            send_sem=send_y_sem.at[to],
            recv_sem=recv_y_sem.at[slot],
            device_id={"sp_1": to},
            device_id_type=MESH,
        )

    for d in range(1, n_y):
        copy_y(lax.rem(place_y + d, n_y), place_y).start()
    for d in range(1, n_y):
        peer = lax.rem(place_y + n_y - d, n_y)
        copy_y(peer, peer).wait_recv()
    total = recv_y[0].astype(F32)
    inside = jnp.concatenate([jnp.zeros((C, width), F32), eye], axis=0)
    for m in range(1, n_y):
        inside = jnp.where(place_y == m, total, inside)
        total = followed_by(total, recv_y[m])
    packet_z[...] = total.astype(BF16)

    def copy_z(to, slot):
        return pltpu.make_async_remote_copy(
            src_ref=packet_z,
            dst_ref=recv_z.at[slot],
            send_sem=send_z_sem.at[to],
            recv_sem=recv_z_sem.at[slot],
            device_id={"sp_0": to},
            device_id_type=MESH,
        )

    for d in range(1, n_z):

        @pl.when(place_z + d < n_z)
        def _():
            copy_z(place_z + d, place_z).start()

    s_ref[...] = jnp.zeros((C, width), F32)
    for m in range(n_z - 1):

        @pl.when(m < place_z)
        def _():
            copy_z(m, m).wait_recv()
            arrived = recv_z[m]
            s_ref[...] = (
                dot_nn(s_ref[...].astype(BF16), bd(arrived[C:])) + arrived[0:C].astype(F32)
            )

    incoming = dot_nn(s_ref[...].astype(BF16), bd(inside[C:])) + inside[0:C]
    incoming_bd = bd(incoming)
    loads[5].wait()
    loads[6].wait()

    span = 2 * ROWS
    ring = RingSum(*ring_refs[:5], ring_refs[5:])

    def produce(d):
        start = lax.rem(ring.chip + d, 4) * span
        rows = pl.ds(pl.multiple_of(start, span), span)
        outcome = local_ref[rows, :] + dot_nt(coef_ref[rows, :], incoming_bd)
        o_hi, o_lo = two_parts(outcome)
        centre = dot_nn(jnp.concatenate([o_hi, o_lo], axis=0), mask_ref[...])
        away = outcome - (centre[0:span] + centre[span:]) * (1.0 / C)
        a_hi, a_lo = two_parts(away * away)
        spread = dot_nn(jnp.concatenate([a_hi, a_lo], axis=0), mask_ref[...])
        spread = (spread[0:span] + spread[span:]) * (1.0 / C)
        normed = away * lax.rsqrt(spread + group_eps)
        mixed = ((normed + extra_ref[rows, :]) * gate_ref[rows, :].astype(F32)).astype(BF16)
        for h in range(2):
            for n in range(HALF // 256):
                ring.part[d, h, :, pl.ds(256 * n, 256)] = dot_nn(
                    mixed, matrix_ref[:, pl.ds(h * HALF + 256 * n, 256)]
                ).astype(BF16)
        ring.produced(d)

    produce(2)
    produce(1)
    ring.pass_on(2)
    produce(3)
    ring.pass_on(1)
    produce(0)
    ring.pass_on(3)
    ring.pass_relayed()
    ring.to_sibling(0).wait_recv()
    ring.arrive()
    squares = jnp.zeros((ROWS, 1), F32)
    for h in range(2):
        cols = pl.ds(h * HALF, HALF)
        stream = skip_ref[:, cols].astype(F32) + ring.result(h)
        stream_ref[:, cols] = stream
        squares = squares + jnp.sum(stream * stream, axis=1, keepdims=True)
    scale_rows = lax.rsqrt(squares * (1.0 / (2 * HALF)) + norm_eps)
    for h in range(2):
        cols = pl.ds(h * HALF, HALF)
        rows_out_ref[h] = (stream_ref[:, cols] * scale_rows * gain_ref[:, cols]).astype(BF16)
    ring.drain()


    for d in range(1, n_y):
        to = lax.rem(place_y + d, n_y)
        copy_y(to, to).wait_send()
    for d in range(1, n_z):

        @pl.when(place_z + d < n_z)
        def _():
            copy_z(place_z + d, place_z).wait_send()


def mixed_rows_of(r, k, v, gate, fd, afl, foff, sd, soff, scale, skip, matrix, gain):
    n_z, n_y = lax.axis_size("sp_0"), lax.axis_size("sp_1")
    length, width = r.shape
    vmem = pl.BlockSpec(memory_space=pltpu.VMEM)
    hbm = pl.BlockSpec(memory_space=pl.ANY)
    return pl.pallas_call(
        functools.partial(mixing_kernel, n_z, n_y),
        out_shape=(
            jax.ShapeDtypeStruct((2, ROWS, HALF), BF16),
            jax.ShapeDtypeStruct((ROWS, 2 * HALF), F32),
        ),
        in_specs=[hbm] * 5 + [vmem, vmem, hbm, vmem, vmem, vmem, hbm, vmem],
        out_specs=(vmem, vmem),
        scratch_shapes=[pltpu.VMEM((length, width), BF16)] * 6
        + [
            pltpu.VMEM((width, 2 * HALF), BF16),
            pltpu.SemaphoreType.DMA((7,)),
            pltpu.VMEM((width, width), BF16),
            pltpu.VMEM((len(LEVELS), width, width), BF16),
            pltpu.VMEM((length, width), F32),
            pltpu.VMEM((length, width), BF16),
            pltpu.VMEM((length, width), F32),
            pltpu.VMEM((2 * C, width), F32),
            pltpu.VMEM((2 * C, width), BF16),
            pltpu.VMEM((n_y, 2 * C, width), BF16),
            pltpu.VMEM((2 * C, width), BF16),
            pltpu.VMEM((n_z, 2 * C, width), BF16),
            pltpu.VMEM((C, width), F32),
            pltpu.SemaphoreType.DMA((n_y,)),
            pltpu.SemaphoreType.DMA((n_y,)),
            pltpu.SemaphoreType.DMA((n_z,)),
            pltpu.SemaphoreType.DMA((n_z,)),
        ]
        + RING_SUM_SCRATCH,
        compiler_params=pltpu.CompilerParams(
            collective_id=0, has_side_effects=True, vmem_limit_bytes=56 * 1024 * 1024
        ),
        cost_estimate=pl.CostEstimate(
            flops=40_000_000_000, bytes_accessed=3_000_000, transcendentals=0
        ),
        name="mixing",
    )(
        r, k, v, gate, fd, afl, foff[None, :], sd, soff[None, :], scale[None, :], skip, matrix,
        gain[None, :],
    )


def per_device(
    skip_stream,
    acceptance_signal,
    lookup_mapped,
    payload_mapped,
    result_switch,
    forget_dynamic_share,
    additive_forget_logarithm,
    forget_feature_offset,
    substitution_dynamic_share,
    substitution_feature_offset,
    diagonal_reward_scales,
    result_matrix,
    mlp_rescaler,
    switch_matrix,
    expand_matrix,
    contract_matrix,
):
    depth, ff = switch_matrix.shape
    paired = jnp.stack(
        [switch_matrix.reshape(depth, -1, 128), expand_matrix.reshape(depth, -1, 128)], axis=2
    ).reshape(depth, 2 * ff)
    with jax.named_scope("weights"):
        gate_up = lax.all_gather(paired, SP, axis=0, tiled=True)
        down = lax.all_gather(contract_matrix, SP, axis=0, tiled=True)
    rows, stream = mixed_rows_of(
        acceptance_signal,
        lookup_mapped,
        payload_mapped,
        result_switch,
        forget_dynamic_share,
        additive_forget_logarithm,
        forget_feature_offset,
        substitution_dynamic_share,
        substitution_feature_offset,
        diagonal_reward_scales,
        skip_stream,
        result_matrix,
        mlp_rescaler,
    )
    return feed_forward(rows, stream, gate_up, down)


def solution(mesh):
    torus = Mesh(mesh.devices.reshape(8, 4, mesh.shape["tp"]), ("sp_0", "sp_1", "tp"))
    in_specs = (
        P(SP_TP, None),
        P(SP, "tp"),
        P(SP, "tp"),
        P(SP, "tp"),
        P(SP, "tp"),
        P(SP, "tp"),
        P(SP, "tp"),
        P("tp"),
        P(SP, "tp"),
        P("tp"),
        P("tp"),
        P("tp", None),
        P(),
        P(SP, "tp"),
        P(SP, "tp"),
        P(SP, "tp"),
    )
    out_specs = P(SP_TP, None)
    return jax.shard_map(
        per_device, mesh=torus, in_specs=in_specs, out_specs=out_specs, check_vma=False
    )
```

```python
import functools

import jax
import jax.numpy as jnp
from jax import lax
from jax.experimental import pallas as pl
from jax.experimental.pallas import tpu as pltpu
from jax.sharding import Mesh
from jax.sharding import PartitionSpec as P

PER_GROUP_DIMS = 64
SP = ("sp_0", "sp_1")
SP_TP = ("sp_0", "sp_1", "tp")
MESH = pl.DeviceIdType.MESH

norm_eps = 1e-06
group_eps = 0.00064
half_step = 0.5
EXP_HALF = 0.6065306597126334

C = 64
TOGETHER = 2
LEVELS = (2, 4, 8, 16, 32)
F32 = jnp.float32
BF16 = jnp.bfloat16


def dot_nn(a, b):
    return lax.dot_general(a, b, (((1,), (0,)), ((), ())), preferred_element_type=F32)


def dot_nt(a, b):
    return lax.dot_general(a, b, (((1,), (1,)), ((), ())), preferred_element_type=F32)


def dot_tn(a, b):
    return lax.dot_general(a, b, (((0,), (0,)), ((), ())), preferred_element_type=F32)


def dot_tn_exact(a, b):
    return lax.dot_general(
        a,
        b,
        (((0,), (0,)), ((), ())),
        precision=lax.Precision.HIGHEST,
        preferred_element_type=F32,
    )


def two_parts(x):
    high = x.astype(BF16)
    return high, (x - high.astype(F32)).astype(BF16)


ROWS = 96
HALF = 1024


def ring_places():
    tp = lax.axis_index("tp")
    chip, core = tp // 2, tp % 2
    right = lax.rem(chip + 1, 4) * 2 + core
    left = lax.rem(chip + 3, 4) * 2 + core
    sibling = chip * 2 + 1 - core
    return chip, core, right, left, sibling


def remote(src, dst, send_sem, recv_sem, to):
    return pltpu.make_async_remote_copy(
        src_ref=src,
        dst_ref=dst,
        send_sem=send_sem,
        recv_sem=recv_sem,
        device_id={"tp": to},
        device_id_type=MESH,
    )


class RingSum:
    def __init__(self, part, sib, pair, relay, arrived, sems):
        self.part, self.sib, self.pair, self.relay, self.arrived = part, sib, pair, relay, arrived
        self.sib_send, self.sib_recv, self.send, self.recv = sems
        self.chip, self.core, self.right, self.left, self.sibling = ring_places()
        self.own = pl.ds(pl.multiple_of(self.core * ROWS, ROWS), ROWS)
        self.other = pl.ds(pl.multiple_of((1 - self.core) * ROWS, ROWS), ROWS)

    def to_sibling(self, d):
        return remote(
            self.part.at[d, :, self.other, :],
            self.sib.at[d],
            self.sib_send.at[d],
            self.sib_recv.at[d],
            self.sibling,
        )

    def hop(self, n):
        src, dst, to = (
            (self.pair.at[2, 0], self.relay.at[0], self.right),
            (self.pair.at[2, 1], self.relay.at[1], self.left),
            (self.pair.at[1, 1], self.arrived.at[0, 1], self.right),
            (self.pair.at[3, 0], self.arrived.at[1, 0], self.left),
            (self.pair.at[1, 0], self.arrived.at[0, 0], self.right),
            (self.pair.at[3, 1], self.arrived.at[1, 1], self.left),
        )[n]
        return remote(src, dst, self.send.at[n], self.recv.at[n], to)

    def produced(self, d):
        self.to_sibling(d).start()

    def summed(self, d, h):
        return self.part[d, h, self.own, :].astype(F32) + self.sib[d, h].astype(F32)

    def pass_on(self, d):
        self.to_sibling(d).wait_recv()
        if d == 2:
            self.pair[2, 0] = self.summed(2, 0).astype(BF16)
            self.hop(0).start()
            self.pair[2, 1] = self.summed(2, 1).astype(BF16)
            self.hop(1).start()
        if d == 1:
            self.pair[1, 1] = self.summed(1, 1).astype(BF16)
            self.hop(2).start()
        if d == 3:
            self.pair[3, 0] = self.summed(3, 0).astype(BF16)
            self.hop(3).start()

    def pass_relayed(self):
        self.hop(0).wait_recv()
        self.pair[1, 0] = (self.summed(1, 0) + self.relay[0].astype(F32)).astype(BF16)
        self.hop(4).start()
        self.hop(1).wait_recv()
        self.pair[3, 1] = (self.summed(3, 1) + self.relay[1].astype(F32)).astype(BF16)
        self.hop(5).start()

    def arrive(self):
        for n in (2, 3, 4, 5):
            self.hop(n).wait_recv()

    def result(self, h):
        return (
            self.summed(0, h)
            + self.arrived[0, h].astype(F32)
            + self.arrived[1, h].astype(F32)
        )

    def drain(self):
        for d in range(4):
            self.to_sibling(d).wait_send()
        for n in range(6):
            self.hop(n).wait_send()


RING_SUM_SCRATCH = [
    pltpu.VMEM((4, 2, 2 * ROWS, HALF), BF16),
    pltpu.VMEM((4, 2, ROWS, HALF), BF16),
    pltpu.VMEM((4, 2, ROWS, HALF), BF16),
    pltpu.VMEM((2, ROWS, HALF), BF16),
    pltpu.VMEM((2, 2, ROWS, HALF), BF16),
    pltpu.SemaphoreType.DMA((4,)),
    pltpu.SemaphoreType.DMA((4,)),
    pltpu.SemaphoreType.DMA((6,)),
    pltpu.SemaphoreType.DMA((6,)),
]


def greet_ring(barrier):
    _, _, right, left, sibling = ring_places()
    for to in (right, left, sibling):
        pl.semaphore_signal(barrier, inc=1, device_id={"tp": to}, device_id_type=MESH)


class WeightGather:
    def __init__(self, gate_up, down, n_z, n_y, send, recv):
        self.gate_up, self.down, self.n_z, self.n_y = gate_up, down, n_z, n_y
        self.send, self.recv = send, recv
        self.z, self.y = lax.axis_index("sp_0"), lax.axis_index("sp_1")
        self.block = gate_up.shape[0] // (n_z * n_y)
        self.started = []

    def z_at(self, d):
        return lax.rem(self.z + d + self.n_z, self.n_z)

    def y_at(self, d):
        return lax.rem(self.y + d + self.n_y, self.n_y)

    def rows(self, z, y, way=None):
        start = (z * self.n_y + y) * self.block
        if way is None:
            return pl.ds(pl.multiple_of(start, 32), self.block)
        half = self.block // 2
        return pl.ds(pl.multiple_of(start + (0 if way > 0 else half), 32), half)

    def group(self, z, way=None):
        size = self.n_y * self.block
        if way is None:
            return pl.ds(pl.multiple_of(z * size, 32), size)
        half = size // 2
        return pl.ds(pl.multiple_of(z * size + (0 if way > 0 else half), 32), half)

    def copy(self, ref, rows, n, device):
        return pltpu.make_async_remote_copy(
            src_ref=ref.at[rows],
            dst_ref=ref.at[rows],
            send_sem=self.send.at[n],
            recv_sem=self.recv.at[n],
            device_id=device,
            device_id_type=MESH,
        )

    def zg(self, way, k, received=False):
        n = (k - 1) * 2 + (way < 0)
        half = way if k == self.n_z // 2 else None
        to = {"sp_0": self.z_at(way)}
        if received:
            return self.copy(self.gate_up, self.rows(self.z_at(-way * k), self.y, half), n, to)
        return self.copy(self.gate_up, self.rows(self.z_at(-way * (k - 1)), self.y, half), n, to)

    def zd(self, way, k, received=False):
        n = 8 + (k - 1) * 2 + (way < 0)
        half = way if k == self.n_z // 2 else None
        to = {"sp_0": self.z_at(way)}
        if received:
            return self.copy(self.down, self.group(self.z_at(-way * k), half), n, to)
        return self.copy(self.down, self.group(self.z_at(-way * (k - 1)), half), n, to)

    def yg(self, d, way, k, received=False):
        n = 16 + (d + 3) * 4 + (k - 1) * 2 + (way < 0)
        half = way if k == 2 else None
        z = self.z_at(d)
        to = {"sp_1": self.y_at(way)}
        if received:
            return self.copy(self.gate_up, self.rows(z, self.y_at(-way * k), half), n, to)
        return self.copy(self.gate_up, self.rows(z, self.y_at(-way * (k - 1)), half), n, to)

    def yd(self, way, k, received=False):
        n = 48 + (k - 1) * 2 + (way < 0)
        half = way if k == 2 else None
        to = {"sp_1": self.y_at(way)}
        if received:
            return self.copy(self.down, self.rows(self.z, self.y_at(-way * k), half), n, to)
        return self.copy(self.down, self.rows(self.z, self.y_at(-way * (k - 1)), half), n, to)

    def start(self, maker, *args):
        for way in (1, -1):
            maker(*args[:-1], way, args[-1]).start()
        self.started.append((maker, args))

    def wait(self, maker, *args):
        for way in (1, -1):
            maker(*args[:-1], way, args[-1], received=True).wait_recv()

    def step(self, n):
        s, w = self.start, self.wait
        if n == 0:
            s(self.yd, 1)
            s(self.zg, 1)
            s(self.yg, 0, 1)
        if n == 1:
            w(self.yd, 1)
            s(self.yd, 2)
            w(self.zg, 1)
            s(self.zg, 2)
            s(self.yg, -1, 1)
            s(self.yg, 1, 1)
        if n == 2:
            w(self.yd, 2)
            s(self.zd, 1)
            w(self.yg, 0, 1)
            s(self.yg, 0, 2)
        if n == 3:
            w(self.zg, 2)
            s(self.zg, 3)
            s(self.yg, -2, 1)
            s(self.yg, 2, 1)
        if n == 4:
            for d in (-1, 1):
                w(self.yg, d, 1)
                s(self.yg, d, 2)
        if n == 5:
            w(self.zd, 1)
            s(self.zd, 2)
        if n == 6:
            w(self.zg, 3)
            s(self.zg, 4)
            s(self.yg, -3, 1)
            s(self.yg, 3, 1)
        if n == 7:
            for d in (-2, 2):
                w(self.yg, d, 1)
                s(self.yg, d, 2)
        if n == 8:
            w(self.zd, 2)
            s(self.zd, 3)
        if n == 9:
            w(self.zg, 4)
            s(self.yg, 4, 1)
        if n == 10:
            for d in (-3, 3):
                w(self.yg, d, 1)
                s(self.yg, d, 2)
        if n == 11:
            w(self.zd, 3)
            s(self.zd, 4)
        if n == 12:
            w(self.yg, 4, 1)
            s(self.yg, 4, 2)

    def gate_up_here(self):
        for d in (0, -1, 1, -2, 2, -3, 3, 4):
            self.wait(self.yg, d, 2)

    def down_here(self):
        self.wait(self.zd, 4)

    def drain(self):
        for maker, args in self.started:
            for way in (1, -1):
                maker(*args[:-1], way, args[-1]).wait_send()


WEIGHT_COPIES = 52


def layer_kernel(
    n_z,
    n_y,
    r_hbm,
    k_hbm,
    v_hbm,
    gate_hbm,
    fd_hbm,
    afl_ref,
    foff_ref,
    sd_hbm,
    soff_ref,
    scale_ref,
    skip_ref,
    matrix_hbm,
    gain_ref,
    switch_hbm,
    expand_hbm,
    contract_hbm,
    out_ref,
    stream_ref,
    r_ref,
    k_ref,
    v_ref,
    gate_ref,
    fd_ref,
    sd_ref,
    matrix_ref,
    load_sem,
    mask_ref,
    level_ref,
    local_ref,
    coef_ref,
    extra_ref,
    sm_ref,
    packet_y,
    recv_y,
    packet_z,
    recv_z,
    s_ref,
    send_y_sem,
    recv_y_sem,
    send_z_sem,
    recv_z_sem,
    gate_up_ref,
    down_ref,
    rows_ref,
    hidden_ref,
    weight_load_sem,
    weight_send,
    weight_recv,
    row_send,
    row_recv,
    side_send,
    side_recv,
    *ring_refs,
):
    length, width = r_ref.shape
    heads = width // C
    place_z = lax.axis_index("sp_0")
    place_y = lax.axis_index("sp_1")

    loads = [
        pltpu.make_async_copy(src, dst, load_sem.at[n])
        for n, (src, dst) in enumerate(
            (
                (r_hbm, r_ref),
                (k_hbm, k_ref),
                (v_hbm, v_ref),
                (fd_hbm, fd_ref),
                (sd_hbm, sd_ref),
                (gate_hbm, gate_ref),
                (matrix_hbm, matrix_ref),
            )
        )
    ]
    gather = WeightGather(gate_up_ref, down_ref, n_z, n_y, weight_send, weight_recv)
    own_rows = gather.rows(place_z, place_y)
    ff = down_ref.shape[1]
    weight_loads = [
        pltpu.make_async_copy(contract_hbm, down_ref.at[own_rows], weight_load_sem.at[0])
    ]
    for n in range(ff // 128):
        for m, src in enumerate((switch_hbm, expand_hbm)):
            weight_loads.append(
                pltpu.make_async_copy(
                    src.at[:, pl.ds(128 * n, 128)],
                    gate_up_ref.at[own_rows, pl.ds(256 * n + 128 * m, 128)],
                    weight_load_sem.at[1 + 2 * n + m],
                )
            )
    for load in weight_loads + loads:
        load.start()
    barrier = pltpu.get_barrier_semaphore()
    greet_ring(barrier)
    for d in range(1, n_y):
        pl.semaphore_signal(
            barrier, inc=1, device_id={"sp_1": lax.rem(place_y + d, n_y)}, device_id_type=MESH
        )
    for d in range(1, n_z):
        pl.semaphore_signal(
            barrier, inc=1, device_id={"sp_0": lax.rem(place_z + d, n_z)}, device_id_type=MESH
        )

    big_row = lax.broadcasted_iota(jnp.int32, (width, width), 0)
    big_col = lax.broadcasted_iota(jnp.int32, (width, width), 1)
    same_head = (big_row // C) == (big_col // C)
    mask_ref[...] = jnp.where(same_head, 1.0, 0.0).astype(BF16)

    t_idx = lax.broadcasted_iota(jnp.int32, (C, width), 0)
    lane = lax.broadcasted_iota(jnp.int32, (C, width), 1)
    j_idx = lane % C
    strict = j_idx < t_idx
    inclusive = j_idx <= t_idx
    pick = jnp.where(
        lax.broadcasted_iota(jnp.int32, (heads, width), 1) // C
        == lax.broadcasted_iota(jnp.int32, (heads, width), 0),
        1.0,
        0.0,
    ).astype(F32)
    eye = jnp.where(j_idx == t_idx, 1.0, 0.0).astype(F32)
    for n, b in enumerate(LEVELS):
        rb = (big_row % C) // b
        cb = (big_col % C) // b
        level_ref[n] = jnp.where(
            same_head & (rb % 2 == 1) & (cb == rb - 1), 1.0, 0.0
        ).astype(BF16)
    first_level = (t_idx % 2 == 1) & (j_idx == t_idx - 1)

    tri = jnp.where(
        (lax.broadcasted_iota(jnp.int32, (C, 2 * C), 1) % C)
        <= lax.broadcasted_iota(jnp.int32, (C, 2 * C), 0),
        1.0,
        0.0,
    ).astype(BF16)

    def tiled(x):
        return jnp.concatenate([x.astype(BF16)] * heads, axis=0)

    def bd(x):
        return tiled(x) * mask_ref[...]

    def diagonal_of(full):
        out = full[0:C]
        for h in range(1, heads):
            out = jnp.where(lane >= h * C, full[h * C : (h + 1) * C], out)
        return out

    sm_ref[0:C, :] = jnp.zeros((C, width), F32)
    sm_ref[C:, :] = eye

    def chunk(c, added, result):
        rows = pl.ds(pl.multiple_of(c * C, C), C)
        r = r_ref[rows, :].astype(F32)
        k = k_ref[rows, :].astype(F32)
        vb = v_ref[rows, :]
        v = vb.astype(F32)
        log_step = added - EXP_HALF * jax.nn.sigmoid(foff_ref[...] + fd_ref[rows, :].astype(F32))
        rate = jax.nn.sigmoid(soff_ref[...] + sd_ref[rows, :].astype(F32))
        k_hi, k_lo = two_parts(k * k)
        d_hi, d_lo = two_parts(r * k * scale_ref[...])
        sums = dot_nn(jnp.concatenate([k_hi, k_lo, d_hi, d_lo], axis=0), mask_ref[...])
        l_hi, l_lo = two_parts(log_step)
        cum = dot_nn(tri, jnp.concatenate([l_hi, l_lo], axis=0))
        yield
        unit = k * lax.rsqrt(sums[0:C] + sums[C : 2 * C] + norm_eps)
        extra_ref[rows, :] = (sums[2 * C : 3 * C] + sums[3 * C :]) * v
        mid = cum[C // 2 - 1 : C // 2]
        end = cum[C - 1 : C]
        rel = cum - mid
        grow = jnp.exp(rel)
        shrink = jnp.exp(-rel)
        before_unit = jnp.exp(rel - log_step) * unit
        read_fwd = r * grow
        key_back = k * shrink
        erase_back = unit * rate * shrink
        grow_mid = jnp.exp(mid)
        grow_rest = jnp.exp(end - mid)
        grow_end = jnp.exp(end)
        left = jnp.concatenate([before_unit, read_fwd], axis=0).astype(BF16)
        by_key = dot_nt(left, bd(key_back))
        by_erase = dot_nt(left, bd(erase_back))
        yield
        key_both = jnp.concatenate(
            [jnp.where(strict, by_key[0:C], 0.0), jnp.where(inclusive, by_key[C:], 0.0)], axis=0
        ).astype(BF16)
        erase_past = jnp.where(strict, by_erase[0:C], 0.0)
        erase_read = jnp.where(inclusive, by_erase[C:], 0.0).astype(BF16)
        by_value = dot_nn(key_both, bd(vb))
        erase_tiled = tiled(erase_past)
        inv = eye - jnp.where(first_level, erase_past, 0.0)
        for n in range(len(LEVELS)):
            half = dot_nn(inv.astype(BF16), erase_tiled * level_ref[n])
            yield
            inv = inv - dot_nn(half.astype(BF16), bd(inv))
            yield
        inv_b = inv.astype(BF16)
        recalled = dot_nn(inv_b, bd(by_value[0:C]))
        carried_map = dot_nn(inv_b, bd(before_unit * grow_mid))
        yield
        recalled_b = recalled.astype(BF16)
        carried_b = carried_map.astype(BF16)
        local = by_value[C:] - dot_nn(erase_read, bd(recalled_b))
        from_start = (read_fwd * grow_mid - dot_nn(erase_read, bd(carried_b))).astype(BF16)
        key_end = (key_back * grow_rest).astype(BF16)
        erase_end = (erase_back * grow_rest).astype(BF16)
        gain = dot_tn(
            jnp.concatenate([vb, -recalled_b], axis=0),
            jnp.concatenate([key_end, erase_end], axis=0),
        )
        loss = dot_tn(carried_b, erase_end)
        yield
        result.append(
            (rows, local, from_start, diagonal_of(gain), loss.astype(BF16) * mask_ref[...], grow_end)
        )

    def group(g, _):
        for n in range(1, 6):

            @pl.when(g == n)
            def _():
                gather.step(n)

        added = dot_tn_exact(afl_ref[:, pl.ds(pl.multiple_of(g * C * TOGETHER, 128), C * TOGETHER)], pick)
        results = [[] for _ in range(TOGETHER)]
        running = [
            chunk(g * TOGETHER + n, added[n * C : (n + 1) * C], results[n]) for n in range(TOGETHER)
        ]
        while running:
            left_over = []
            for one in running:
                try:
                    next(one)
                    left_over.append(one)
                except StopIteration:
                    pass
            running = left_over
        sm = sm_ref[...]
        for n in range(TOGETHER):
            rows, local, from_start, gain, loss, grow_end = results[n][0]
            sm_b = sm.astype(BF16)
            local_ref[rows, :] = local + dot_nt(from_start, bd(sm_b[0:C]))
            coef_ref[rows, :] = dot_nt(from_start, bd(sm_b[C:])).astype(BF16)
            sm = sm * grow_end - dot_nn(sm_b, loss)
            sm = jnp.concatenate([sm[0:C] + gain, sm[C:]], axis=0)
        sm_ref[...] = sm
        return 0

    for load in weight_loads:
        load.wait()
    pl.semaphore_wait(barrier, n_y - 1 + n_z - 1 + 3)
    gather.step(0)
    for load in loads[:5]:
        load.wait()
    lax.fori_loop(0, length // (C * TOGETHER), group, 0)

    def followed_by(sm, packet):
        prod = dot_nn(sm.astype(BF16), bd(packet[C:]))
        return jnp.concatenate([prod[0:C] + packet[0:C].astype(F32), prod[C:]], axis=0)

    own = sm_ref[...].astype(BF16)
    packet_y[...] = own
    recv_y[place_y] = own

    def copy_y(to, slot):
        return pltpu.make_async_remote_copy(
            src_ref=packet_y,
            dst_ref=recv_y.at[slot],
            send_sem=send_y_sem.at[to],
            recv_sem=recv_y_sem.at[slot],
            device_id={"sp_1": to},
            device_id_type=MESH,
        )

    for d in range(1, n_y):
        copy_y(lax.rem(place_y + d, n_y), place_y).start()
    gather.step(6)
    for d in range(1, n_y):
        peer = lax.rem(place_y + n_y - d, n_y)
        copy_y(peer, peer).wait_recv()
    total = recv_y[0].astype(F32)
    inside = jnp.concatenate([jnp.zeros((C, width), F32), eye], axis=0)
    for m in range(1, n_y):
        inside = jnp.where(place_y == m, total, inside)
        total = followed_by(total, recv_y[m])
    packet_z[...] = total.astype(BF16)

    def copy_z(to, slot):
        return pltpu.make_async_remote_copy(
            src_ref=packet_z,
            dst_ref=recv_z.at[slot],
            send_sem=send_z_sem.at[to],
            recv_sem=recv_z_sem.at[slot],
            device_id={"sp_0": to},
            device_id_type=MESH,
        )

    for d in range(1, n_z):

        @pl.when(place_z + d < n_z)
        def _():
            copy_z(place_z + d, place_z).start()

    gather.step(7)
    s_ref[...] = jnp.zeros((C, width), F32)
    for m in range(n_z - 1):

        @pl.when(m < place_z)
        def _():
            copy_z(m, m).wait_recv()
            arrived = recv_z[m]
            s_ref[...] = (
                dot_nn(s_ref[...].astype(BF16), bd(arrived[C:])) + arrived[0:C].astype(F32)
            )

    incoming = dot_nn(s_ref[...].astype(BF16), bd(inside[C:])) + inside[0:C]
    incoming_bd = bd(incoming)
    loads[5].wait()
    loads[6].wait()

    span = 2 * ROWS
    ring = RingSum(*ring_refs[:5], ring_refs[5:9])

    def produce(d):
        start = lax.rem(ring.chip + d, 4) * span
        rows = pl.ds(pl.multiple_of(start, span), span)
        outcome = local_ref[rows, :] + dot_nt(coef_ref[rows, :], incoming_bd)
        o_hi, o_lo = two_parts(outcome)
        centre = dot_nn(jnp.concatenate([o_hi, o_lo], axis=0), mask_ref[...])
        away = outcome - (centre[0:span] + centre[span:]) * (1.0 / C)
        a_hi, a_lo = two_parts(away * away)
        spread = dot_nn(jnp.concatenate([a_hi, a_lo], axis=0), mask_ref[...])
        spread = (spread[0:span] + spread[span:]) * (1.0 / C)
        normed = away * lax.rsqrt(spread + group_eps)
        mixed = ((normed + extra_ref[rows, :]) * gate_ref[rows, :].astype(F32)).astype(BF16)
        for h in range(2):
            for n in range(HALF // 256):
                ring.part[d, h, :, pl.ds(256 * n, 256)] = dot_nn(
                    mixed, matrix_ref[:, pl.ds(h * HALF + 256 * n, 256)]
                ).astype(BF16)
        ring.produced(d)

    gather.step(8)
    produce(2)
    produce(1)
    gather.step(9)
    ring.pass_on(2)
    produce(3)
    ring.pass_on(1)
    gather.step(10)
    produce(0)
    ring.pass_on(3)
    gather.step(11)
    ring.pass_relayed()
    ring.to_sibling(0).wait_recv()
    ring.arrive()
    squares = jnp.zeros((ROWS, 1), F32)
    for h in range(2):
        cols = pl.ds(h * HALF, HALF)
        stream = skip_ref[:, cols].astype(F32) + ring.result(h)
        stream_ref[:, cols] = stream
        squares = squares + jnp.sum(stream * stream, axis=1, keepdims=True)
    scale_rows = lax.rsqrt(squares * (1.0 / (2 * HALF)) + norm_eps)
    chip, core, right, left, sibling = ring_places()
    here = pl.ds(pl.multiple_of(core * ROWS, ROWS), ROWS)
    there = pl.ds(pl.multiple_of((1 - core) * ROWS, ROWS), ROWS)

    def chip_at(d):
        return lax.rem(chip + d, 4)

    for h in range(2):
        cols = pl.ds(h * HALF, HALF)
        rows_ref[chip, h, here, :] = (stream_ref[:, cols] * scale_rows * gain_ref[:, cols]).astype(
            BF16
        )

    def hop(n):
        d, h, to = (
            (0, 0, right),
            (0, 1, left),
            (0, 1, right),
            (0, 0, left),
            (3, 0, right),
            (1, 1, left),
        )[n]
        block = rows_ref.at[chip_at(d), h, here, :]
        return remote(block, block, row_send.at[n], row_recv.at[n], to)

    def arrival(n):
        d, h = ((3, 0), (1, 1), (3, 1), (1, 0), (2, 0), (2, 1))[n]
        block = rows_ref.at[chip_at(d), h, here, :]
        return remote(block, block, row_send.at[n], row_recv.at[n], sibling)

    def side(n):
        d, h = ((0, 0), (0, 1), (1, 0), (1, 1), (3, 0), (3, 1), (2, 0), (2, 1))[n]
        block = rows_ref.at[chip_at(d), h, here, :]
        return remote(block, block, side_send.at[n], side_recv.at[n], sibling)

    def side_arrival(n):
        d, h = ((0, 0), (0, 1), (1, 0), (1, 1), (3, 0), (3, 1), (2, 0), (2, 1))[n]
        block = rows_ref.at[chip_at(d), h, there, :]
        return remote(block, block, side_send.at[n], side_recv.at[n], sibling)

    for n in range(4):
        hop(n).start()
    side(0).start()
    side(1).start()
    gather.step(12)

    ring_2 = RingSum(*ring_refs[9:14], ring_refs[14:])
    ff_half = hidden_ref.shape[1]

    def feed(d):
        block = chip_at(d)
        x = [rows_ref[block, 0], rows_ref[block, 1]]
        for n in range(ff_half // 128):
            cols = pl.ds(256 * n, 256)
            both = dot_nn(x[0], gate_up_ref[0:HALF, cols]) + dot_nn(x[1], gate_up_ref[HALF:, cols])
            gate_act, up_act = both[:, :128], both[:, 128:]
            hidden_ref[:, pl.ds(128 * n, 128)] = (
                gate_act * jax.nn.sigmoid(gate_act) * up_act
            ).astype(BF16)
        if d == 0:
            gather.down_here()
        hidden = hidden_ref[...]
        for h in range(2):
            for n in range(HALF // 256):
                ring_2.part[d, h, :, pl.ds(256 * n, 256)] = dot_nt(
                    hidden, down_ref[pl.ds(h * HALF + 256 * n, 256), :]
                ).astype(BF16)
        ring_2.produced(d)

    side_arrival(0).wait_recv()
    side_arrival(1).wait_recv()
    gather.gate_up_here()
    feed(0)
    arrival(0).wait_recv()
    hop(4).start()
    side(4).start()
    arrival(1).wait_recv()
    hop(5).start()
    side(3).start()
    arrival(2).wait_recv()
    side(5).start()
    arrival(3).wait_recv()
    side(2).start()
    side_arrival(4).wait_recv()
    side_arrival(5).wait_recv()
    feed(3)
    side_arrival(2).wait_recv()
    side_arrival(3).wait_recv()
    arrival(4).wait_recv()
    side(6).start()
    arrival(5).wait_recv()
    side(7).start()
    ring_2.pass_on(3)
    feed(1)
    ring_2.pass_on(1)
    side_arrival(6).wait_recv()
    side_arrival(7).wait_recv()
    feed(2)
    ring_2.pass_on(2)
    ring_2.pass_relayed()
    ring_2.to_sibling(0).wait_recv()
    ring_2.arrive()
    for h in range(2):
        out_ref[:, pl.ds(h * HALF, HALF)] = (
            stream_ref[:, pl.ds(h * HALF, HALF)] + half_step * ring_2.result(h)
        ).astype(BF16)
    ring_2.drain()
    for n in range(6):
        hop(n).wait_send()
    for n in range(8):
        side(n).wait_send()
    ring.drain()
    gather.drain()
    for d in range(1, n_y):
        to = lax.rem(place_y + d, n_y)
        copy_y(to, to).wait_send()
    for d in range(1, n_z):

        @pl.when(place_z + d < n_z)
        def _():
            copy_z(place_z + d, place_z).wait_send()


def layer(r, k, v, gate, fd, afl, foff, sd, soff, scale, skip, matrix, gain, switch, expand, contract):
    n_z, n_y = lax.axis_size("sp_0"), lax.axis_size("sp_1")
    length, width = r.shape
    ff = switch.shape[1]
    depth = switch.shape[0] * n_z * n_y
    vmem = pl.BlockSpec(memory_space=pltpu.VMEM)
    hbm = pl.BlockSpec(memory_space=pl.ANY)
    dma = pltpu.SemaphoreType.DMA
    return pl.pallas_call(
        functools.partial(layer_kernel, n_z, n_y),
        out_shape=jax.ShapeDtypeStruct((ROWS, 2 * HALF), BF16),
        in_specs=[hbm] * 5 + [vmem, vmem, hbm, vmem, vmem, vmem, hbm, vmem, hbm, hbm, hbm],
        out_specs=vmem,
        scratch_shapes=[pltpu.VMEM((ROWS, 2 * HALF), F32)]
        + [pltpu.VMEM((length, width), BF16)] * 6
        + [
            pltpu.VMEM((width, 2 * HALF), BF16),
            dma((7,)),
            pltpu.VMEM((width, width), BF16),
            pltpu.VMEM((len(LEVELS), width, width), BF16),
            pltpu.VMEM((length, width), F32),
            pltpu.VMEM((length, width), BF16),
            pltpu.VMEM((length, width), F32),
            pltpu.VMEM((2 * C, width), F32),
            pltpu.VMEM((2 * C, width), BF16),
            pltpu.VMEM((n_y, 2 * C, width), BF16),
            pltpu.VMEM((2 * C, width), BF16),
            pltpu.VMEM((n_z, 2 * C, width), BF16),
            pltpu.VMEM((C, width), F32),
            dma((n_y,)),
            dma((n_y,)),
            dma((n_z,)),
            dma((n_z,)),
            pltpu.VMEM((depth, 2 * ff), BF16),
            pltpu.VMEM((depth, ff), BF16),
            pltpu.VMEM((4, 2, 2 * ROWS, HALF), BF16),
            pltpu.VMEM((2 * ROWS, ff), BF16),
            dma((1 + 2 * (ff // 128),)),
            dma((WEIGHT_COPIES,)),
            dma((WEIGHT_COPIES,)),
            dma((6,)),
            dma((6,)),
            dma((8,)),
            dma((8,)),
        ]
        + RING_SUM_SCRATCH
        + RING_SUM_SCRATCH,
        compiler_params=pltpu.CompilerParams(
            collective_id=0, has_side_effects=True, vmem_limit_bytes=60 * 1024 * 1024
        ),
        cost_estimate=pl.CostEstimate(
            flops=40_000_000_000, bytes_accessed=8_000_000, transcendentals=0
        ),
        name="layer",
    )(
        r, k, v, gate, fd, afl.T, foff[None, :], sd, soff[None, :], scale[None, :], skip, matrix,
        gain[None, :], switch, expand, contract,
    )


def per_device(
    skip_stream,
    acceptance_signal,
    lookup_mapped,
    payload_mapped,
    result_switch,
    forget_dynamic_share,
    additive_forget_logarithm,
    forget_feature_offset,
    substitution_dynamic_share,
    substitution_feature_offset,
    diagonal_reward_scales,
    result_matrix,
    mlp_rescaler,
    switch_matrix,
    expand_matrix,
    contract_matrix,
):
    return layer(
        acceptance_signal,
        lookup_mapped,
        payload_mapped,
        result_switch,
        forget_dynamic_share,
        additive_forget_logarithm,
        forget_feature_offset,
        substitution_dynamic_share,
        substitution_feature_offset,
        diagonal_reward_scales,
        skip_stream,
        result_matrix,
        mlp_rescaler,
        switch_matrix,
        expand_matrix,
        contract_matrix,
    )


def solution(mesh):
    torus = Mesh(mesh.devices.reshape(8, 4, mesh.shape["tp"]), ("sp_0", "sp_1", "tp"))
    in_specs = (
        P(SP_TP, None),
        P(SP, "tp"),
        P(SP, "tp"),
        P(SP, "tp"),
        P(SP, "tp"),
        P(SP, "tp"),
        P(SP, "tp"),
        P("tp"),
        P(SP, "tp"),
        P("tp"),
        P("tp"),
        P("tp", None),
        P(),
        P(SP, "tp"),
        P(SP, "tp"),
        P(SP, "tp"),
    )
    out_specs = P(SP_TP, None)
    return jax.shard_map(
        per_device, mesh=torus, in_specs=in_specs, out_specs=out_specs, check_vma=False
    )
```

```python
import functools

import jax
import jax.numpy as jnp
from jax import lax
from jax.experimental import pallas as pl
from jax.experimental.pallas import tpu as pltpu
from jax.sharding import Mesh
from jax.sharding import PartitionSpec as P

PER_GROUP_DIMS = 64
SP = ("sp_0", "sp_1")
SP_TP = ("sp_0", "sp_1", "tp")
MESH = pl.DeviceIdType.MESH

norm_eps = 1e-06
group_eps = 0.00064
half_step = 0.5
EXP_HALF = 0.6065306597126334

C = 64
TOGETHER = 2
LEVELS = (2, 4, 8, 16, 32)
F32 = jnp.float32
BF16 = jnp.bfloat16


def dot_nn(a, b):
    return lax.dot_general(a, b, (((1,), (0,)), ((), ())), preferred_element_type=F32)


def dot_nt(a, b):
    return lax.dot_general(a, b, (((1,), (1,)), ((), ())), preferred_element_type=F32)


def dot_tn(a, b):
    return lax.dot_general(a, b, (((0,), (0,)), ((), ())), preferred_element_type=F32)


def dot_tn_exact(a, b):
    return lax.dot_general(
        a,
        b,
        (((0,), (0,)), ((), ())),
        precision=lax.Precision.HIGHEST,
        preferred_element_type=F32,
    )


def two_parts(x):
    high = x.astype(BF16)
    return high, (x - high.astype(F32)).astype(BF16)


ROWS = 96
BATCHES = 2
PIECE = ROWS // BATCHES
HALF = 1024


def ring_places():
    tp = lax.axis_index("tp")
    chip, core = tp // 2, tp % 2
    right = lax.rem(chip + 1, 4) * 2 + core
    left = lax.rem(chip + 3, 4) * 2 + core
    sibling = chip * 2 + 1 - core
    return chip, core, right, left, sibling


def remote(src, dst, send_sem, recv_sem, to):
    return pltpu.make_async_remote_copy(
        src_ref=src,
        dst_ref=dst,
        send_sem=send_sem,
        recv_sem=recv_sem,
        device_id={"tp": to},
        device_id_type=MESH,
    )


class RingSum:
    def __init__(self, part, sib, pair, relay, arrived, sems):
        self.part, self.sib, self.pair, self.relay, self.arrived = part, sib, pair, relay, arrived
        self.sib_send, self.sib_recv, self.send, self.recv = sems
        self.chip, self.core, self.right, self.left, self.sibling = ring_places()
        self.own = pl.ds(pl.multiple_of(self.core * PIECE, PIECE), PIECE)
        self.other = pl.ds(pl.multiple_of((1 - self.core) * PIECE, PIECE), PIECE)

    def to_sibling(self, d):
        return remote(
            self.part.at[d, :, self.other, :],
            self.sib.at[d],
            self.sib_send.at[d],
            self.sib_recv.at[d],
            self.sibling,
        )

    def hop(self, n):
        src, dst, to = (
            (self.pair.at[2, 0], self.relay.at[0], self.right),
            (self.pair.at[2, 1], self.relay.at[1], self.left),
            (self.pair.at[1, 1], self.arrived.at[0, 1], self.right),
            (self.pair.at[3, 0], self.arrived.at[1, 0], self.left),
            (self.pair.at[1, 0], self.arrived.at[0, 0], self.right),
            (self.pair.at[3, 1], self.arrived.at[1, 1], self.left),
        )[n]
        return remote(src, dst, self.send.at[n], self.recv.at[n], to)

    def produced(self, d):
        self.to_sibling(d).start()

    def summed(self, d, h):
        return self.part[d, h, self.own, :].astype(F32) + self.sib[d, h].astype(F32)

    def pass_on(self, d):
        self.to_sibling(d).wait_recv()
        if d == 2:
            self.pair[2, 0] = self.summed(2, 0).astype(BF16)
            self.hop(0).start()
            self.pair[2, 1] = self.summed(2, 1).astype(BF16)
            self.hop(1).start()
        if d == 1:
            self.pair[1, 1] = self.summed(1, 1).astype(BF16)
            self.hop(2).start()
        if d == 3:
            self.pair[3, 0] = self.summed(3, 0).astype(BF16)
            self.hop(3).start()

    def pass_relayed(self):
        self.hop(0).wait_recv()
        self.pair[1, 0] = (self.summed(1, 0) + self.relay[0].astype(F32)).astype(BF16)
        self.hop(4).start()
        self.hop(1).wait_recv()
        self.pair[3, 1] = (self.summed(3, 1) + self.relay[1].astype(F32)).astype(BF16)
        self.hop(5).start()

    def arrive(self):
        for n in (2, 3, 4, 5):
            self.hop(n).wait_recv()

    def result(self, h):
        return (
            self.summed(0, h)
            + self.arrived[0, h].astype(F32)
            + self.arrived[1, h].astype(F32)
        )

    def drain(self):
        for d in range(4):
            self.to_sibling(d).wait_send()
        for n in range(6):
            self.hop(n).wait_send()


RING_SUM_SCRATCH = [
    pltpu.VMEM((4, 2, 2 * PIECE, HALF), BF16),
    pltpu.VMEM((4, 2, PIECE, HALF), BF16),
    pltpu.VMEM((4, 2, PIECE, HALF), BF16),
    pltpu.VMEM((2, PIECE, HALF), BF16),
    pltpu.VMEM((2, 2, PIECE, HALF), BF16),
    pltpu.SemaphoreType.DMA((4,)),
    pltpu.SemaphoreType.DMA((4,)),
    pltpu.SemaphoreType.DMA((6,)),
    pltpu.SemaphoreType.DMA((6,)),
]


def greet_ring(barrier):
    _, _, right, left, sibling = ring_places()
    for to in (right, left, sibling):
        pl.semaphore_signal(barrier, inc=1, device_id={"tp": to}, device_id_type=MESH)


class WeightGather:
    def __init__(self, gate_up, down, n_z, n_y, send, recv):
        self.gate_up, self.down, self.n_z, self.n_y = gate_up, down, n_z, n_y
        self.send, self.recv = send, recv
        self.z, self.y = lax.axis_index("sp_0"), lax.axis_index("sp_1")
        self.block = gate_up.shape[0] // (n_z * n_y)
        self.started = []

    def z_at(self, d):
        return lax.rem(self.z + d + self.n_z, self.n_z)

    def y_at(self, d):
        return lax.rem(self.y + d + self.n_y, self.n_y)

    def rows(self, z, y, way=None):
        start = (z * self.n_y + y) * self.block
        if way is None:
            return pl.ds(pl.multiple_of(start, 32), self.block)
        half = self.block // 2
        return pl.ds(pl.multiple_of(start + (0 if way > 0 else half), 32), half)

    def group(self, z, way=None):
        size = self.n_y * self.block
        if way is None:
            return pl.ds(pl.multiple_of(z * size, 32), size)
        half = size // 2
        return pl.ds(pl.multiple_of(z * size + (0 if way > 0 else half), 32), half)

    def copy(self, ref, rows, n, device):
        return pltpu.make_async_remote_copy(
            src_ref=ref.at[rows],
            dst_ref=ref.at[rows],
            send_sem=self.send.at[n],
            recv_sem=self.recv.at[n],
            device_id=device,
            device_id_type=MESH,
        )

    def zg(self, way, k, received=False):
        n = (k - 1) * 2 + (way < 0)
        half = way if k == self.n_z // 2 else None
        to = {"sp_0": self.z_at(way)}
        if received:
            return self.copy(self.gate_up, self.rows(self.z_at(-way * k), self.y, half), n, to)
        return self.copy(self.gate_up, self.rows(self.z_at(-way * (k - 1)), self.y, half), n, to)

    def zd(self, way, k, received=False):
        n = 8 + (k - 1) * 2 + (way < 0)
        half = way if k == self.n_z // 2 else None
        to = {"sp_0": self.z_at(way)}
        if received:
            return self.copy(self.down, self.group(self.z_at(-way * k), half), n, to)
        return self.copy(self.down, self.group(self.z_at(-way * (k - 1)), half), n, to)

    def yg(self, d, way, k, received=False):
        n = 16 + (d + 3) * 4 + (k - 1) * 2 + (way < 0)
        half = way if k == 2 else None
        z = self.z_at(d)
        to = {"sp_1": self.y_at(way)}
        if received:
            return self.copy(self.gate_up, self.rows(z, self.y_at(-way * k), half), n, to)
        return self.copy(self.gate_up, self.rows(z, self.y_at(-way * (k - 1)), half), n, to)

    def yd(self, way, k, received=False):
        n = 48 + (k - 1) * 2 + (way < 0)
        half = way if k == 2 else None
        to = {"sp_1": self.y_at(way)}
        if received:
            return self.copy(self.down, self.rows(self.z, self.y_at(-way * k), half), n, to)
        return self.copy(self.down, self.rows(self.z, self.y_at(-way * (k - 1)), half), n, to)

    def start(self, maker, *args):
        for way in (1, -1):
            maker(*args[:-1], way, args[-1]).start()
        self.started.append((maker, args))

    def wait(self, maker, *args):
        for way in (1, -1):
            maker(*args[:-1], way, args[-1], received=True).wait_recv()

    def both(self, act, d, k):
        for side in (-d, d):
            act(self.yg, side, k)

    def step(self, n):
        s, w = self.start, self.wait
        if n == 1:
            s(self.yd, 1)
            s(self.zg, 1)
            s(self.yg, 0, 1)
        if n == 3:
            w(self.yd, 1)
            s(self.yd, 2)
            w(self.zg, 1)
            s(self.zg, 2)
            self.both(s, 1, 1)
        if n == 4:
            w(self.yd, 2)
            s(self.zd, 1)
            w(self.yg, 0, 1)
            s(self.yg, 0, 2)
        if n == 5:
            w(self.zg, 2)
            s(self.zg, 3)
        if n == 6:
            self.both(s, 2, 1)
        if n == 7:
            self.both(w, 1, 1)
            self.both(s, 1, 2)
            w(self.zd, 1)
            s(self.zd, 2)
        if n == 8:
            w(self.zg, 3)
            s(self.zg, 4)
        if n == 15:
            self.both(s, 3, 1)
        if n == 9:
            self.both(w, 2, 1)
            self.both(s, 2, 2)
        if n == 10:
            w(self.zd, 2)
            s(self.zd, 3)
        if n == 11:
            w(self.zg, 4)
            s(self.yg, 4, 1)
        if n == 14:
            self.both(w, 3, 1)
            self.both(s, 3, 2)
        if n == 12:
            w(self.zd, 3)
            s(self.zd, 4)
        if n == 13:
            w(self.yg, 4, 1)
            s(self.yg, 4, 2)

    def gate_up_here(self):
        for d in (0, -1, 1, -2, 2, -3, 3, 4):
            self.wait(self.yg, d, 2)

    def down_here(self):
        self.wait(self.zd, 4)

    def drain(self):
        for maker, args in self.started:
            for way in (1, -1):
                maker(*args[:-1], way, args[-1]).wait_send()


WEIGHT_COPIES = 52


def layer_kernel(
    n_z,
    n_y,
    r_hbm,
    k_hbm,
    v_hbm,
    gate_hbm,
    fd_hbm,
    afl_ref,
    foff_ref,
    sd_hbm,
    soff_ref,
    scale_ref,
    skip_ref,
    matrix_hbm,
    gain_ref,
    switch_hbm,
    expand_hbm,
    contract_hbm,
    out_ref,
    stream_ref,
    r_ref,
    k_ref,
    v_ref,
    gate_ref,
    fd_ref,
    sd_ref,
    matrix_ref,
    load_sem,
    mask_ref,
    level_ref,
    local_ref,
    coef_ref,
    extra_ref,
    sm_ref,
    packet_y,
    recv_y,
    packet_z,
    recv_z,
    packet_in,
    recv_in,
    s_ref,
    send_in_sem,
    recv_in_sem,
    send_y_sem,
    recv_y_sem,
    send_z_sem,
    recv_z_sem,
    gate_up_ref,
    down_ref,
    rows_ref,
    hidden_ref,
    weight_load_sem,
    weight_send,
    weight_recv,
    row_send,
    row_recv,
    side_send,
    side_recv,
    *ring_refs,
):
    length, width = r_ref.shape
    heads = width // C
    place_z = lax.axis_index("sp_0")
    place_y = lax.axis_index("sp_1")

    loads = [
        pltpu.make_async_copy(src, dst, load_sem.at[n])
        for n, (src, dst) in enumerate(
            (
                (r_hbm, r_ref),
                (k_hbm, k_ref),
                (v_hbm, v_ref),
                (fd_hbm, fd_ref),
                (sd_hbm, sd_ref),
                (gate_hbm, gate_ref),
                (matrix_hbm, matrix_ref),
            )
        )
    ]
    gather = WeightGather(gate_up_ref, down_ref, n_z, n_y, weight_send, weight_recv)
    own_rows = gather.rows(place_z, place_y)
    ff = down_ref.shape[1]
    weight_loads = [
        pltpu.make_async_copy(contract_hbm, down_ref.at[own_rows], weight_load_sem.at[0])
    ]
    for n in range(ff // 128):
        for m, src in enumerate((switch_hbm, expand_hbm)):
            weight_loads.append(
                pltpu.make_async_copy(
                    src.at[:, pl.ds(128 * n, 128)],
                    gate_up_ref.at[own_rows, pl.ds(256 * n + 128 * m, 128)],
                    weight_load_sem.at[1 + 2 * n + m],
                )
            )
    for load in loads[:5] + weight_loads + loads[5:]:
        load.start()
    barrier = pltpu.get_barrier_semaphore()
    greet_ring(barrier)
    for d in range(1, n_y):
        pl.semaphore_signal(
            barrier, inc=1, device_id={"sp_1": lax.rem(place_y + d, n_y)}, device_id_type=MESH
        )
    for d in range(1, n_z):
        pl.semaphore_signal(
            barrier, inc=1, device_id={"sp_0": lax.rem(place_z + d, n_z)}, device_id_type=MESH
        )

    big_row = lax.broadcasted_iota(jnp.int32, (width, width), 0)
    big_col = lax.broadcasted_iota(jnp.int32, (width, width), 1)
    same_head = (big_row // C) == (big_col // C)
    mask_ref[...] = jnp.where(same_head, 1.0, 0.0).astype(BF16)

    t_idx = lax.broadcasted_iota(jnp.int32, (C, width), 0)
    lane = lax.broadcasted_iota(jnp.int32, (C, width), 1)
    j_idx = lane % C
    strict = j_idx < t_idx
    inclusive = j_idx <= t_idx
    pick = jnp.where(
        lax.broadcasted_iota(jnp.int32, (heads, width), 1) // C
        == lax.broadcasted_iota(jnp.int32, (heads, width), 0),
        1.0,
        0.0,
    ).astype(F32)
    eye = jnp.where(j_idx == t_idx, 1.0, 0.0).astype(F32)
    for n, b in enumerate(LEVELS):
        rb = (big_row % C) // b
        cb = (big_col % C) // b
        level_ref[n] = jnp.where(
            same_head & (rb % 2 == 1) & (cb == rb - 1), 1.0, 0.0
        ).astype(BF16)
    first_level = (t_idx % 2 == 1) & (j_idx == t_idx - 1)

    tri = jnp.where(
        (lax.broadcasted_iota(jnp.int32, (C, 2 * C), 1) % C)
        <= lax.broadcasted_iota(jnp.int32, (C, 2 * C), 0),
        1.0,
        0.0,
    ).astype(BF16)

    def tiled(x):
        return jnp.concatenate([x.astype(BF16)] * heads, axis=0)

    def bd(x):
        return tiled(x) * mask_ref[...]

    def diagonal_of(full):
        out = full[0:C]
        for h in range(1, heads):
            out = jnp.where(lane >= h * C, full[h * C : (h + 1) * C], out)
        return out

    sm_ref[0:C, :] = jnp.zeros((C, width), F32)
    sm_ref[C:, :] = eye

    def chunk(c, added, result):
        rows = pl.ds(pl.multiple_of(c * C, C), C)
        r = r_ref[rows, :].astype(F32)
        k = k_ref[rows, :].astype(F32)
        vb = v_ref[rows, :]
        v = vb.astype(F32)
        log_step = added - EXP_HALF * jax.nn.sigmoid(foff_ref[...] + fd_ref[rows, :].astype(F32))
        rate = jax.nn.sigmoid(soff_ref[...] + sd_ref[rows, :].astype(F32))
        k_hi, k_lo = two_parts(k * k)
        d_hi, d_lo = two_parts(r * k * scale_ref[...])
        sums = dot_nn(jnp.concatenate([k_hi, k_lo, d_hi, d_lo], axis=0), mask_ref[...])
        l_hi, l_lo = two_parts(log_step)
        cum = dot_nn(tri, jnp.concatenate([l_hi, l_lo], axis=0))
        yield
        unit = k * lax.rsqrt(sums[0:C] + sums[C : 2 * C] + norm_eps)
        extra_ref[rows, :] = (sums[2 * C : 3 * C] + sums[3 * C :]) * v
        mid = cum[C // 2 - 1 : C // 2]
        end = cum[C - 1 : C]
        rel = cum - mid
        grow = jnp.exp(rel)
        shrink = jnp.exp(-rel)
        before_unit = jnp.exp(rel - log_step) * unit
        read_fwd = r * grow
        key_back = k * shrink
        erase_back = unit * rate * shrink
        grow_mid = jnp.exp(mid)
        grow_rest = jnp.exp(end - mid)
        grow_end = jnp.exp(end)
        left = jnp.concatenate([before_unit, read_fwd], axis=0).astype(BF16)
        by_key = dot_nt(left, bd(key_back))
        by_erase = dot_nt(left, bd(erase_back))
        yield
        key_both = jnp.concatenate(
            [jnp.where(strict, by_key[0:C], 0.0), jnp.where(inclusive, by_key[C:], 0.0)], axis=0
        ).astype(BF16)
        erase_past = jnp.where(strict, by_erase[0:C], 0.0)
        erase_read = jnp.where(inclusive, by_erase[C:], 0.0).astype(BF16)
        by_value = dot_nn(key_both, bd(vb))
        erase_tiled = tiled(erase_past)
        inv = eye - jnp.where(first_level, erase_past, 0.0)
        for n in range(len(LEVELS)):
            half = dot_nn(inv.astype(BF16), erase_tiled * level_ref[n])
            yield
            inv = inv - dot_nn(half.astype(BF16), bd(inv))
            yield
        inv_b = inv.astype(BF16)
        recalled = dot_nn(inv_b, bd(by_value[0:C]))
        carried_map = dot_nn(inv_b, bd(before_unit * grow_mid))
        yield
        recalled_b = recalled.astype(BF16)
        carried_b = carried_map.astype(BF16)
        local = by_value[C:] - dot_nn(erase_read, bd(recalled_b))
        from_start = (read_fwd * grow_mid - dot_nn(erase_read, bd(carried_b))).astype(BF16)
        key_end = (key_back * grow_rest).astype(BF16)
        erase_end = (erase_back * grow_rest).astype(BF16)
        gain = dot_tn(
            jnp.concatenate([vb, -recalled_b], axis=0),
            jnp.concatenate([key_end, erase_end], axis=0),
        )
        loss = dot_tn(carried_b, erase_end)
        yield
        result.append(
            (rows, local, from_start, diagonal_of(gain), loss.astype(BF16) * mask_ref[...], grow_end)
        )

    def group(g, _):
        for n in (1, 3, 4, 5):

            @pl.when(g == n)
            def _():
                if n == 1:
                    for load in weight_loads:
                        load.wait()
                    pl.semaphore_wait(barrier, n_y - 1 + n_z - 1 + 3)
                gather.step(n)

        added = dot_tn_exact(afl_ref[:, pl.ds(pl.multiple_of(g * C * TOGETHER, 128), C * TOGETHER)], pick)
        results = [[] for _ in range(TOGETHER)]
        running = [
            chunk(g * TOGETHER + n, added[n * C : (n + 1) * C], results[n]) for n in range(TOGETHER)
        ]
        while running:
            left_over = []
            for one in running:
                try:
                    next(one)
                    left_over.append(one)
                except StopIteration:
                    pass
            running = left_over
        sm = sm_ref[...]
        for n in range(TOGETHER):
            rows, local, from_start, gain, loss, grow_end = results[n][0]
            sm_b = sm.astype(BF16)
            local_ref[rows, :] = local + dot_nt(from_start, bd(sm_b[0:C]))
            coef_ref[rows, :] = dot_nt(from_start, bd(sm_b[C:])).astype(BF16)
            sm = sm * grow_end - dot_nn(sm_b, loss)
            sm = jnp.concatenate([sm[0:C] + gain, sm[C:]], axis=0)
        sm_ref[...] = sm
        return 0

    for load in loads[:5]:
        load.wait()
    lax.fori_loop(0, length // (C * TOGETHER), group, 0)

    low = lax.broadcasted_iota(jnp.int32, (C, 2 * C), 1) < C

    def swapped(x):
        return jnp.concatenate([x[:, C:], x[:, :C]], axis=1)

    def map_of(packet):
        wide = packet.astype(F32)
        return jnp.concatenate(
            [jnp.where(low, swapped(wide), 0.0), jnp.where(low, 0.0, wide)], axis=0
        ).astype(BF16)

    def followed_by(before, packet):
        return dot_nn(before.astype(BF16), map_of(packet)) + jnp.where(low, packet.astype(F32), 0.0)

    sm = sm_ref[...]
    for h in range(heads):
        cols = slice(h * C, (h + 1) * C)
        packet_y[h] = jnp.concatenate([sm[0:C, cols], sm[C:, cols]], axis=1).astype(BF16)
    recv_y[place_y] = packet_y[place_y]

    def copy_y(to, slot):
        return pltpu.make_async_remote_copy(
            src_ref=packet_y.at[to],
            dst_ref=recv_y.at[slot],
            send_sem=send_y_sem.at[to],
            recv_sem=recv_y_sem.at[slot],
            device_id={"sp_1": to},
            device_id_type=MESH,
        )

    for d in range(1, n_y):
        copy_y(lax.rem(place_y + d, n_y), place_y).start()
    gather.step(6)
    for d in range(1, n_y):
        peer = lax.rem(place_y + n_y - d, n_y)
        copy_y(peer, peer).wait_recv()
    small_eye = jnp.where(
        lax.broadcasted_iota(jnp.int32, (C, 2 * C), 1)
        == lax.broadcasted_iota(jnp.int32, (C, 2 * C), 0) + C,
        1.0,
        0.0,
    ).astype(F32)
    insides = [small_eye, recv_y[0].astype(F32)]
    for m in range(1, n_y):
        insides.append(followed_by(insides[m], recv_y[m]))
    packet_z[...] = insides[n_y].astype(BF16)

    def copy_z(to, slot):
        return pltpu.make_async_remote_copy(
            src_ref=packet_z,
            dst_ref=recv_z.at[slot],
            send_sem=send_z_sem.at[to],
            recv_sem=recv_z_sem.at[slot],
            device_id={"sp_0": to},
            device_id_type=MESH,
        )

    for d in range(1, n_z):

        @pl.when(place_z + d < n_z)
        def _():
            copy_z(place_z + d, place_z).start()

    gather.step(7)
    gather.step(8)
    s_ref[...] = jnp.zeros((C, 2 * C), F32)
    for m in range(n_z - 1):

        @pl.when(m < place_z)
        def _():
            copy_z(m, m).wait_recv()
            s_ref[...] = jnp.where(low, followed_by(s_ref[...], recv_z[m]), 0.0)

    before = s_ref[...].astype(BF16)
    for m in range(n_y):
        inside = insides[m]
        packet_in[m] = (dot_nn(before, map_of(inside)) + jnp.where(low, inside, 0.0)).astype(BF16)
    recv_in[place_y] = packet_in[place_y]

    def copy_in(to, slot):
        return pltpu.make_async_remote_copy(
            src_ref=packet_in.at[to],
            dst_ref=recv_in.at[slot],
            send_sem=send_in_sem.at[to],
            recv_sem=recv_in_sem.at[slot],
            device_id={"sp_1": to},
            device_id_type=MESH,
        )

    for d in range(1, n_y):
        copy_in(lax.rem(place_y + d, n_y), place_y).start()
    gather.step(15)
    for d in range(1, n_y):
        peer = lax.rem(place_y + n_y - d, n_y)
        copy_in(peer, peer).wait_recv()
    blocks = []
    for h in range(heads):
        state = recv_in[h].astype(F32)
        state = jnp.where(low, state, 0.0) if h % 2 == 0 else jnp.where(low, 0.0, swapped(state))
        empty = jnp.zeros((C, 2 * C), F32)
        blocks.append(
            jnp.concatenate([state if p == h // 2 else empty for p in range(heads // 2)], axis=1)
        )
    incoming_bd = jnp.concatenate(blocks, axis=0).astype(BF16)
    loads[5].wait()
    loads[6].wait()

    span = 2 * PIECE
    rings = [RingSum(*ring_refs[9 * n : 9 * n + 5], ring_refs[9 * n + 5 : 9 * n + 9]) for n in range(2 * BATCHES)]
    chip, core, right, left, sibling = ring_places()
    here = pl.ds(pl.multiple_of(core * PIECE, PIECE), PIECE)
    there = pl.ds(pl.multiple_of((1 - core) * PIECE, PIECE), PIECE)

    def chip_at(d):
        return lax.rem(chip + d, 4)

    def produce(b, d):
        def taken(ref):
            first = chip_at(d) * (2 * ROWS) + b * PIECE
            return jnp.concatenate(
                [
                    ref[pl.ds(pl.multiple_of(first + n * ROWS, PIECE), PIECE), :].astype(F32)
                    for n in range(2)
                ],
                axis=0,
            )

        outcome = taken(local_ref) + dot_nt(taken(coef_ref).astype(BF16), incoming_bd)
        o_hi, o_lo = two_parts(outcome)
        centre = dot_nn(jnp.concatenate([o_hi, o_lo], axis=0), mask_ref[...])
        away = outcome - (centre[0:span] + centre[span:]) * (1.0 / C)
        a_hi, a_lo = two_parts(away * away)
        spread = dot_nn(jnp.concatenate([a_hi, a_lo], axis=0), mask_ref[...])
        spread = (spread[0:span] + spread[span:]) * (1.0 / C)
        normed = away * lax.rsqrt(spread + group_eps)
        mixed = ((normed + taken(extra_ref)) * taken(gate_ref)).astype(BF16)
        for h in range(2):
            for n in range(HALF // 256):
                rings[b].part[d, h, :, pl.ds(256 * n, 256)] = dot_nn(
                    mixed, matrix_ref[:, pl.ds(h * HALF + 256 * n, 256)]
                ).astype(BF16)
        rings[b].produced(d)

    def normed_rows(b):
        rows = pl.ds(b * PIECE, PIECE)
        squares = jnp.zeros((PIECE, 1), F32)
        for h in range(2):
            cols = pl.ds(h * HALF, HALF)
            stream = skip_ref[rows, cols].astype(F32) + rings[b].result(h)
            stream_ref[rows, cols] = stream
            squares = squares + jnp.sum(stream * stream, axis=1, keepdims=True)
        scale_rows = lax.rsqrt(squares * (1.0 / (2 * HALF)) + norm_eps)
        for h in range(2):
            cols = pl.ds(h * HALF, HALF)
            rows_ref[b, chip, h, here, :] = (
                stream_ref[rows, cols] * scale_rows * gain_ref[:, cols]
            ).astype(BF16)
        for n in range(4):
            hop(b, n).start()
        side(b, 0).start()
        side(b, 1).start()

    def hop(b, n):
        d, h, to = (
            (0, 0, right),
            (0, 1, left),
            (0, 1, right),
            (0, 0, left),
            (3, 0, right),
            (1, 1, left),
        )[n]
        block = rows_ref.at[b, chip_at(d), h, here, :]
        return remote(block, block, row_send.at[b, n], row_recv.at[b, n], to)

    def arrival(b, n):
        d, h = ((3, 0), (1, 1), (3, 1), (1, 0), (2, 0), (2, 1))[n]
        block = rows_ref.at[b, chip_at(d), h, here, :]
        return remote(block, block, row_send.at[b, n], row_recv.at[b, n], sibling)

    sides = ((0, 0), (0, 1), (1, 0), (1, 1), (3, 0), (3, 1), (2, 0), (2, 1))

    def side(b, n):
        d, h = sides[n]
        block = rows_ref.at[b, chip_at(d), h, here, :]
        return remote(block, block, side_send.at[b, n], side_recv.at[b, n], sibling)

    def side_arrival(b, n):
        d, h = sides[n]
        block = rows_ref.at[b, chip_at(d), h, there, :]
        return remote(block, block, side_send.at[b, n], side_recv.at[b, n], sibling)

    def relay_rows(b):
        arrival(b, 0).wait_recv()
        hop(b, 4).start()
        side(b, 4).start()
        arrival(b, 1).wait_recv()
        hop(b, 5).start()
        side(b, 3).start()

    def share_near(b):
        arrival(b, 2).wait_recv()
        side(b, 5).start()
        arrival(b, 3).wait_recv()
        side(b, 2).start()

    def share_far(b):
        arrival(b, 4).wait_recv()
        side(b, 6).start()
        arrival(b, 5).wait_recv()
        side(b, 7).start()

    def feed(*blocks):
        for b, d in blocks:
            for n in {0: (0, 1), 1: (2, 3), 3: (4, 5), 2: (6, 7)}[d]:
                side_arrival(b, n).wait_recv()
        x = [
            jnp.concatenate([rows_ref[b, chip_at(d), h] for b, d in blocks], axis=0)
            for h in range(2)
        ]
        filled = pl.ds(0, len(blocks) * span)
        for n in range(hidden_ref.shape[1] // 128):
            cols = pl.ds(256 * n, 256)
            both = dot_nn(x[0], gate_up_ref[0:HALF, cols]) + dot_nn(x[1], gate_up_ref[HALF:, cols])
            gate_act, up_act = both[:, :128], both[:, 128:]
            hidden_ref[filled, pl.ds(128 * n, 128)] = (
                gate_act * jax.nn.sigmoid(gate_act) * up_act
            ).astype(BF16)
        if blocks == ((0, 0),):
            gather.down_here()
        hidden = hidden_ref[filled, :]
        for h in range(2):
            for n in range(HALF // 256):
                product = dot_nt(hidden, down_ref[pl.ds(h * HALF + 256 * n, 256), :]).astype(BF16)
                for m, (b, d) in enumerate(blocks):
                    rings[BATCHES + b].part[d, h, :, pl.ds(256 * n, 256)] = product[
                        m * span : (m + 1) * span
                    ]
        for b, d in blocks:
            rings[BATCHES + b].produced(d)

    def finish(b):
        ring = rings[BATCHES + b]
        rows = pl.ds(b * PIECE, PIECE)
        ring.to_sibling(0).wait_recv()
        ring.arrive()
        for h in range(2):
            cols = pl.ds(h * HALF, HALF)
            out_ref[rows, cols] = (stream_ref[rows, cols] + half_step * ring.result(h)).astype(BF16)

    gather.step(9)
    produce(0, 2)
    gather.step(10)
    produce(0, 1)
    rings[0].pass_on(2)
    produce(0, 3)
    rings[0].pass_on(1)
    produce(0, 0)
    rings[0].pass_on(3)
    produce(1, 2)
    gather.step(11)
    produce(1, 1)
    rings[1].pass_on(2)
    produce(1, 3)
    gather.step(14)
    rings[0].pass_relayed()
    rings[1].pass_on(1)
    produce(1, 0)
    rings[1].pass_on(3)
    gather.step(12)
    rings[1].pass_relayed()
    rings[0].to_sibling(0).wait_recv()
    rings[0].arrive()
    normed_rows(0)
    gather.step(13)
    rings[1].to_sibling(0).wait_recv()
    rings[1].arrive()
    normed_rows(1)
    gather.gate_up_here()
    feed((0, 0))
    relay_rows(0)
    share_near(0)
    feed((0, 3), (0, 1))
    share_far(0)
    relay_rows(1)
    rings[2].pass_on(3)
    rings[2].pass_on(1)
    share_near(1)
    feed((0, 2), (1, 0))
    rings[2].pass_on(2)
    share_far(1)
    feed((1, 3), (1, 1))
    rings[2].pass_relayed()
    rings[3].pass_on(3)
    rings[3].pass_on(1)
    feed((1, 2))
    rings[3].pass_on(2)
    finish(0)
    rings[3].pass_relayed()
    finish(1)
    for ring in rings:
        ring.drain()
    for b in range(BATCHES):
        for n in range(6):
            hop(b, n).wait_send()
        for n in range(8):
            side(b, n).wait_send()
    gather.drain()
    for d in range(1, n_y):
        to = lax.rem(place_y + d, n_y)
        copy_y(to, to).wait_send()
        copy_in(to, to).wait_send()
    for d in range(1, n_z):

        @pl.when(place_z + d < n_z)
        def _():
            copy_z(place_z + d, place_z).wait_send()


def layer(r, k, v, gate, fd, afl, foff, sd, soff, scale, skip, matrix, gain, switch, expand, contract):
    n_z, n_y = lax.axis_size("sp_0"), lax.axis_size("sp_1")
    length, width = r.shape
    ff = switch.shape[1]
    depth = switch.shape[0] * n_z * n_y
    vmem = pl.BlockSpec(memory_space=pltpu.VMEM)
    hbm = pl.BlockSpec(memory_space=pl.ANY)
    dma = pltpu.SemaphoreType.DMA
    return pl.pallas_call(
        functools.partial(layer_kernel, n_z, n_y),
        out_shape=jax.ShapeDtypeStruct((ROWS, 2 * HALF), BF16),
        in_specs=[hbm] * 5 + [vmem, vmem, hbm, vmem, vmem, vmem, hbm, vmem, hbm, hbm, hbm],
        out_specs=vmem,
        scratch_shapes=[pltpu.VMEM((ROWS, 2 * HALF), F32)]
        + [pltpu.VMEM((length, width), BF16)] * 6
        + [
            pltpu.VMEM((width, 2 * HALF), BF16),
            dma((7,)),
            pltpu.VMEM((width, width), BF16),
            pltpu.VMEM((len(LEVELS), width, width), BF16),
            pltpu.VMEM((length, width), F32),
            pltpu.VMEM((length, width), BF16),
            pltpu.VMEM((length, width), F32),
            pltpu.VMEM((2 * C, width), F32),
            pltpu.VMEM((n_y, C, 2 * C), BF16),
            pltpu.VMEM((n_y, C, 2 * C), BF16),
            pltpu.VMEM((C, 2 * C), BF16),
            pltpu.VMEM((n_z, C, 2 * C), BF16),
            pltpu.VMEM((n_y, C, 2 * C), BF16),
            pltpu.VMEM((n_y, C, 2 * C), BF16),
            pltpu.VMEM((C, 2 * C), F32),
            dma((n_y,)),
            dma((n_y,)),
            dma((n_y,)),
            dma((n_y,)),
            dma((n_z,)),
            dma((n_z,)),
            pltpu.VMEM((depth, 2 * ff), BF16),
            pltpu.VMEM((depth, ff), BF16),
            pltpu.VMEM((BATCHES, 4, 2, 2 * PIECE, HALF), BF16),
            pltpu.VMEM((4 * PIECE, ff), BF16),
            dma((1 + 2 * (ff // 128),)),
            dma((WEIGHT_COPIES,)),
            dma((WEIGHT_COPIES,)),
            dma((BATCHES, 6)),
            dma((BATCHES, 6)),
            dma((BATCHES, 8)),
            dma((BATCHES, 8)),
        ]
        + RING_SUM_SCRATCH * (2 * BATCHES),
        compiler_params=pltpu.CompilerParams(
            collective_id=0, has_side_effects=True, vmem_limit_bytes=60 * 1024 * 1024
        ),
        cost_estimate=pl.CostEstimate(
            flops=40_000_000_000, bytes_accessed=8_000_000, transcendentals=0
        ),
        name="layer",
    )(
        r, k, v, gate, fd, afl.T, foff[None, :], sd, soff[None, :], scale[None, :], skip, matrix,
        gain[None, :], switch, expand, contract,
    )


def per_device(
    skip_stream,
    acceptance_signal,
    lookup_mapped,
    payload_mapped,
    result_switch,
    forget_dynamic_share,
    additive_forget_logarithm,
    forget_feature_offset,
    substitution_dynamic_share,
    substitution_feature_offset,
    diagonal_reward_scales,
    result_matrix,
    mlp_rescaler,
    switch_matrix,
    expand_matrix,
    contract_matrix,
):
    return layer(
        acceptance_signal,
        lookup_mapped,
        payload_mapped,
        result_switch,
        forget_dynamic_share,
        additive_forget_logarithm,
        forget_feature_offset,
        substitution_dynamic_share,
        substitution_feature_offset,
        diagonal_reward_scales,
        skip_stream,
        result_matrix,
        mlp_rescaler,
        switch_matrix,
        expand_matrix,
        contract_matrix,
    )


def solution(mesh):
    torus = Mesh(mesh.devices.reshape(8, 4, mesh.shape["tp"]), ("sp_0", "sp_1", "tp"))
    in_specs = (
        P(SP_TP, None),
        P(SP, "tp"),
        P(SP, "tp"),
        P(SP, "tp"),
        P(SP, "tp"),
        P(SP, "tp"),
        P(SP, "tp"),
        P("tp"),
        P(SP, "tp"),
        P("tp"),
        P("tp"),
        P("tp", None),
        P(),
        P(SP, "tp"),
        P(SP, "tp"),
        P(SP, "tp"),
    )
    out_specs = P(SP_TP, None)
    return jax.shard_map(
        per_device, mesh=torus, in_specs=in_specs, out_specs=out_specs, check_vma=False
    )
```

```python
import functools

import jax
import jax.numpy as jnp
from jax import lax
from jax.experimental import pallas as pl
from jax.experimental.pallas import tpu as pltpu
from jax.sharding import Mesh
from jax.sharding import PartitionSpec as P

PER_GROUP_DIMS = 64
SP = ("sp_0", "sp_1")
SP_TP = ("sp_0", "sp_1", "tp")
MESH = pl.DeviceIdType.MESH

norm_eps = 1e-06
group_eps = 0.00064
half_step = 0.5
EXP_HALF = 0.6065306597126334

C = 64
TOGETHER = 2
LEVELS = (2, 4, 8, 16, 32)
F32 = jnp.float32
BF16 = jnp.bfloat16


def dot_nn(a, b):
    return lax.dot_general(a, b, (((1,), (0,)), ((), ())), preferred_element_type=F32)


def dot_nt(a, b):
    return lax.dot_general(a, b, (((1,), (1,)), ((), ())), preferred_element_type=F32)


def dot_tn(a, b):
    return lax.dot_general(a, b, (((0,), (0,)), ((), ())), preferred_element_type=F32)


def dot_tn_exact(a, b):
    return lax.dot_general(
        a,
        b,
        (((0,), (0,)), ((), ())),
        precision=lax.Precision.HIGHEST,
        preferred_element_type=F32,
    )


def two_parts(x):
    high = x.astype(BF16)
    return high, (x - high.astype(F32)).astype(BF16)


ROWS = 96
BATCHES = 2
PIECE = ROWS // BATCHES
HALF = 1024


def ring_places():
    tp = lax.axis_index("tp")
    chip, core = tp // 2, tp % 2
    right = lax.rem(chip + 1, 4) * 2 + core
    left = lax.rem(chip + 3, 4) * 2 + core
    sibling = chip * 2 + 1 - core
    return chip, core, right, left, sibling


def remote(src, dst, send_sem, recv_sem, to):
    return pltpu.make_async_remote_copy(
        src_ref=src,
        dst_ref=dst,
        send_sem=send_sem,
        recv_sem=recv_sem,
        device_id={"tp": to},
        device_id_type=MESH,
    )


class RingSum:
    def __init__(self, part, sib, pair, relay, arrived, sems):
        self.part, self.sib, self.pair, self.relay, self.arrived = part, sib, pair, relay, arrived
        self.sib_send, self.sib_recv, self.send, self.recv = sems
        self.chip, self.core, self.right, self.left, self.sibling = ring_places()
        self.own = pl.ds(pl.multiple_of(self.core * PIECE, PIECE), PIECE)
        self.other = pl.ds(pl.multiple_of((1 - self.core) * PIECE, PIECE), PIECE)

    def to_sibling(self, d):
        return remote(
            self.part.at[d, :, self.other, :],
            self.sib.at[d],
            self.sib_send.at[d],
            self.sib_recv.at[d],
            self.sibling,
        )

    def hop(self, n):
        src, dst, to = (
            (self.pair.at[2, 0], self.relay.at[0], self.right),
            (self.pair.at[2, 1], self.relay.at[1], self.left),
            (self.pair.at[1, 1], self.arrived.at[0, 1], self.right),
            (self.pair.at[3, 0], self.arrived.at[1, 0], self.left),
            (self.pair.at[1, 0], self.arrived.at[0, 0], self.right),
            (self.pair.at[3, 1], self.arrived.at[1, 1], self.left),
        )[n]
        return remote(src, dst, self.send.at[n], self.recv.at[n], to)

    def produced(self, d):
        self.to_sibling(d).start()

    def summed(self, d, h):
        return self.part[d, h, self.own, :].astype(F32) + self.sib[d, h].astype(F32)

    def pass_on(self, d):
        self.to_sibling(d).wait_recv()
        if d == 2:
            self.pair[2, 0] = self.summed(2, 0).astype(BF16)
            self.hop(0).start()
            self.pair[2, 1] = self.summed(2, 1).astype(BF16)
            self.hop(1).start()
        if d == 1:
            self.pair[1, 1] = self.summed(1, 1).astype(BF16)
            self.hop(2).start()
        if d == 3:
            self.pair[3, 0] = self.summed(3, 0).astype(BF16)
            self.hop(3).start()

    def pass_relayed(self):
        self.hop(0).wait_recv()
        self.pair[1, 0] = (self.summed(1, 0) + self.relay[0].astype(F32)).astype(BF16)
        self.hop(4).start()
        self.hop(1).wait_recv()
        self.pair[3, 1] = (self.summed(3, 1) + self.relay[1].astype(F32)).astype(BF16)
        self.hop(5).start()

    def arrive(self):
        for n in (2, 3, 4, 5):
            self.hop(n).wait_recv()

    def result(self, h):
        return (
            self.summed(0, h)
            + self.arrived[0, h].astype(F32)
            + self.arrived[1, h].astype(F32)
        )

    def drain(self):
        for d in range(4):
            self.to_sibling(d).wait_send()
        for n in range(6):
            self.hop(n).wait_send()


RING_SUM_SCRATCH = [
    pltpu.VMEM((4, 2, 2 * PIECE, HALF), BF16),
    pltpu.VMEM((4, 2, PIECE, HALF), BF16),
    pltpu.VMEM((4, 2, PIECE, HALF), BF16),
    pltpu.VMEM((2, PIECE, HALF), BF16),
    pltpu.VMEM((2, 2, PIECE, HALF), BF16),
    pltpu.SemaphoreType.DMA((4,)),
    pltpu.SemaphoreType.DMA((4,)),
    pltpu.SemaphoreType.DMA((6,)),
    pltpu.SemaphoreType.DMA((6,)),
]


def greet_ring(barrier):
    _, _, right, left, sibling = ring_places()
    for to in (right, left, sibling):
        pl.semaphore_signal(barrier, inc=1, device_id={"tp": to}, device_id_type=MESH)


class WeightGather:
    def __init__(self, gate_up, down, n_z, n_y, send, recv):
        self.gate_up, self.down, self.n_z, self.n_y = gate_up, down, n_z, n_y
        self.send, self.recv = send, recv
        self.z, self.y = lax.axis_index("sp_0"), lax.axis_index("sp_1")
        self.block = gate_up.shape[0] // (n_z * n_y)
        self.started = []

    def z_at(self, d):
        return lax.rem(self.z + d + self.n_z, self.n_z)

    def y_at(self, d):
        return lax.rem(self.y + d + self.n_y, self.n_y)

    def rows(self, z, y, way=None):
        start = (z * self.n_y + y) * self.block
        if way is None:
            return pl.ds(pl.multiple_of(start, 32), self.block)
        half = self.block // 2
        return pl.ds(pl.multiple_of(start + (0 if way > 0 else half), 32), half)

    def group(self, z, way=None):
        size = self.n_y * self.block
        if way is None:
            return pl.ds(pl.multiple_of(z * size, 32), size)
        half = size // 2
        return pl.ds(pl.multiple_of(z * size + (0 if way > 0 else half), 32), half)

    def copy(self, ref, rows, n, device):
        return pltpu.make_async_remote_copy(
            src_ref=ref.at[rows],
            dst_ref=ref.at[rows],
            send_sem=self.send.at[n],
            recv_sem=self.recv.at[n],
            device_id=device,
            device_id_type=MESH,
        )

    def zg(self, way, k, received=False):
        n = (k - 1) * 2 + (way < 0)
        half = way if k == self.n_z // 2 else None
        to = {"sp_0": self.z_at(way)}
        if received:
            return self.copy(self.gate_up, self.rows(self.z_at(-way * k), self.y, half), n, to)
        return self.copy(self.gate_up, self.rows(self.z_at(-way * (k - 1)), self.y, half), n, to)

    def zd(self, way, k, received=False):
        n = 8 + (k - 1) * 2 + (way < 0)
        half = way if k == self.n_z // 2 else None
        to = {"sp_0": self.z_at(way)}
        if received:
            return self.copy(self.down, self.group(self.z_at(-way * k), half), n, to)
        return self.copy(self.down, self.group(self.z_at(-way * (k - 1)), half), n, to)

    def yg(self, d, way, k, received=False):
        n = 16 + (d + 3) * 4 + (k - 1) * 2 + (way < 0)
        half = way if k == 2 else None
        z = self.z_at(d)
        to = {"sp_1": self.y_at(way)}
        if received:
            return self.copy(self.gate_up, self.rows(z, self.y_at(-way * k), half), n, to)
        return self.copy(self.gate_up, self.rows(z, self.y_at(-way * (k - 1)), half), n, to)

    def yd(self, way, k, received=False):
        n = 48 + (k - 1) * 2 + (way < 0)
        half = way if k == 2 else None
        to = {"sp_1": self.y_at(way)}
        if received:
            return self.copy(self.down, self.rows(self.z, self.y_at(-way * k), half), n, to)
        return self.copy(self.down, self.rows(self.z, self.y_at(-way * (k - 1)), half), n, to)

    def start(self, maker, *args):
        for way in (1, -1):
            maker(*args[:-1], way, args[-1]).start()
        self.started.append((maker, args))

    def wait(self, maker, *args):
        for way in (1, -1):
            maker(*args[:-1], way, args[-1], received=True).wait_recv()

    def both(self, act, d, k):
        for side in (-d, d):
            act(self.yg, side, k)

    def step(self, n):
        s, w = self.start, self.wait
        if n == 1:
            s(self.yd, 1)
            s(self.zg, 1)
            s(self.yg, 0, 1)
        if n == 3:
            w(self.yd, 1)
            s(self.yd, 2)
            w(self.zg, 1)
            s(self.zg, 2)
            self.both(s, 1, 1)
        if n == 4:
            w(self.yd, 2)
            s(self.zd, 1)
            w(self.yg, 0, 1)
            s(self.yg, 0, 2)
        if n == 5:
            w(self.zg, 2)
            s(self.zg, 3)
        if n == 6:
            self.both(s, 2, 1)
        if n == 7:
            self.both(w, 1, 1)
            self.both(s, 1, 2)
            w(self.zd, 1)
            s(self.zd, 2)
        if n == 8:
            w(self.zg, 3)
            s(self.zg, 4)
        if n == 15:
            self.both(s, 3, 1)
        if n == 9:
            self.both(w, 2, 1)
            self.both(s, 2, 2)
        if n == 10:
            w(self.zd, 2)
            s(self.zd, 3)
        if n == 11:
            w(self.zg, 4)
            s(self.yg, 4, 1)
        if n == 14:
            self.both(w, 3, 1)
            self.both(s, 3, 2)
        if n == 12:
            w(self.zd, 3)
            s(self.zd, 4)
        if n == 13:
            w(self.yg, 4, 1)
            s(self.yg, 4, 2)

    def gate_up_here(self):
        for d in (0, -1, 1, -2, 2, -3, 3, 4):
            self.wait(self.yg, d, 2)

    def down_here(self):
        self.wait(self.zd, 4)

    def drain(self):
        for maker, args in self.started:
            for way in (1, -1):
                maker(*args[:-1], way, args[-1]).wait_send()


WEIGHT_COPIES = 52


def layer_kernel(
    n_z,
    n_y,
    r_hbm,
    k_hbm,
    v_hbm,
    gate_hbm,
    fd_hbm,
    afl_hbm,
    foff_hbm,
    sd_hbm,
    soff_hbm,
    scale_hbm,
    skip_hbm,
    matrix_hbm,
    gain_hbm,
    switch_hbm,
    expand_hbm,
    contract_hbm,
    out_ref,
    stream_ref,
    r_ref,
    k_ref,
    v_ref,
    gate_ref,
    fd_ref,
    sd_ref,
    matrix_ref,
    afl_ref,
    foff_ref,
    soff_ref,
    scale_ref,
    skip_ref,
    gain_ref,
    load_sem,
    mask_ref,
    level_ref,
    local_ref,
    coef_ref,
    extra_ref,
    sm_ref,
    packet_y,
    recv_y,
    packet_z,
    recv_z,
    packet_in,
    recv_in,
    send_in_sem,
    recv_in_sem,
    send_y_sem,
    recv_y_sem,
    send_z_sem,
    recv_z_sem,
    gate_up_ref,
    down_ref,
    rows_ref,
    hidden_ref,
    weight_load_sem,
    weight_send,
    weight_recv,
    row_send,
    row_recv,
    side_send,
    side_recv,
    *ring_refs,
):
    length, width = r_ref.shape
    heads = width // C
    place_z = lax.axis_index("sp_0")
    place_y = lax.axis_index("sp_1")

    loads = [
        pltpu.make_async_copy(src, dst, load_sem.at[n])
        for n, (src, dst) in enumerate(
            (
                (r_hbm, r_ref),
                (k_hbm, k_ref),
                (v_hbm, v_ref),
                (fd_hbm, fd_ref),
                (sd_hbm, sd_ref),
                (afl_hbm, afl_ref),
                (foff_hbm, foff_ref),
                (soff_hbm, soff_ref),
                (scale_hbm, scale_ref),
                (gate_hbm, gate_ref),
                (matrix_hbm, matrix_ref),
                (skip_hbm, skip_ref),
                (gain_hbm, gain_ref),
            )
        )
    ]
    gather = WeightGather(gate_up_ref, down_ref, n_z, n_y, weight_send, weight_recv)
    own_rows = gather.rows(place_z, place_y)
    ff = down_ref.shape[1]
    weight_loads = [
        pltpu.make_async_copy(contract_hbm, down_ref.at[own_rows], weight_load_sem.at[0])
    ]
    for n in range(ff // 128):
        for m, src in enumerate((switch_hbm, expand_hbm)):
            weight_loads.append(
                pltpu.make_async_copy(
                    src.at[:, pl.ds(128 * n, 128)],
                    gate_up_ref.at[own_rows, pl.ds(256 * n + 128 * m, 128)],
                    weight_load_sem.at[1 + 2 * n + m],
                )
            )
    for load in loads[:9] + weight_loads + loads[9:]:
        load.start()
    barrier = pltpu.get_barrier_semaphore()
    greet_ring(barrier)
    for d in range(1, n_y):
        pl.semaphore_signal(
            barrier, inc=1, device_id={"sp_1": lax.rem(place_y + d, n_y)}, device_id_type=MESH
        )
    for d in range(1, n_z):
        pl.semaphore_signal(
            barrier, inc=1, device_id={"sp_0": lax.rem(place_z + d, n_z)}, device_id_type=MESH
        )

    big_row = lax.broadcasted_iota(jnp.int32, (width, width), 0)
    big_col = lax.broadcasted_iota(jnp.int32, (width, width), 1)
    same_head = (big_row // C) == (big_col // C)
    mask_ref[...] = jnp.where(same_head, 1.0, 0.0).astype(BF16)

    t_idx = lax.broadcasted_iota(jnp.int32, (C, width), 0)
    lane = lax.broadcasted_iota(jnp.int32, (C, width), 1)
    j_idx = lane % C
    strict = j_idx < t_idx
    inclusive = j_idx <= t_idx
    pick = jnp.where(
        lax.broadcasted_iota(jnp.int32, (heads, width), 1) // C
        == lax.broadcasted_iota(jnp.int32, (heads, width), 0),
        1.0,
        0.0,
    ).astype(F32)
    eye = jnp.where(j_idx == t_idx, 1.0, 0.0).astype(F32)
    for n, b in enumerate(LEVELS):
        rb = (big_row % C) // b
        cb = (big_col % C) // b
        level_ref[n] = jnp.where(
            same_head & (rb % 2 == 1) & (cb == rb - 1), 1.0, 0.0
        ).astype(BF16)
    first_level = (t_idx % 2 == 1) & (j_idx == t_idx - 1)

    tri = jnp.where(
        (lax.broadcasted_iota(jnp.int32, (C, 2 * C), 1) % C)
        <= lax.broadcasted_iota(jnp.int32, (C, 2 * C), 0),
        1.0,
        0.0,
    ).astype(BF16)

    def tiled(x):
        return jnp.concatenate([x.astype(BF16)] * heads, axis=0)

    def bd(x):
        return tiled(x) * mask_ref[...]

    def bd2(x):
        return jnp.concatenate([x.astype(BF16)] * 2, axis=0) * mask_ref[0 : 2 * C, 0 : 2 * C]

    def paired(product, axis, a, x, y):
        outs = []
        for p in range(heads // 2):
            cols = slice(p * 2 * C, (p + 1) * 2 * C)
            right_side = jnp.concatenate([bd2(x[:, cols]), bd2(y[:, cols])], axis=axis)
            outs.append(product(a[:, cols], right_side))
        return (
            jnp.concatenate([o[:, : 2 * C] for o in outs], axis=1),
            jnp.concatenate([o[:, 2 * C :] for o in outs], axis=1),
        )

    def diagonal_of(full):
        out = full[0:C]
        for h in range(1, heads):
            out = jnp.where(lane >= h * C, full[h * C : (h + 1) * C], out)
        return out

    sm_ref[0:C, :] = jnp.zeros((C, width), F32)
    sm_ref[C:, :] = eye

    def chunk(c, added, result):
        rows = pl.ds(pl.multiple_of(c * C, C), C)
        r = r_ref[rows, :].astype(F32)
        k = k_ref[rows, :].astype(F32)
        vb = v_ref[rows, :]
        v = vb.astype(F32)
        log_step = added - EXP_HALF * jax.nn.sigmoid(foff_ref[...] + fd_ref[rows, :].astype(F32))
        rate = jax.nn.sigmoid(soff_ref[...] + sd_ref[rows, :].astype(F32))
        k_hi, k_lo = two_parts(k * k)
        d_hi, d_lo = two_parts(r * k * scale_ref[...])
        sums = dot_nn(jnp.concatenate([k_hi, k_lo, d_hi, d_lo], axis=0), mask_ref[...])
        l_hi, l_lo = two_parts(log_step)
        cum = dot_nn(tri, jnp.concatenate([l_hi, l_lo], axis=0))
        yield
        unit = k * lax.rsqrt(sums[0:C] + sums[C : 2 * C] + norm_eps)
        extra_ref[rows, :] = (sums[2 * C : 3 * C] + sums[3 * C :]) * v
        mid = cum[C // 2 - 1 : C // 2]
        end = cum[C - 1 : C]
        rel = cum - mid
        grow = jnp.exp(rel)
        shrink = jnp.exp(-rel)
        before_unit = jnp.exp(rel - log_step) * unit
        read_fwd = r * grow
        key_back = k * shrink
        erase_back = unit * rate * shrink
        grow_mid = jnp.exp(mid)
        grow_rest = jnp.exp(end - mid)
        grow_end = jnp.exp(end)
        left = jnp.concatenate([before_unit, read_fwd], axis=0).astype(BF16)
        by_key, by_erase = paired(dot_nt, 0, left, key_back, erase_back)
        yield
        key_both = jnp.concatenate(
            [jnp.where(strict, by_key[0:C], 0.0), jnp.where(inclusive, by_key[C:], 0.0)], axis=0
        ).astype(BF16)
        erase_past = jnp.where(strict, by_erase[0:C], 0.0)
        erase_read = jnp.where(inclusive, by_erase[C:], 0.0).astype(BF16)
        by_value = dot_nn(key_both, bd(vb))
        erase_tiled = tiled(erase_past)
        inv = eye - jnp.where(first_level, erase_past, 0.0)
        for n in range(len(LEVELS)):
            half = dot_nn(inv.astype(BF16), erase_tiled * level_ref[n])
            yield
            inv = inv - dot_nn(half.astype(BF16), bd(inv))
            yield
        inv_b = inv.astype(BF16)
        recalled, carried_map = paired(
            dot_nn, 1, inv_b, by_value[0:C], before_unit * grow_mid
        )
        yield
        recalled_b = recalled.astype(BF16)
        carried_b = carried_map.astype(BF16)
        local_less, start_less = paired(dot_nn, 1, erase_read, recalled_b, carried_b)
        local = by_value[C:] - local_less
        from_start = (read_fwd * grow_mid - start_less).astype(BF16)
        key_end = (key_back * grow_rest).astype(BF16)
        erase_end = (erase_back * grow_rest).astype(BF16)
        gain = dot_tn(
            jnp.concatenate([vb, -recalled_b], axis=0),
            jnp.concatenate([key_end, erase_end], axis=0),
        )
        loss = dot_tn(carried_b, erase_end)
        yield
        result.append(
            (rows, local, from_start, diagonal_of(gain), loss.astype(BF16) * mask_ref[...], grow_end)
        )

    def group(g, _):
        for n in (1, 3, 4, 5):

            @pl.when(g == n)
            def _():
                if n == 1:
                    for load in weight_loads:
                        load.wait()
                    pl.semaphore_wait(barrier, n_y - 1 + n_z - 1 + 3)
                gather.step(n)

        added = dot_tn_exact(afl_ref[:, pl.ds(pl.multiple_of(g * C * TOGETHER, 128), C * TOGETHER)], pick)
        results = [[] for _ in range(TOGETHER)]
        running = [
            chunk(g * TOGETHER + n, added[n * C : (n + 1) * C], results[n]) for n in range(TOGETHER)
        ]
        while running:
            left_over = []
            for one in running:
                try:
                    next(one)
                    left_over.append(one)
                except StopIteration:
                    pass
            running = left_over
        sm = sm_ref[...]
        for n in range(TOGETHER):
            rows, local, from_start, gain, loss, grow_end = results[n][0]
            sm_b = sm.astype(BF16)
            from_state, coef = paired(dot_nt, 0, from_start, sm_b[0:C], sm_b[C:])
            local_ref[rows, :] = local + from_state
            coef_ref[rows, :] = coef.astype(BF16)
            sm = sm * grow_end - dot_nn(sm_b, loss)
            sm = jnp.concatenate([sm[0:C] + gain, sm[C:]], axis=0)
        sm_ref[...] = sm
        return 0

    for load in loads[:9]:
        load.wait()
    lax.fori_loop(0, length // (C * TOGETHER), group, 0)

    low = lax.broadcasted_iota(jnp.int32, (C, 2 * C), 1) < C

    def swapped(x):
        return jnp.concatenate([x[:, C:], x[:, :C]], axis=1)

    def map_of(packet):
        wide = packet.astype(F32)
        return jnp.concatenate(
            [jnp.where(low, swapped(wide), 0.0), jnp.where(low, 0.0, wide)], axis=0
        ).astype(BF16)

    def followed_by(before, packet):
        return dot_nn(before.astype(BF16), map_of(packet)) + jnp.where(low, packet.astype(F32), 0.0)

    sm = sm_ref[...]
    for h in range(heads):
        cols = slice(h * C, (h + 1) * C)
        packet_y[h] = jnp.concatenate([sm[0:C, cols], sm[C:, cols]], axis=1).astype(BF16)
    recv_y[place_y] = packet_y[place_y]

    def copy_y(to, slot):
        return pltpu.make_async_remote_copy(
            src_ref=packet_y.at[to],
            dst_ref=recv_y.at[slot],
            send_sem=send_y_sem.at[to],
            recv_sem=recv_y_sem.at[slot],
            device_id={"sp_1": to},
            device_id_type=MESH,
        )

    for d in range(1, n_y):
        copy_y(lax.rem(place_y + d, n_y), place_y).start()
    gather.step(6)
    for d in range(1, n_y):
        peer = lax.rem(place_y + n_y - d, n_y)
        copy_y(peer, peer).wait_recv()
    small_eye = jnp.where(
        lax.broadcasted_iota(jnp.int32, (C, 2 * C), 1)
        == lax.broadcasted_iota(jnp.int32, (C, 2 * C), 0) + C,
        1.0,
        0.0,
    ).astype(F32)
    insides = [small_eye, recv_y[0].astype(F32)]
    for m in range(1, n_y):
        insides.append(followed_by(insides[m], recv_y[m]))
    packet_z[...] = insides[n_y].astype(BF16)

    def copy_z(to, slot):
        return pltpu.make_async_remote_copy(
            src_ref=packet_z,
            dst_ref=recv_z.at[slot],
            send_sem=send_z_sem.at[to],
            recv_sem=recv_z_sem.at[slot],
            device_id={"sp_0": to},
            device_id_type=MESH,
        )

    for d in range(1, n_z):

        @pl.when(place_z + d < n_z)
        def _():
            copy_z(place_z + d, place_z).start()

    gather.step(7)
    gather.step(8)
    for m in range(n_z - 1):

        @pl.when(m < place_z)
        def _():
            copy_z(m, m).wait_recv()

        @pl.when(m >= place_z)
        def _():
            recv_z[m] = small_eye.astype(BF16)

    runs = [recv_z[m] for m in range(n_z - 1)]
    while len(runs) > 1:
        runs = [
            followed_by(runs[m], runs[m + 1]) if m + 1 < len(runs) else runs[m]
            for m in range(0, len(runs), 2)
        ]
    before = jnp.where(low, runs[0].astype(F32), 0.0).astype(BF16)
    for m in range(n_y):
        inside = insides[m]
        packet_in[m] = (dot_nn(before, map_of(inside)) + jnp.where(low, inside, 0.0)).astype(BF16)
    recv_in[place_y] = packet_in[place_y]

    def copy_in(to, slot):
        return pltpu.make_async_remote_copy(
            src_ref=packet_in.at[to],
            dst_ref=recv_in.at[slot],
            send_sem=send_in_sem.at[to],
            recv_sem=recv_in_sem.at[slot],
            device_id={"sp_1": to},
            device_id_type=MESH,
        )

    for d in range(1, n_y):
        copy_in(lax.rem(place_y + d, n_y), place_y).start()
    gather.step(15)
    for d in range(1, n_y):
        peer = lax.rem(place_y + n_y - d, n_y)
        copy_in(peer, peer).wait_recv()
    blocks = []
    for h in range(heads):
        state = recv_in[h].astype(F32)
        state = jnp.where(low, state, 0.0) if h % 2 == 0 else jnp.where(low, 0.0, swapped(state))
        empty = jnp.zeros((C, 2 * C), F32)
        blocks.append(
            jnp.concatenate([state if p == h // 2 else empty for p in range(heads // 2)], axis=1)
        )
    incoming_bd = jnp.concatenate(blocks, axis=0).astype(BF16)
    for load in loads[9:]:
        load.wait()

    span = 2 * PIECE
    rings = [RingSum(*ring_refs[9 * n : 9 * n + 5], ring_refs[9 * n + 5 : 9 * n + 9]) for n in range(2 * BATCHES)]
    chip, core, right, left, sibling = ring_places()
    here = pl.ds(pl.multiple_of(core * PIECE, PIECE), PIECE)
    there = pl.ds(pl.multiple_of((1 - core) * PIECE, PIECE), PIECE)

    def chip_at(d):
        return lax.rem(chip + d, 4)

    def produce(b, d):
        def taken(ref):
            first = chip_at(d) * (2 * ROWS) + b * PIECE
            return jnp.concatenate(
                [
                    ref[pl.ds(pl.multiple_of(first + n * ROWS, PIECE), PIECE), :].astype(F32)
                    for n in range(2)
                ],
                axis=0,
            )

        outcome = taken(local_ref) + dot_nt(taken(coef_ref).astype(BF16), incoming_bd)
        o_hi, o_lo = two_parts(outcome)
        centre = dot_nn(jnp.concatenate([o_hi, o_lo], axis=0), mask_ref[...])
        away = outcome - (centre[0:span] + centre[span:]) * (1.0 / C)
        a_hi, a_lo = two_parts(away * away)
        spread = dot_nn(jnp.concatenate([a_hi, a_lo], axis=0), mask_ref[...])
        spread = (spread[0:span] + spread[span:]) * (1.0 / C)
        normed = away * lax.rsqrt(spread + group_eps)
        mixed = ((normed + taken(extra_ref)) * taken(gate_ref)).astype(BF16)
        for h in range(2):
            for n in range(HALF // 256):
                rings[b].part[d, h, :, pl.ds(256 * n, 256)] = dot_nn(
                    mixed, matrix_ref[:, pl.ds(h * HALF + 256 * n, 256)]
                ).astype(BF16)
        rings[b].produced(d)

    def normed_rows(b):
        rows = pl.ds(b * PIECE, PIECE)
        squares = jnp.zeros((PIECE, 1), F32)
        for h in range(2):
            cols = pl.ds(h * HALF, HALF)
            stream = skip_ref[rows, cols].astype(F32) + rings[b].result(h)
            stream_ref[rows, cols] = stream
            squares = squares + jnp.sum(stream * stream, axis=1, keepdims=True)
        scale_rows = lax.rsqrt(squares * (1.0 / (2 * HALF)) + norm_eps)
        for h in range(2):
            cols = pl.ds(h * HALF, HALF)
            rows_ref[b, chip, h, here, :] = (
                stream_ref[rows, cols] * scale_rows * gain_ref[:, cols]
            ).astype(BF16)
        for n in range(4):
            hop(b, n).start()
        side(b, 0).start()
        side(b, 1).start()

    def hop(b, n):
        d, h, to = (
            (0, 0, right),
            (0, 1, left),
            (0, 1, right),
            (0, 0, left),
            (3, 0, right),
            (1, 1, left),
        )[n]
        block = rows_ref.at[b, chip_at(d), h, here, :]
        return remote(block, block, row_send.at[b, n], row_recv.at[b, n], to)

    def arrival(b, n):
        d, h = ((3, 0), (1, 1), (3, 1), (1, 0), (2, 0), (2, 1))[n]
        block = rows_ref.at[b, chip_at(d), h, here, :]
        return remote(block, block, row_send.at[b, n], row_recv.at[b, n], sibling)

    sides = ((0, 0), (0, 1), (1, 0), (1, 1), (3, 0), (3, 1), (2, 0), (2, 1))

    def side(b, n):
        d, h = sides[n]
        block = rows_ref.at[b, chip_at(d), h, here, :]
        return remote(block, block, side_send.at[b, n], side_recv.at[b, n], sibling)

    def side_arrival(b, n):
        d, h = sides[n]
        block = rows_ref.at[b, chip_at(d), h, there, :]
        return remote(block, block, side_send.at[b, n], side_recv.at[b, n], sibling)

    def relay_rows(b):
        arrival(b, 0).wait_recv()
        hop(b, 4).start()
        side(b, 4).start()
        arrival(b, 1).wait_recv()
        hop(b, 5).start()
        side(b, 3).start()

    def share_near(b):
        arrival(b, 2).wait_recv()
        side(b, 5).start()
        arrival(b, 3).wait_recv()
        side(b, 2).start()

    def share_far(b):
        arrival(b, 4).wait_recv()
        side(b, 6).start()
        arrival(b, 5).wait_recv()
        side(b, 7).start()

    def feed(*blocks):
        for b, d in blocks:
            for n in {0: (0, 1), 1: (2, 3), 3: (4, 5), 2: (6, 7)}[d]:
                side_arrival(b, n).wait_recv()
        x = [
            jnp.concatenate([rows_ref[b, chip_at(d), h] for b, d in blocks], axis=0)
            for h in range(2)
        ]
        filled = pl.ds(0, len(blocks) * span)
        for n in range(hidden_ref.shape[1] // 128):
            cols = pl.ds(256 * n, 256)
            both = dot_nn(x[0], gate_up_ref[0:HALF, cols]) + dot_nn(x[1], gate_up_ref[HALF:, cols])
            gate_act, up_act = both[:, :128], both[:, 128:]
            hidden_ref[filled, pl.ds(128 * n, 128)] = (
                gate_act * jax.nn.sigmoid(gate_act) * up_act
            ).astype(BF16)
        if blocks == ((0, 0),):
            gather.down_here()
        hidden = hidden_ref[filled, :]
        for h in range(2):
            for n in range(HALF // 256):
                product = dot_nt(hidden, down_ref[pl.ds(h * HALF + 256 * n, 256), :]).astype(BF16)
                for m, (b, d) in enumerate(blocks):
                    rings[BATCHES + b].part[d, h, :, pl.ds(256 * n, 256)] = product[
                        m * span : (m + 1) * span
                    ]
        for b, d in blocks:
            rings[BATCHES + b].produced(d)

    def finish(b):
        ring = rings[BATCHES + b]
        rows = pl.ds(b * PIECE, PIECE)
        ring.to_sibling(0).wait_recv()
        ring.arrive()
        for h in range(2):
            cols = pl.ds(h * HALF, HALF)
            out_ref[rows, cols] = (stream_ref[rows, cols] + half_step * ring.result(h)).astype(BF16)

    gather.step(9)
    produce(0, 2)
    produce(0, 1)
    rings[0].pass_on(2)
    gather.step(10)
    produce(0, 3)
    rings[0].pass_on(1)
    produce(0, 0)
    rings[0].pass_on(3)
    produce(1, 2)
    gather.step(11)
    produce(1, 1)
    rings[1].pass_on(2)
    produce(1, 3)
    gather.step(14)
    rings[0].pass_relayed()
    rings[1].pass_on(1)
    produce(1, 0)
    rings[1].pass_on(3)
    gather.step(12)
    rings[1].pass_relayed()
    rings[0].to_sibling(0).wait_recv()
    rings[0].arrive()
    normed_rows(0)
    gather.step(13)
    rings[1].to_sibling(0).wait_recv()
    rings[1].arrive()
    normed_rows(1)
    gather.gate_up_here()
    feed((0, 0))
    relay_rows(0)
    share_near(0)
    feed((1, 0))
    relay_rows(1)
    feed((0, 3), (0, 1))
    share_far(0)
    share_near(1)
    rings[2].pass_on(3)
    rings[2].pass_on(1)
    feed((0, 2))
    share_far(1)
    rings[2].pass_on(2)
    feed((1, 2))
    rings[2].pass_relayed()
    rings[3].pass_on(2)
    feed((1, 3), (1, 1))
    rings[3].pass_on(3)
    rings[3].pass_on(1)
    rings[3].pass_relayed()
    finish(0)
    finish(1)
    for ring in rings:
        ring.drain()
    for b in range(BATCHES):
        for n in range(6):
            hop(b, n).wait_send()
        for n in range(8):
            side(b, n).wait_send()
    gather.drain()
    for d in range(1, n_y):
        to = lax.rem(place_y + d, n_y)
        copy_y(to, to).wait_send()
        copy_in(to, to).wait_send()
    for d in range(1, n_z):

        @pl.when(place_z + d < n_z)
        def _():
            copy_z(place_z + d, place_z).wait_send()


def layer(r, k, v, gate, fd, afl, foff, sd, soff, scale, skip, matrix, gain, switch, expand, contract):
    n_z, n_y = lax.axis_size("sp_0"), lax.axis_size("sp_1")
    length, width = r.shape
    ff = switch.shape[1]
    depth = switch.shape[0] * n_z * n_y
    vmem = pl.BlockSpec(memory_space=pltpu.VMEM)
    hbm = pl.BlockSpec(memory_space=pl.ANY)
    dma = pltpu.SemaphoreType.DMA
    return pl.pallas_call(
        functools.partial(layer_kernel, n_z, n_y),
        out_shape=jax.ShapeDtypeStruct((ROWS, 2 * HALF), BF16),
        in_specs=[hbm] * 16,
        out_specs=vmem,
        scratch_shapes=[pltpu.VMEM((ROWS, 2 * HALF), F32)]
        + [pltpu.VMEM((length, width), BF16)] * 6
        + [
            pltpu.VMEM((width, 2 * HALF), BF16),
            pltpu.VMEM((width // C, length), F32),
            pltpu.VMEM((1, width), F32),
            pltpu.VMEM((1, width), F32),
            pltpu.VMEM((1, width), F32),
            pltpu.VMEM((ROWS, 2 * HALF), BF16),
            pltpu.VMEM((1, 2 * HALF), F32),
            dma((13,)),
            pltpu.VMEM((width, width), BF16),
            pltpu.VMEM((len(LEVELS), width, width), BF16),
            pltpu.VMEM((length, width), F32),
            pltpu.VMEM((length, width), BF16),
            pltpu.VMEM((length, width), F32),
            pltpu.VMEM((2 * C, width), F32),
            pltpu.VMEM((n_y, C, 2 * C), BF16),
            pltpu.VMEM((n_y, C, 2 * C), BF16),
            pltpu.VMEM((C, 2 * C), BF16),
            pltpu.VMEM((n_z, C, 2 * C), BF16),
            pltpu.VMEM((n_y, C, 2 * C), BF16),
            pltpu.VMEM((n_y, C, 2 * C), BF16),
            dma((n_y,)),
            dma((n_y,)),
            dma((n_y,)),
            dma((n_y,)),
            dma((n_z,)),
            dma((n_z,)),
            pltpu.VMEM((depth, 2 * ff), BF16),
            pltpu.VMEM((depth, ff), BF16),
            pltpu.VMEM((BATCHES, 4, 2, 2 * PIECE, HALF), BF16),
            pltpu.VMEM((4 * PIECE, ff), BF16),
            dma((1 + 2 * (ff // 128),)),
            dma((WEIGHT_COPIES,)),
            dma((WEIGHT_COPIES,)),
            dma((BATCHES, 6)),
            dma((BATCHES, 6)),
            dma((BATCHES, 8)),
            dma((BATCHES, 8)),
        ]
        + RING_SUM_SCRATCH * (2 * BATCHES),
        compiler_params=pltpu.CompilerParams(
            collective_id=0, has_side_effects=True, vmem_limit_bytes=60 * 1024 * 1024
        ),
        cost_estimate=pl.CostEstimate(
            flops=40_000_000_000, bytes_accessed=8_000_000, transcendentals=0
        ),
        name="layer",
    )(
        r, k, v, gate, fd, afl.T, foff[None, :], sd, soff[None, :], scale[None, :], skip, matrix,
        gain[None, :], switch, expand, contract,
    )


def per_device(
    skip_stream,
    acceptance_signal,
    lookup_mapped,
    payload_mapped,
    result_switch,
    forget_dynamic_share,
    additive_forget_logarithm,
    forget_feature_offset,
    substitution_dynamic_share,
    substitution_feature_offset,
    diagonal_reward_scales,
    result_matrix,
    mlp_rescaler,
    switch_matrix,
    expand_matrix,
    contract_matrix,
):
    return layer(
        acceptance_signal,
        lookup_mapped,
        payload_mapped,
        result_switch,
        forget_dynamic_share,
        additive_forget_logarithm,
        forget_feature_offset,
        substitution_dynamic_share,
        substitution_feature_offset,
        diagonal_reward_scales,
        skip_stream,
        result_matrix,
        mlp_rescaler,
        switch_matrix,
        expand_matrix,
        contract_matrix,
    )


def solution(mesh):
    torus = Mesh(mesh.devices.reshape(8, 4, mesh.shape["tp"]), ("sp_0", "sp_1", "tp"))
    in_specs = (
        P(SP_TP, None),
        P(SP, "tp"),
        P(SP, "tp"),
        P(SP, "tp"),
        P(SP, "tp"),
        P(SP, "tp"),
        P(SP, "tp"),
        P("tp"),
        P(SP, "tp"),
        P("tp"),
        P("tp"),
        P("tp", None),
        P(),
        P(SP, "tp"),
        P(SP, "tp"),
        P(SP, "tp"),
    )
    out_specs = P(SP_TP, None)
    return jax.shard_map(
        per_device, mesh=torus, in_specs=in_specs, out_specs=out_specs, check_vma=False
    )
```

```python
import functools

import jax
import jax.numpy as jnp
from jax import lax
from jax.experimental import pallas as pl
from jax.experimental.pallas import tpu as pltpu
from jax.sharding import Mesh
from jax.sharding import PartitionSpec as P

PER_GROUP_DIMS = 64
SP = ("sp_0", "sp_1")
SP_TP = ("sp_0", "sp_1", "tp")
MESH = pl.DeviceIdType.MESH

norm_eps = 1e-06
group_eps = 0.00064
half_step = 0.5
EXP_HALF = 0.6065306597126334

C = 64
TOGETHER = 2
LEVELS = (2, 4, 8, 16, 32)
F32 = jnp.float32
BF16 = jnp.bfloat16


def dot_nn(a, b):
    return lax.dot_general(a, b, (((1,), (0,)), ((), ())), preferred_element_type=F32)


def dot_nt(a, b):
    return lax.dot_general(a, b, (((1,), (1,)), ((), ())), preferred_element_type=F32)


def dot_tn(a, b):
    return lax.dot_general(a, b, (((0,), (0,)), ((), ())), preferred_element_type=F32)


def dot_tn_exact(a, b):
    return lax.dot_general(
        a,
        b,
        (((0,), (0,)), ((), ())),
        precision=lax.Precision.HIGHEST,
        preferred_element_type=F32,
    )


def two_parts(x):
    high = x.astype(BF16)
    return high, (x - high.astype(F32)).astype(BF16)


ROWS = 96
BATCHES = 2
PIECE = ROWS // BATCHES
HALF = 1024


def ring_places():
    tp = lax.axis_index("tp")
    chip, core = tp // 2, tp % 2
    right = lax.rem(chip + 1, 4) * 2 + core
    left = lax.rem(chip + 3, 4) * 2 + core
    sibling = chip * 2 + 1 - core
    return chip, core, right, left, sibling


def remote(src, dst, send_sem, recv_sem, to):
    return pltpu.make_async_remote_copy(
        src_ref=src,
        dst_ref=dst,
        send_sem=send_sem,
        recv_sem=recv_sem,
        device_id={"tp": to},
        device_id_type=MESH,
    )


def all_sent(ref, sem):
    pltpu.make_async_copy(ref, ref, sem).wait()


class RingSum:
    def __init__(self, part, sib, pair, relay, arrived, sems):
        self.part, self.sib, self.pair, self.relay, self.arrived = part, sib, pair, relay, arrived
        self.sib_send, self.sib_recv, self.send, self.recv = sems
        self.chip, self.core, self.right, self.left, self.sibling = ring_places()
        self.own = pl.ds(pl.multiple_of(self.core * PIECE, PIECE), PIECE)
        self.other = pl.ds(pl.multiple_of((1 - self.core) * PIECE, PIECE), PIECE)

    def to_sibling(self, d):
        return remote(
            self.part.at[d, :, self.other, :],
            self.sib.at[d],
            self.sib_send.at[0],
            self.sib_recv.at[d],
            self.sibling,
        )

    def hop(self, n):
        src, dst, to = (
            (self.pair.at[2, 0], self.relay.at[0], self.right),
            (self.pair.at[2, 1], self.relay.at[1], self.left),
            (self.pair.at[1, 1], self.arrived.at[0, 1], self.right),
            (self.pair.at[3, 0], self.arrived.at[1, 0], self.left),
            (self.pair.at[1, 0], self.arrived.at[0, 0], self.right),
            (self.pair.at[3, 1], self.arrived.at[1, 1], self.left),
        )[n]
        return remote(src, dst, self.send.at[0], self.recv.at[n], to)

    def produced(self, d):
        self.to_sibling(d).start()

    def summed(self, d, h):
        return self.part[d, h, self.own, :].astype(F32) + self.sib[d, h].astype(F32)

    def pass_on(self, d):
        self.to_sibling(d).wait_recv()
        if d == 2:
            self.pair[2, 0] = self.summed(2, 0).astype(BF16)
            self.hop(0).start()
            self.pair[2, 1] = self.summed(2, 1).astype(BF16)
            self.hop(1).start()
        if d == 1:
            self.pair[1, 1] = self.summed(1, 1).astype(BF16)
            self.hop(2).start()
        if d == 3:
            self.pair[3, 0] = self.summed(3, 0).astype(BF16)
            self.hop(3).start()

    def pass_relayed(self):
        self.hop(0).wait_recv()
        self.pair[1, 0] = (self.summed(1, 0) + self.relay[0].astype(F32)).astype(BF16)
        self.hop(4).start()
        self.hop(1).wait_recv()
        self.pair[3, 1] = (self.summed(3, 1) + self.relay[1].astype(F32)).astype(BF16)
        self.hop(5).start()

    def arrive(self):
        for n in (2, 3, 4, 5):
            self.hop(n).wait_recv()

    def result(self, h):
        return (
            self.summed(0, h)
            + self.arrived[0, h].astype(F32)
            + self.arrived[1, h].astype(F32)
        )

    def drain(self):
        all_sent(self.sib, self.sib_send.at[0])
        all_sent(self.pair.at[0:3], self.send.at[0])


RING_SUM_SCRATCH = [
    pltpu.VMEM((4, 2, 2 * PIECE, HALF), BF16),
    pltpu.VMEM((4, 2, PIECE, HALF), BF16),
    pltpu.VMEM((4, 2, PIECE, HALF), BF16),
    pltpu.VMEM((2, PIECE, HALF), BF16),
    pltpu.VMEM((2, 2, PIECE, HALF), BF16),
    pltpu.SemaphoreType.DMA((1,)),
    pltpu.SemaphoreType.DMA((4,)),
    pltpu.SemaphoreType.DMA((1,)),
    pltpu.SemaphoreType.DMA((6,)),
]


def greet_ring(barrier):
    _, _, right, left, sibling = ring_places()
    for to in (right, left, sibling):
        pl.semaphore_signal(barrier, inc=1, device_id={"tp": to}, device_id_type=MESH)


class WeightGather:
    def __init__(self, gate_up, down, n_z, n_y, send, recv):
        self.gate_up, self.down, self.n_z, self.n_y = gate_up, down, n_z, n_y
        self.send, self.recv = send, recv
        self.z, self.y = lax.axis_index("sp_0"), lax.axis_index("sp_1")
        self.block = gate_up.shape[0] // (n_z * n_y)

    def z_at(self, d):
        return lax.rem(self.z + d + self.n_z, self.n_z)

    def y_at(self, d):
        return lax.rem(self.y + d + self.n_y, self.n_y)

    def rows(self, z, y, way=None):
        start = (z * self.n_y + y) * self.block
        if way is None:
            return pl.ds(pl.multiple_of(start, 32), self.block)
        half = self.block // 2
        return pl.ds(pl.multiple_of(start + (0 if way > 0 else half), 32), half)

    def group(self, z, way=None):
        size = self.n_y * self.block
        if way is None:
            return pl.ds(pl.multiple_of(z * size, 32), size)
        half = size // 2
        return pl.ds(pl.multiple_of(z * size + (0 if way > 0 else half), 32), half)

    def copy(self, ref, rows, n, device):
        return pltpu.make_async_remote_copy(
            src_ref=ref.at[rows],
            dst_ref=ref.at[rows],
            send_sem=self.send.at[0 if ref is self.gate_up else 1],
            recv_sem=self.recv.at[n],
            device_id=device,
            device_id_type=MESH,
        )

    def zg(self, way, k, received=False):
        n = (k - 1) * 2 + (way < 0)
        half = way if k == self.n_z // 2 else None
        to = {"sp_0": self.z_at(way)}
        if received:
            return self.copy(self.gate_up, self.rows(self.z_at(-way * k), self.y, half), n, to)
        return self.copy(self.gate_up, self.rows(self.z_at(-way * (k - 1)), self.y, half), n, to)

    def zd(self, way, k, received=False):
        n = 8 + (k - 1) * 2 + (way < 0)
        half = way if k == self.n_z // 2 else None
        to = {"sp_0": self.z_at(way)}
        if received:
            return self.copy(self.down, self.group(self.z_at(-way * k), half), n, to)
        return self.copy(self.down, self.group(self.z_at(-way * (k - 1)), half), n, to)

    def yg(self, d, way, k, received=False):
        n = 16 + (d + 3) * 4 + (k - 1) * 2 + (way < 0)
        half = way if k == 2 else None
        z = self.z_at(d)
        to = {"sp_1": self.y_at(way)}
        if received:
            return self.copy(self.gate_up, self.rows(z, self.y_at(-way * k), half), n, to)
        return self.copy(self.gate_up, self.rows(z, self.y_at(-way * (k - 1)), half), n, to)

    def yd(self, way, k, received=False):
        n = 48 + (k - 1) * 2 + (way < 0)
        half = way if k == 2 else None
        to = {"sp_1": self.y_at(way)}
        if received:
            return self.copy(self.down, self.rows(self.z, self.y_at(-way * k), half), n, to)
        return self.copy(self.down, self.rows(self.z, self.y_at(-way * (k - 1)), half), n, to)

    def start(self, maker, *args):
        for way in (1, -1):
            maker(*args[:-1], way, args[-1]).start()

    def wait(self, maker, *args):
        for way in (1, -1):
            maker(*args[:-1], way, args[-1], received=True).wait_recv()

    def both(self, act, d, k):
        for side in (-d, d):
            act(self.yg, side, k)

    def step(self, n):
        s, w = self.start, self.wait
        if n == 1:
            s(self.yd, 1)
            s(self.zg, 1)
            s(self.yg, 0, 1)
        if n == 3:
            w(self.yd, 1)
            s(self.yd, 2)
            w(self.zg, 1)
            s(self.zg, 2)
            self.both(s, 1, 1)
        if n == 4:
            w(self.yd, 2)
            s(self.zd, 1)
            w(self.yg, 0, 1)
            s(self.yg, 0, 2)
        if n == 5:
            w(self.zg, 2)
            s(self.zg, 3)
        if n == 6:
            self.both(s, 2, 1)
        if n == 7:
            self.both(w, 1, 1)
            self.both(s, 1, 2)
            w(self.zd, 1)
            s(self.zd, 2)
        if n == 8:
            w(self.zg, 3)
            s(self.zg, 4)
        if n == 15:
            self.both(s, 3, 1)
        if n == 9:
            self.both(w, 2, 1)
            self.both(s, 2, 2)
        if n == 10:
            w(self.zd, 2)
            s(self.zd, 3)
        if n == 11:
            w(self.zg, 4)
            s(self.yg, 4, 1)
        if n == 14:
            self.both(w, 3, 1)
            self.both(s, 3, 2)
        if n == 12:
            w(self.zd, 3)
            s(self.zd, 4)
        if n == 13:
            w(self.yg, 4, 1)
            s(self.yg, 4, 2)

    def gate_up_here(self):
        for d in (0, -1, 1, -2, 2, -3, 3, 4):
            self.wait(self.yg, d, 2)

    def down_here(self):
        self.wait(self.zd, 4)

    def drain(self):
        rows = self.gate_up.shape[0] - self.block
        all_sent(self.gate_up.at[0:rows], self.send.at[0])
        all_sent(self.down.at[0:rows], self.send.at[1])


WEIGHT_COPIES = 52


def layer_kernel(
    n_z,
    n_y,
    r_hbm,
    k_hbm,
    v_hbm,
    gate_hbm,
    fd_hbm,
    afl_hbm,
    foff_hbm,
    sd_hbm,
    soff_hbm,
    scale_hbm,
    skip_hbm,
    matrix_hbm,
    gain_hbm,
    switch_hbm,
    expand_hbm,
    contract_hbm,
    out_ref,
    stream_ref,
    r_ref,
    k_ref,
    v_ref,
    gate_ref,
    fd_ref,
    sd_ref,
    matrix_ref,
    afl_ref,
    foff_ref,
    soff_ref,
    scale_ref,
    skip_ref,
    gain_ref,
    load_sem,
    mask_ref,
    level_ref,
    local_ref,
    coef_ref,
    extra_ref,
    sm_ref,
    packet_y,
    recv_y,
    packet_z,
    recv_z,
    packet_in,
    recv_in,
    send_in_sem,
    recv_in_sem,
    send_y_sem,
    recv_y_sem,
    send_z_sem,
    recv_z_sem,
    gate_up_ref,
    down_ref,
    rows_ref,
    hidden_ref,
    weight_load_sem,
    weight_send,
    weight_recv,
    row_send,
    row_recv,
    side_send,
    side_recv,
    *ring_refs,
):
    length, width = r_ref.shape
    heads = width // C
    place_z = lax.axis_index("sp_0")
    place_y = lax.axis_index("sp_1")

    loads = [
        pltpu.make_async_copy(src, dst, load_sem.at[n])
        for n, (src, dst) in enumerate(
            (
                (r_hbm, r_ref),
                (k_hbm, k_ref),
                (v_hbm, v_ref),
                (fd_hbm, fd_ref),
                (sd_hbm, sd_ref),
                (afl_hbm, afl_ref),
                (foff_hbm, foff_ref),
                (soff_hbm, soff_ref),
                (scale_hbm, scale_ref),
                (gate_hbm, gate_ref),
                (matrix_hbm, matrix_ref),
                (skip_hbm, skip_ref),
                (gain_hbm, gain_ref),
            )
        )
    ]
    gather = WeightGather(gate_up_ref, down_ref, n_z, n_y, weight_send, weight_recv)
    own_rows = gather.rows(place_z, place_y)
    ff = down_ref.shape[1]
    weight_loads = [
        pltpu.make_async_copy(contract_hbm, down_ref.at[own_rows], weight_load_sem.at[0])
    ]
    for n in range(ff // 128):
        for m, src in enumerate((switch_hbm, expand_hbm)):
            weight_loads.append(
                pltpu.make_async_copy(
                    src.at[:, pl.ds(128 * n, 128)],
                    gate_up_ref.at[own_rows, pl.ds(256 * n + 128 * m, 128)],
                    weight_load_sem.at[1],
                )
            )
    for load in loads[:9] + weight_loads + loads[9:]:
        load.start()
    barrier = pltpu.get_barrier_semaphore()
    greet_ring(barrier)
    for d in range(1, n_y):
        pl.semaphore_signal(
            barrier, inc=1, device_id={"sp_1": lax.rem(place_y + d, n_y)}, device_id_type=MESH
        )
    for d in range(1, n_z):
        pl.semaphore_signal(
            barrier, inc=1, device_id={"sp_0": lax.rem(place_z + d, n_z)}, device_id_type=MESH
        )

    big_row = lax.broadcasted_iota(jnp.int32, (width, width), 0)
    big_col = lax.broadcasted_iota(jnp.int32, (width, width), 1)
    same_head = (big_row // C) == (big_col // C)
    mask_ref[...] = jnp.where(same_head, 1.0, 0.0).astype(BF16)

    t_idx = lax.broadcasted_iota(jnp.int32, (C, width), 0)
    lane = lax.broadcasted_iota(jnp.int32, (C, width), 1)
    j_idx = lane % C
    strict = j_idx < t_idx
    inclusive = j_idx <= t_idx
    pick = jnp.where(
        lax.broadcasted_iota(jnp.int32, (heads, width), 1) // C
        == lax.broadcasted_iota(jnp.int32, (heads, width), 0),
        1.0,
        0.0,
    ).astype(F32)
    eye = jnp.where(j_idx == t_idx, 1.0, 0.0).astype(F32)
    for n, b in enumerate(LEVELS):
        rb = (big_row % C) // b
        cb = (big_col % C) // b
        level_ref[n] = jnp.where(
            same_head & (rb % 2 == 1) & (cb == rb - 1), 1.0, 0.0
        ).astype(BF16)
    first_level = (t_idx % 2 == 1) & (j_idx == t_idx - 1)

    tri = jnp.where(
        (lax.broadcasted_iota(jnp.int32, (C, 2 * C), 1) % C)
        <= lax.broadcasted_iota(jnp.int32, (C, 2 * C), 0),
        1.0,
        0.0,
    ).astype(BF16)

    def tiled(x):
        return jnp.concatenate([x.astype(BF16)] * heads, axis=0)

    def bd(x):
        return tiled(x) * mask_ref[...]

    def bd2(x):
        return jnp.concatenate([x.astype(BF16)] * 2, axis=0) * mask_ref[0 : 2 * C, 0 : 2 * C]

    def paired(product, axis, a, x, y):
        outs = []
        for p in range(heads // 2):
            cols = slice(p * 2 * C, (p + 1) * 2 * C)
            right_side = jnp.concatenate([bd2(x[:, cols]), bd2(y[:, cols])], axis=axis)
            outs.append(product(a[:, cols], right_side))
        return (
            jnp.concatenate([o[:, : 2 * C] for o in outs], axis=1),
            jnp.concatenate([o[:, 2 * C :] for o in outs], axis=1),
        )

    def diagonal_of(full):
        out = full[0:C]
        for h in range(1, heads):
            out = jnp.where(lane >= h * C, full[h * C : (h + 1) * C], out)
        return out

    sm_ref[0:C, :] = jnp.zeros((C, width), F32)
    sm_ref[C:, :] = eye

    def chunk(c, added, result):
        rows = pl.ds(pl.multiple_of(c * C, C), C)
        r = r_ref[rows, :].astype(F32)
        k = k_ref[rows, :].astype(F32)
        vb = v_ref[rows, :]
        v = vb.astype(F32)
        log_step = added - EXP_HALF * jax.nn.sigmoid(foff_ref[...] + fd_ref[rows, :].astype(F32))
        rate = jax.nn.sigmoid(soff_ref[...] + sd_ref[rows, :].astype(F32))
        k_hi, k_lo = two_parts(k * k)
        d_hi, d_lo = two_parts(r * k * scale_ref[...])
        sums = dot_nn(jnp.concatenate([k_hi, k_lo, d_hi, d_lo], axis=0), mask_ref[...])
        l_hi, l_lo = two_parts(log_step)
        cum = dot_nn(tri, jnp.concatenate([l_hi, l_lo], axis=0))
        yield
        unit = k * lax.rsqrt(sums[0:C] + sums[C : 2 * C] + norm_eps)
        extra_ref[rows, :] = (sums[2 * C : 3 * C] + sums[3 * C :]) * v
        mid = cum[C // 2 - 1 : C // 2]
        end = cum[C - 1 : C]
        rel = cum - mid
        grow = jnp.exp(rel)
        shrink = jnp.exp(-rel)
        before_unit = jnp.exp(rel - log_step) * unit
        read_fwd = r * grow
        key_back = k * shrink
        erase_back = unit * rate * shrink
        grow_mid = jnp.exp(mid)
        grow_rest = jnp.exp(end - mid)
        grow_end = jnp.exp(end)
        left = jnp.concatenate([before_unit, read_fwd], axis=0).astype(BF16)
        by_key, by_erase = paired(dot_nt, 0, left, key_back, erase_back)
        yield
        key_both = jnp.concatenate(
            [jnp.where(strict, by_key[0:C], 0.0), jnp.where(inclusive, by_key[C:], 0.0)], axis=0
        ).astype(BF16)
        erase_past = jnp.where(strict, by_erase[0:C], 0.0)
        erase_read = jnp.where(inclusive, by_erase[C:], 0.0).astype(BF16)
        by_value = dot_nn(key_both, bd(vb))
        erase_tiled = tiled(erase_past)
        inv = eye - jnp.where(first_level, erase_past, 0.0)
        for n in range(len(LEVELS)):
            half = dot_nn(inv.astype(BF16), erase_tiled * level_ref[n])
            yield
            inv = inv - dot_nn(half.astype(BF16), bd(inv))
            yield
        inv_b = inv.astype(BF16)
        recalled, carried_map = paired(
            dot_nn, 1, inv_b, by_value[0:C], before_unit * grow_mid
        )
        yield
        recalled_b = recalled.astype(BF16)
        carried_b = carried_map.astype(BF16)
        local_less, start_less = paired(dot_nn, 1, erase_read, recalled_b, carried_b)
        local = by_value[C:] - local_less
        from_start = (read_fwd * grow_mid - start_less).astype(BF16)
        key_end = (key_back * grow_rest).astype(BF16)
        erase_end = (erase_back * grow_rest).astype(BF16)
        gain = dot_tn(
            jnp.concatenate([vb, -recalled_b], axis=0),
            jnp.concatenate([key_end, erase_end], axis=0),
        )
        loss = dot_tn(carried_b, erase_end)
        yield
        result.append(
            (rows, local, from_start, diagonal_of(gain), loss.astype(BF16) * mask_ref[...], grow_end)
        )

    def group(g, _):
        for n in (1, 3, 4, 5):

            @pl.when(g == n)
            def _():
                if n == 1:
                    weight_loads[0].wait()
                    all_sent(gate_up_ref.at[own_rows], weight_load_sem.at[1])
                    pl.semaphore_wait(barrier, n_y - 1 + n_z - 1 + 3)
                gather.step(n)

        added = dot_tn_exact(afl_ref[:, pl.ds(pl.multiple_of(g * C * TOGETHER, 128), C * TOGETHER)], pick)
        results = [[] for _ in range(TOGETHER)]
        running = [
            chunk(g * TOGETHER + n, added[n * C : (n + 1) * C], results[n]) for n in range(TOGETHER)
        ]
        while running:
            left_over = []
            for one in running:
                try:
                    next(one)
                    left_over.append(one)
                except StopIteration:
                    pass
            running = left_over
        sm = sm_ref[...]
        for n in range(TOGETHER):
            rows, local, from_start, gain, loss, grow_end = results[n][0]
            sm_b = sm.astype(BF16)
            from_state, coef = paired(dot_nt, 0, from_start, sm_b[0:C], sm_b[C:])
            local_ref[rows, :] = local + from_state
            coef_ref[rows, :] = coef.astype(BF16)
            sm = sm * grow_end - dot_nn(sm_b, loss)
            sm = jnp.concatenate([sm[0:C] + gain, sm[C:]], axis=0)
        sm_ref[...] = sm
        return 0

    for load in loads[:9]:
        load.wait()
    lax.fori_loop(0, length // (C * TOGETHER), group, 0)

    low = lax.broadcasted_iota(jnp.int32, (C, 2 * C), 1) < C

    def swapped(x):
        return jnp.concatenate([x[:, C:], x[:, :C]], axis=1)

    def map_of(packet):
        wide = packet.astype(F32)
        return jnp.concatenate(
            [jnp.where(low, swapped(wide), 0.0), jnp.where(low, 0.0, wide)], axis=0
        ).astype(BF16)

    def followed_by(before, packet):
        return dot_nn(before.astype(BF16), map_of(packet)) + jnp.where(low, packet.astype(F32), 0.0)

    sm = sm_ref[...]
    for h in range(heads):
        cols = slice(h * C, (h + 1) * C)
        packet_y[h] = jnp.concatenate([sm[0:C, cols], sm[C:, cols]], axis=1).astype(BF16)
    recv_y[place_y] = packet_y[place_y]

    def copy_y(to, slot):
        return pltpu.make_async_remote_copy(
            src_ref=packet_y.at[to],
            dst_ref=recv_y.at[slot],
            send_sem=send_y_sem.at[to],
            recv_sem=recv_y_sem.at[slot],
            device_id={"sp_1": to},
            device_id_type=MESH,
        )

    for d in range(1, n_y):
        copy_y(lax.rem(place_y + d, n_y), place_y).start()
    gather.step(6)
    for d in range(1, n_y):
        peer = lax.rem(place_y + n_y - d, n_y)
        copy_y(peer, peer).wait_recv()
    small_eye = jnp.where(
        lax.broadcasted_iota(jnp.int32, (C, 2 * C), 1)
        == lax.broadcasted_iota(jnp.int32, (C, 2 * C), 0) + C,
        1.0,
        0.0,
    ).astype(F32)
    insides = [small_eye, recv_y[0].astype(F32)]
    for m in range(1, n_y):
        insides.append(followed_by(insides[m], recv_y[m]))
    packet_z[...] = insides[n_y].astype(BF16)

    def copy_z(to, slot):
        return pltpu.make_async_remote_copy(
            src_ref=packet_z,
            dst_ref=recv_z.at[slot],
            send_sem=send_z_sem.at[to],
            recv_sem=recv_z_sem.at[slot],
            device_id={"sp_0": to},
            device_id_type=MESH,
        )

    for d in range(1, n_z):

        @pl.when(place_z + d < n_z)
        def _():
            copy_z(place_z + d, place_z).start()

    gather.step(7)
    gather.step(8)
    for m in range(n_z - 1):

        @pl.when(m < place_z)
        def _():
            copy_z(m, m).wait_recv()

        @pl.when(m >= place_z)
        def _():
            recv_z[m] = small_eye.astype(BF16)

    runs = [recv_z[m] for m in range(n_z - 1)]
    while len(runs) > 1:
        runs = [
            followed_by(runs[m], runs[m + 1]) if m + 1 < len(runs) else runs[m]
            for m in range(0, len(runs), 2)
        ]
    before = jnp.where(low, runs[0].astype(F32), 0.0).astype(BF16)
    for m in range(n_y):
        inside = insides[m]
        packet_in[m] = (dot_nn(before, map_of(inside)) + jnp.where(low, inside, 0.0)).astype(BF16)
    recv_in[place_y] = packet_in[place_y]

    def copy_in(to, slot):
        return pltpu.make_async_remote_copy(
            src_ref=packet_in.at[to],
            dst_ref=recv_in.at[slot],
            send_sem=send_in_sem.at[to],
            recv_sem=recv_in_sem.at[slot],
            device_id={"sp_1": to},
            device_id_type=MESH,
        )

    for d in range(1, n_y):
        copy_in(lax.rem(place_y + d, n_y), place_y).start()
    gather.step(15)
    for d in range(1, n_y):
        peer = lax.rem(place_y + n_y - d, n_y)
        copy_in(peer, peer).wait_recv()
    blocks = []
    for h in range(heads):
        state = recv_in[h].astype(F32)
        state = jnp.where(low, state, 0.0) if h % 2 == 0 else jnp.where(low, 0.0, swapped(state))
        empty = jnp.zeros((C, 2 * C), F32)
        blocks.append(
            jnp.concatenate([state if p == h // 2 else empty for p in range(heads // 2)], axis=1)
        )
    incoming_bd = jnp.concatenate(blocks, axis=0).astype(BF16)
    for load in loads[9:]:
        load.wait()

    span = 2 * PIECE
    rings = [RingSum(*ring_refs[9 * n : 9 * n + 5], ring_refs[9 * n + 5 : 9 * n + 9]) for n in range(2 * BATCHES)]
    chip, core, right, left, sibling = ring_places()
    here = pl.ds(pl.multiple_of(core * PIECE, PIECE), PIECE)
    there = pl.ds(pl.multiple_of((1 - core) * PIECE, PIECE), PIECE)

    def chip_at(d):
        return lax.rem(chip + d, 4)

    def produce(b, d):
        def taken(ref):
            first = chip_at(d) * (2 * ROWS) + b * PIECE
            return jnp.concatenate(
                [
                    ref[pl.ds(pl.multiple_of(first + n * ROWS, PIECE), PIECE), :].astype(F32)
                    for n in range(2)
                ],
                axis=0,
            )

        outcome = taken(local_ref) + dot_nt(taken(coef_ref).astype(BF16), incoming_bd)
        o_hi, o_lo = two_parts(outcome)
        centre = dot_nn(jnp.concatenate([o_hi, o_lo], axis=0), mask_ref[...])
        away = outcome - (centre[0:span] + centre[span:]) * (1.0 / C)
        a_hi, a_lo = two_parts(away * away)
        spread = dot_nn(jnp.concatenate([a_hi, a_lo], axis=0), mask_ref[...])
        spread = (spread[0:span] + spread[span:]) * (1.0 / C)
        normed = away * lax.rsqrt(spread + group_eps)
        mixed = ((normed + taken(extra_ref)) * taken(gate_ref)).astype(BF16)
        for h in range(2):
            for n in range(HALF // 256):
                rings[b].part[d, h, :, pl.ds(256 * n, 256)] = dot_nn(
                    mixed, matrix_ref[:, pl.ds(h * HALF + 256 * n, 256)]
                ).astype(BF16)
        rings[b].produced(d)

    def normed_rows(b):
        rows = pl.ds(b * PIECE, PIECE)
        squares = jnp.zeros((PIECE, 1), F32)
        for h in range(2):
            cols = pl.ds(h * HALF, HALF)
            stream = skip_ref[rows, cols].astype(F32) + rings[b].result(h)
            stream_ref[rows, cols] = stream
            squares = squares + jnp.sum(stream * stream, axis=1, keepdims=True)
        scale_rows = lax.rsqrt(squares * (1.0 / (2 * HALF)) + norm_eps)
        for h in range(2):
            cols = pl.ds(h * HALF, HALF)
            rows_ref[b, chip, h, here, :] = (
                stream_ref[rows, cols] * scale_rows * gain_ref[:, cols]
            ).astype(BF16)
        for n in range(4):
            hop(b, n).start()
        side(b, 0).start()
        side(b, 1).start()

    def hop(b, n):
        d, h, to = (
            (0, 0, right),
            (0, 1, left),
            (0, 1, right),
            (0, 0, left),
            (3, 0, right),
            (1, 1, left),
        )[n]
        block = rows_ref.at[b, chip_at(d), h, here, :]
        return remote(block, block, row_send.at[b], row_recv.at[b, n], to)

    def arrival(b, n):
        d, h = ((3, 0), (1, 1), (3, 1), (1, 0), (2, 0), (2, 1))[n]
        block = rows_ref.at[b, chip_at(d), h, here, :]
        return remote(block, block, row_send.at[b], row_recv.at[b, n], sibling)

    sides = ((0, 0), (0, 1), (1, 0), (1, 1), (3, 0), (3, 1), (2, 0), (2, 1))

    def side(b, n):
        d, h = sides[n]
        block = rows_ref.at[b, chip_at(d), h, here, :]
        return remote(block, block, side_send.at[b], side_recv.at[b, n], sibling)

    def side_arrival(b, n):
        d, h = sides[n]
        block = rows_ref.at[b, chip_at(d), h, there, :]
        return remote(block, block, side_send.at[b], side_recv.at[b, n], sibling)

    def relay_rows(b):
        arrival(b, 0).wait_recv()
        hop(b, 4).start()
        side(b, 4).start()
        arrival(b, 1).wait_recv()
        hop(b, 5).start()
        side(b, 3).start()

    def share_near(b):
        arrival(b, 2).wait_recv()
        side(b, 5).start()
        arrival(b, 3).wait_recv()
        side(b, 2).start()

    def share_far(b):
        arrival(b, 4).wait_recv()
        side(b, 6).start()
        arrival(b, 5).wait_recv()
        side(b, 7).start()

    def feed(*blocks):
        for b, d in blocks:
            for n in {0: (0, 1), 1: (2, 3), 3: (4, 5), 2: (6, 7)}[d]:
                side_arrival(b, n).wait_recv()
        x = [
            jnp.concatenate([rows_ref[b, chip_at(d), h] for b, d in blocks], axis=0)
            for h in range(2)
        ]
        filled = pl.ds(0, len(blocks) * span)
        for n in range(hidden_ref.shape[1] // 128):
            cols = pl.ds(256 * n, 256)
            both = dot_nn(x[0], gate_up_ref[0:HALF, cols]) + dot_nn(x[1], gate_up_ref[HALF:, cols])
            gate_act, up_act = both[:, :128], both[:, 128:]
            hidden_ref[filled, pl.ds(128 * n, 128)] = (
                gate_act * jax.nn.sigmoid(gate_act) * up_act
            ).astype(BF16)
        if blocks == ((0, 0),):
            gather.down_here()
        hidden = hidden_ref[filled, :]
        for h in range(2):
            for n in range(HALF // 256):
                product = dot_nt(hidden, down_ref[pl.ds(h * HALF + 256 * n, 256), :]).astype(BF16)
                for m, (b, d) in enumerate(blocks):
                    rings[BATCHES + b].part[d, h, :, pl.ds(256 * n, 256)] = product[
                        m * span : (m + 1) * span
                    ]
        for b, d in blocks:
            rings[BATCHES + b].produced(d)

    def finish(b):
        ring = rings[BATCHES + b]
        rows = pl.ds(b * PIECE, PIECE)
        ring.to_sibling(0).wait_recv()
        ring.arrive()
        for h in range(2):
            cols = pl.ds(h * HALF, HALF)
            out_ref[rows, cols] = (stream_ref[rows, cols] + half_step * ring.result(h)).astype(BF16)

    gather.step(9)
    produce(0, 2)
    produce(0, 1)
    rings[0].pass_on(2)
    gather.step(10)
    produce(0, 3)
    rings[0].pass_on(1)
    produce(0, 0)
    rings[0].pass_on(3)
    produce(1, 2)
    gather.step(11)
    produce(1, 1)
    rings[1].pass_on(2)
    produce(1, 3)
    gather.step(14)
    rings[0].pass_relayed()
    rings[1].pass_on(1)
    produce(1, 0)
    rings[1].pass_on(3)
    rings[1].pass_relayed()
    rings[0].to_sibling(0).wait_recv()
    rings[0].arrive()
    normed_rows(0)
    gather.step(12)
    gather.step(13)
    rings[1].to_sibling(0).wait_recv()
    rings[1].arrive()
    normed_rows(1)
    gather.gate_up_here()
    feed((0, 0))
    relay_rows(0)
    share_near(0)
    feed((1, 0))
    relay_rows(1)
    feed((0, 3), (0, 1))
    share_far(0)
    share_near(1)
    rings[2].pass_on(3)
    rings[2].pass_on(1)
    feed((0, 2))
    share_far(1)
    rings[2].pass_on(2)
    feed((1, 2))
    rings[3].pass_on(2)
    rings[2].pass_relayed()
    feed((1, 3), (1, 1))
    rings[3].pass_on(3)
    rings[3].pass_on(1)
    rings[3].pass_relayed()
    finish(0)
    finish(1)
    for ring in rings:
        ring.drain()
    for b in range(BATCHES):
        all_sent(rows_ref.at[b, 0:3, :, 0:PIECE, :], row_send.at[b])
        all_sent(rows_ref.at[b, :, :, 0:PIECE, :], side_send.at[b])
    gather.drain()
    for d in range(1, n_y):
        to = lax.rem(place_y + d, n_y)
        copy_y(to, to).wait_send()
        copy_in(to, to).wait_send()
    for d in range(1, n_z):

        @pl.when(place_z + d < n_z)
        def _():
            copy_z(place_z + d, place_z).wait_send()


def layer(r, k, v, gate, fd, afl, foff, sd, soff, scale, skip, matrix, gain, switch, expand, contract):
    n_z, n_y = lax.axis_size("sp_0"), lax.axis_size("sp_1")
    length, width = r.shape
    ff = switch.shape[1]
    depth = switch.shape[0] * n_z * n_y
    vmem = pl.BlockSpec(memory_space=pltpu.VMEM)
    hbm = pl.BlockSpec(memory_space=pl.ANY)
    dma = pltpu.SemaphoreType.DMA
    return pl.pallas_call(
        functools.partial(layer_kernel, n_z, n_y),
        out_shape=jax.ShapeDtypeStruct((ROWS, 2 * HALF), BF16),
        in_specs=[hbm] * 16,
        out_specs=vmem,
        scratch_shapes=[pltpu.VMEM((ROWS, 2 * HALF), F32)]
        + [pltpu.VMEM((length, width), BF16)] * 6
        + [
            pltpu.VMEM((width, 2 * HALF), BF16),
            pltpu.VMEM((width // C, length), F32),
            pltpu.VMEM((1, width), F32),
            pltpu.VMEM((1, width), F32),
            pltpu.VMEM((1, width), F32),
            pltpu.VMEM((ROWS, 2 * HALF), BF16),
            pltpu.VMEM((1, 2 * HALF), F32),
            dma((13,)),
            pltpu.VMEM((width, width), BF16),
            pltpu.VMEM((len(LEVELS), width, width), BF16),
            pltpu.VMEM((length, width), F32),
            pltpu.VMEM((length, width), BF16),
            pltpu.VMEM((length, width), F32),
            pltpu.VMEM((2 * C, width), F32),
            pltpu.VMEM((n_y, C, 2 * C), BF16),
            pltpu.VMEM((n_y, C, 2 * C), BF16),
            pltpu.VMEM((C, 2 * C), BF16),
            pltpu.VMEM((n_z, C, 2 * C), BF16),
            pltpu.VMEM((n_y, C, 2 * C), BF16),
            pltpu.VMEM((n_y, C, 2 * C), BF16),
            dma((n_y,)),
            dma((n_y,)),
            dma((n_y,)),
            dma((n_y,)),
            dma((n_z,)),
            dma((n_z,)),
            pltpu.VMEM((depth, 2 * ff), BF16),
            pltpu.VMEM((depth, ff), BF16),
            pltpu.VMEM((BATCHES, 4, 2, 2 * PIECE, HALF), BF16),
            pltpu.VMEM((4 * PIECE, ff), BF16),
            dma((2,)),
            dma((2,)),
            dma((WEIGHT_COPIES,)),
            dma((BATCHES,)),
            dma((BATCHES, 6)),
            dma((BATCHES,)),
            dma((BATCHES, 8)),
        ]
        + RING_SUM_SCRATCH * (2 * BATCHES),
        compiler_params=pltpu.CompilerParams(
            collective_id=0, has_side_effects=True, vmem_limit_bytes=60 * 1024 * 1024
        ),
        cost_estimate=pl.CostEstimate(
            flops=40_000_000_000, bytes_accessed=8_000_000, transcendentals=0
        ),
        name="layer",
    )(
        r, k, v, gate, fd, afl.T, foff[None, :], sd, soff[None, :], scale[None, :], skip, matrix,
        gain[None, :], switch, expand, contract,
    )


def per_device(
    skip_stream,
    acceptance_signal,
    lookup_mapped,
    payload_mapped,
    result_switch,
    forget_dynamic_share,
    additive_forget_logarithm,
    forget_feature_offset,
    substitution_dynamic_share,
    substitution_feature_offset,
    diagonal_reward_scales,
    result_matrix,
    mlp_rescaler,
    switch_matrix,
    expand_matrix,
    contract_matrix,
):
    return layer(
        acceptance_signal,
        lookup_mapped,
        payload_mapped,
        result_switch,
        forget_dynamic_share,
        additive_forget_logarithm,
        forget_feature_offset,
        substitution_dynamic_share,
        substitution_feature_offset,
        diagonal_reward_scales,
        skip_stream,
        result_matrix,
        mlp_rescaler,
        switch_matrix,
        expand_matrix,
        contract_matrix,
    )


def solution(mesh):
    torus = Mesh(mesh.devices.reshape(8, 4, mesh.shape["tp"]), ("sp_0", "sp_1", "tp"))
    in_specs = (
        P(SP_TP, None),
        P(SP, "tp"),
        P(SP, "tp"),
        P(SP, "tp"),
        P(SP, "tp"),
        P(SP, "tp"),
        P(SP, "tp"),
        P("tp"),
        P(SP, "tp"),
        P("tp"),
        P("tp"),
        P("tp", None),
        P(),
        P(SP, "tp"),
        P(SP, "tp"),
        P(SP, "tp"),
    )
    out_specs = P(SP_TP, None)
    return jax.shard_map(
        per_device, mesh=torus, in_specs=in_specs, out_specs=out_specs, check_vma=False
    )
```

```python
import functools

import jax
import jax.numpy as jnp
from jax import lax
from jax.experimental import pallas as pl
from jax.experimental.pallas import tpu as pltpu
from jax.sharding import Mesh
from jax.sharding import PartitionSpec as P

PER_GROUP_DIMS = 64
SP = ("sp_0", "sp_1")
SP_TP = ("sp_0", "sp_1", "tp")
MESH = pl.DeviceIdType.MESH

norm_eps = 1e-06
group_eps = 0.00064
half_step = 0.5
EXP_HALF = 0.6065306597126334

C = 64
TOGETHER = 2
LEVELS = (2, 4, 8, 16, 32)
F32 = jnp.float32
BF16 = jnp.bfloat16


def dot_nn(a, b):
    return lax.dot_general(a, b, (((1,), (0,)), ((), ())), preferred_element_type=F32)


def dot_nt(a, b):
    return lax.dot_general(a, b, (((1,), (1,)), ((), ())), preferred_element_type=F32)


def dot_tn(a, b):
    return lax.dot_general(a, b, (((0,), (0,)), ((), ())), preferred_element_type=F32)


def dot_tn_exact(a, b):
    return lax.dot_general(
        a,
        b,
        (((0,), (0,)), ((), ())),
        precision=lax.Precision.HIGHEST,
        preferred_element_type=F32,
    )


def two_parts(x):
    high = x.astype(BF16)
    return high, (x - high.astype(F32)).astype(BF16)


ROWS = 96
BATCHES = 2
PIECE = ROWS // BATCHES
HALF = 1024


def ring_places():
    tp = lax.axis_index("tp")
    chip, core = tp // 2, tp % 2
    right = lax.rem(chip + 1, 4) * 2 + core
    left = lax.rem(chip + 3, 4) * 2 + core
    sibling = chip * 2 + 1 - core
    return chip, core, right, left, sibling


def remote(src, dst, send_sem, recv_sem, to):
    return pltpu.make_async_remote_copy(
        src_ref=src,
        dst_ref=dst,
        send_sem=send_sem,
        recv_sem=recv_sem,
        device_id={"tp": to},
        device_id_type=MESH,
    )


def all_moved(ref, sem):
    pltpu.make_async_copy(ref, ref, sem).wait()


class RingSum:
    def __init__(self, part, sib, pair, relay, arrived, sems):
        self.part, self.sib, self.pair, self.relay, self.arrived = part, sib, pair, relay, arrived
        self.sib_send, self.sib_recv, self.send, self.recv = sems
        self.chip, self.core, self.right, self.left, self.sibling = ring_places()
        self.own = pl.ds(pl.multiple_of(self.core * PIECE, PIECE), PIECE)
        self.other = pl.ds(pl.multiple_of((1 - self.core) * PIECE, PIECE), PIECE)

    def to_sibling(self, d):
        return remote(
            self.part.at[d, :, self.other, :],
            self.sib.at[d],
            self.sib_send.at[0],
            self.sib_recv.at[d],
            self.sibling,
        )

    def hop(self, n):
        src, dst, to = (
            (self.pair.at[2, 0], self.relay.at[0], self.right),
            (self.pair.at[2, 1], self.relay.at[1], self.left),
            (self.pair.at[1, 1], self.arrived.at[0, 1], self.right),
            (self.pair.at[3, 0], self.arrived.at[1, 0], self.left),
            (self.pair.at[1, 0], self.arrived.at[0, 0], self.right),
            (self.pair.at[3, 1], self.arrived.at[1, 1], self.left),
        )[n]
        return remote(src, dst, self.send.at[0], self.recv.at[min(n, 2)], to)

    def produced(self, d):
        self.to_sibling(d).start()

    def summed(self, d, h):
        return self.part[d, h, self.own, :].astype(F32) + self.sib[d, h].astype(F32)

    def pass_on(self, d):
        self.to_sibling(d).wait_recv()
        if d == 2:
            self.pair[2, 0] = self.summed(2, 0).astype(BF16)
            self.hop(0).start()
            self.pair[2, 1] = self.summed(2, 1).astype(BF16)
            self.hop(1).start()
        if d == 1:
            self.pair[1, 1] = self.summed(1, 1).astype(BF16)
            self.hop(2).start()
        if d == 3:
            self.pair[3, 0] = self.summed(3, 0).astype(BF16)
            self.hop(3).start()

    def pass_relayed(self):
        self.hop(0).wait_recv()
        self.pair[1, 0] = (self.summed(1, 0) + self.relay[0].astype(F32)).astype(BF16)
        self.hop(4).start()
        self.hop(1).wait_recv()
        self.pair[3, 1] = (self.summed(3, 1) + self.relay[1].astype(F32)).astype(BF16)
        self.hop(5).start()

    def arrive(self):
        all_moved(self.arrived, self.recv.at[2])

    def result(self, h):
        return (
            self.summed(0, h)
            + self.arrived[0, h].astype(F32)
            + self.arrived[1, h].astype(F32)
        )

    def drain(self):
        all_moved(self.sib, self.sib_send.at[0])
        all_moved(self.pair.at[0:3], self.send.at[0])


RING_SUM_SCRATCH = [
    pltpu.VMEM((4, 2, 2 * PIECE, HALF), BF16),
    pltpu.VMEM((4, 2, PIECE, HALF), BF16),
    pltpu.VMEM((4, 2, PIECE, HALF), BF16),
    pltpu.VMEM((2, PIECE, HALF), BF16),
    pltpu.VMEM((2, 2, PIECE, HALF), BF16),
    pltpu.SemaphoreType.DMA((1,)),
    pltpu.SemaphoreType.DMA((4,)),
    pltpu.SemaphoreType.DMA((1,)),
    pltpu.SemaphoreType.DMA((3,)),
]


def greet_ring(barrier):
    _, _, right, left, sibling = ring_places()
    for to in (right, left, sibling):
        pl.semaphore_signal(barrier, inc=1, device_id={"tp": to}, device_id_type=MESH)


class WeightGather:
    def __init__(self, gate_up, down, n_z, n_y, send, recv):
        self.gate_up, self.down, self.n_z, self.n_y = gate_up, down, n_z, n_y
        self.send, self.recv = send, recv
        self.z, self.y = lax.axis_index("sp_0"), lax.axis_index("sp_1")
        self.block = gate_up.shape[0] // (n_z * n_y)

    def z_at(self, d):
        return lax.rem(self.z + d + self.n_z, self.n_z)

    def y_at(self, d):
        return lax.rem(self.y + d + self.n_y, self.n_y)

    def rows(self, z, y, way=None):
        start = (z * self.n_y + y) * self.block
        if way is None:
            return pl.ds(pl.multiple_of(start, 32), self.block)
        half = self.block // 2
        return pl.ds(pl.multiple_of(start + (0 if way > 0 else half), 32), half)

    def group(self, z, way=None):
        size = self.n_y * self.block
        if way is None:
            return pl.ds(pl.multiple_of(z * size, 32), size)
        half = size // 2
        return pl.ds(pl.multiple_of(z * size + (0 if way > 0 else half), 32), half)

    def copy(self, ref, rows, n, device):
        return pltpu.make_async_remote_copy(
            src_ref=ref.at[rows],
            dst_ref=ref.at[rows],
            send_sem=self.send.at[0 if ref is self.gate_up else 1],
            recv_sem=self.recv.at[n],
            device_id=device,
            device_id_type=MESH,
        )

    def zg(self, way, k, received=False):
        n = (k - 1) * 2 + (way < 0)
        half = way if k == self.n_z // 2 else None
        to = {"sp_0": self.z_at(way)}
        if received:
            return self.copy(self.gate_up, self.rows(self.z_at(-way * k), self.y, half), n, to)
        return self.copy(self.gate_up, self.rows(self.z_at(-way * (k - 1)), self.y, half), n, to)

    def zd(self, way, k, received=False):
        n = 8 + (k - 1) * 2 + (way < 0)
        half = way if k == self.n_z // 2 else None
        to = {"sp_0": self.z_at(way)}
        if received:
            return self.copy(self.down, self.group(self.z_at(-way * k), half), n, to)
        return self.copy(self.down, self.group(self.z_at(-way * (k - 1)), half), n, to)

    def yg(self, d, way, k, received=False):
        n = 16 + (d + 3) * 2 + (way < 0) if k == 1 else 36
        half = way if k == 2 else None
        z = self.z_at(d)
        to = {"sp_1": self.y_at(way)}
        if received:
            return self.copy(self.gate_up, self.rows(z, self.y_at(-way * k), half), n, to)
        return self.copy(self.gate_up, self.rows(z, self.y_at(-way * (k - 1)), half), n, to)

    def yd(self, way, k, received=False):
        n = 32 + (k - 1) * 2 + (way < 0)
        half = way if k == 2 else None
        to = {"sp_1": self.y_at(way)}
        if received:
            return self.copy(self.down, self.rows(self.z, self.y_at(-way * k), half), n, to)
        return self.copy(self.down, self.rows(self.z, self.y_at(-way * (k - 1)), half), n, to)

    def start(self, maker, *args):
        for way in (1, -1):
            maker(*args[:-1], way, args[-1]).start()

    def wait(self, maker, *args):
        for way in (1, -1):
            maker(*args[:-1], way, args[-1], received=True).wait_recv()

    def both(self, act, d, k):
        for side in (-d, d):
            act(self.yg, side, k)

    def step(self, n):
        s, w = self.start, self.wait
        if n == 1:
            s(self.yd, 1)
            s(self.zg, 1)
            s(self.yg, 0, 1)
        if n == 3:
            w(self.yd, 1)
            s(self.yd, 2)
            w(self.zg, 1)
            s(self.zg, 2)
            self.both(s, 1, 1)
        if n == 4:
            w(self.yd, 2)
            s(self.zd, 1)
            w(self.yg, 0, 1)
            s(self.yg, 0, 2)
        if n == 5:
            w(self.zg, 2)
            s(self.zg, 3)
        if n == 6:
            self.both(s, 2, 1)
        if n == 7:
            self.both(w, 1, 1)
            self.both(s, 1, 2)
            w(self.zd, 1)
            s(self.zd, 2)
        if n == 8:
            w(self.zg, 3)
            s(self.zg, 4)
        if n == 15:
            self.both(s, 3, 1)
        if n == 9:
            self.both(w, 2, 1)
            self.both(s, 2, 2)
        if n == 10:
            w(self.zd, 2)
            s(self.zd, 3)
        if n == 11:
            w(self.zg, 4)
            s(self.yg, 4, 1)
        if n == 14:
            self.both(w, 3, 1)
            self.both(s, 3, 2)
        if n == 12:
            w(self.zd, 3)
            s(self.zd, 4)
        if n == 13:
            w(self.yg, 4, 1)
            s(self.yg, 4, 2)

    def gate_up_here(self):
        all_moved(self.gate_up.at[0 : self.n_z * self.block], self.recv.at[36])

    def down_here(self):
        self.wait(self.zd, 4)

    def drain(self):
        rows = self.gate_up.shape[0] - self.block
        all_moved(self.gate_up.at[0:rows], self.send.at[0])
        all_moved(self.down.at[0:rows], self.send.at[1])


WEIGHT_ARRIVALS = 37


def layer_kernel(
    n_z,
    n_y,
    r_hbm,
    k_hbm,
    v_hbm,
    gate_hbm,
    fd_hbm,
    afl_hbm,
    foff_hbm,
    sd_hbm,
    soff_hbm,
    scale_hbm,
    skip_hbm,
    matrix_hbm,
    gain_hbm,
    switch_hbm,
    expand_hbm,
    contract_hbm,
    out_ref,
    stream_ref,
    r_ref,
    k_ref,
    v_ref,
    gate_ref,
    fd_ref,
    sd_ref,
    matrix_ref,
    afl_ref,
    foff_ref,
    soff_ref,
    scale_ref,
    skip_ref,
    gain_ref,
    load_sem,
    mask_ref,
    level_ref,
    local_ref,
    coef_ref,
    extra_ref,
    sm_ref,
    packet_y,
    recv_y,
    packet_z,
    recv_z,
    packet_in,
    recv_in,
    send_in_sem,
    recv_in_sem,
    send_y_sem,
    recv_y_sem,
    send_z_sem,
    recv_z_sem,
    gate_up_ref,
    down_ref,
    rows_ref,
    hidden_ref,
    weight_load_sem,
    weight_send,
    weight_recv,
    row_send,
    row_recv,
    side_send,
    side_recv,
    *ring_refs,
):
    length, width = r_ref.shape
    heads = width // C
    place_z = lax.axis_index("sp_0")
    place_y = lax.axis_index("sp_1")

    loads = [
        pltpu.make_async_copy(src, dst, load_sem.at[n])
        for n, (src, dst) in enumerate(
            (
                (r_hbm, r_ref),
                (k_hbm, k_ref),
                (v_hbm, v_ref),
                (fd_hbm, fd_ref),
                (sd_hbm, sd_ref),
                (afl_hbm, afl_ref),
                (foff_hbm, foff_ref),
                (soff_hbm, soff_ref),
                (scale_hbm, scale_ref),
                (gate_hbm, gate_ref),
                (matrix_hbm, matrix_ref),
                (skip_hbm, skip_ref),
                (gain_hbm, gain_ref),
            )
        )
    ]
    gather = WeightGather(gate_up_ref, down_ref, n_z, n_y, weight_send, weight_recv)
    own_rows = gather.rows(place_z, place_y)
    ff = down_ref.shape[1]
    weight_loads = [
        pltpu.make_async_copy(contract_hbm, down_ref.at[own_rows], weight_load_sem.at[0])
    ]
    for n in range(ff // 128):
        for m, src in enumerate((switch_hbm, expand_hbm)):
            weight_loads.append(
                pltpu.make_async_copy(
                    src.at[:, pl.ds(128 * n, 128)],
                    gate_up_ref.at[own_rows, pl.ds(256 * n + 128 * m, 128)],
                    weight_load_sem.at[1],
                )
            )
    for load in loads[:9] + weight_loads + loads[9:]:
        load.start()
    barrier = pltpu.get_barrier_semaphore()
    greet_ring(barrier)
    for d in range(1, n_y):
        pl.semaphore_signal(
            barrier, inc=1, device_id={"sp_1": lax.rem(place_y + d, n_y)}, device_id_type=MESH
        )
    for d in range(1, n_z):
        pl.semaphore_signal(
            barrier, inc=1, device_id={"sp_0": lax.rem(place_z + d, n_z)}, device_id_type=MESH
        )

    big_row = lax.broadcasted_iota(jnp.int32, (width, width), 0)
    big_col = lax.broadcasted_iota(jnp.int32, (width, width), 1)
    same_head = (big_row // C) == (big_col // C)
    mask_ref[...] = jnp.where(same_head, 1.0, 0.0).astype(BF16)

    t_idx = lax.broadcasted_iota(jnp.int32, (C, width), 0)
    lane = lax.broadcasted_iota(jnp.int32, (C, width), 1)
    j_idx = lane % C
    strict = j_idx < t_idx
    inclusive = j_idx <= t_idx
    pick = jnp.where(
        lax.broadcasted_iota(jnp.int32, (heads, width), 1) // C
        == lax.broadcasted_iota(jnp.int32, (heads, width), 0),
        1.0,
        0.0,
    ).astype(F32)
    eye = jnp.where(j_idx == t_idx, 1.0, 0.0).astype(F32)
    for n, b in enumerate(LEVELS):
        rb = (big_row % C) // b
        cb = (big_col % C) // b
        level_ref[n] = jnp.where(
            same_head & (rb % 2 == 1) & (cb == rb - 1), 1.0, 0.0
        ).astype(BF16)
    first_level = (t_idx % 2 == 1) & (j_idx == t_idx - 1)

    tri = jnp.where(
        (lax.broadcasted_iota(jnp.int32, (C, 2 * C), 1) % C)
        <= lax.broadcasted_iota(jnp.int32, (C, 2 * C), 0),
        1.0,
        0.0,
    ).astype(BF16)

    def tiled(x):
        return jnp.concatenate([x.astype(BF16)] * heads, axis=0)

    def bd(x):
        return tiled(x) * mask_ref[...]

    def bd2(x):
        return jnp.concatenate([x.astype(BF16)] * 2, axis=0) * mask_ref[0 : 2 * C, 0 : 2 * C]

    def paired(product, axis, a, x, y):
        outs = []
        for p in range(heads // 2):
            cols = slice(p * 2 * C, (p + 1) * 2 * C)
            right_side = jnp.concatenate([bd2(x[:, cols]), bd2(y[:, cols])], axis=axis)
            outs.append(product(a[:, cols], right_side))
        return (
            jnp.concatenate([o[:, : 2 * C] for o in outs], axis=1),
            jnp.concatenate([o[:, 2 * C :] for o in outs], axis=1),
        )

    def diagonal_of(full):
        out = full[0:C]
        for h in range(1, heads):
            out = jnp.where(lane >= h * C, full[h * C : (h + 1) * C], out)
        return out

    sm_ref[0:C, :] = jnp.zeros((C, width), F32)
    sm_ref[C:, :] = eye

    def chunk(c, added, result):
        rows = pl.ds(pl.multiple_of(c * C, C), C)
        r = r_ref[rows, :].astype(F32)
        k = k_ref[rows, :].astype(F32)
        vb = v_ref[rows, :]
        v = vb.astype(F32)
        log_step = added - EXP_HALF * jax.nn.sigmoid(foff_ref[...] + fd_ref[rows, :].astype(F32))
        rate = jax.nn.sigmoid(soff_ref[...] + sd_ref[rows, :].astype(F32))
        k_hi, k_lo = two_parts(k * k)
        d_hi, d_lo = two_parts(r * k * scale_ref[...])
        sums = dot_nn(jnp.concatenate([k_hi, k_lo, d_hi, d_lo], axis=0), mask_ref[...])
        l_hi, l_lo = two_parts(log_step)
        cum = dot_nn(tri, jnp.concatenate([l_hi, l_lo], axis=0))
        yield
        unit = k * lax.rsqrt(sums[0:C] + sums[C : 2 * C] + norm_eps)
        extra_ref[rows, :] = (sums[2 * C : 3 * C] + sums[3 * C :]) * v
        mid = cum[C // 2 - 1 : C // 2]
        end = cum[C - 1 : C]
        rel = cum - mid
        grow = jnp.exp(rel)
        shrink = jnp.exp(-rel)
        before_unit = jnp.exp(rel - log_step) * unit
        read_fwd = r * grow
        key_back = k * shrink
        erase_back = unit * rate * shrink
        grow_mid = jnp.exp(mid)
        grow_rest = jnp.exp(end - mid)
        grow_end = jnp.exp(end)
        left = jnp.concatenate([before_unit, read_fwd], axis=0).astype(BF16)
        by_key, by_erase = paired(dot_nt, 0, left, key_back, erase_back)
        yield
        key_both = jnp.concatenate(
            [jnp.where(strict, by_key[0:C], 0.0), jnp.where(inclusive, by_key[C:], 0.0)], axis=0
        ).astype(BF16)
        erase_past = jnp.where(strict, by_erase[0:C], 0.0)
        erase_read = jnp.where(inclusive, by_erase[C:], 0.0).astype(BF16)
        by_value = dot_nn(key_both, bd(vb))
        erase_tiled = tiled(erase_past)
        inv = eye - jnp.where(first_level, erase_past, 0.0)
        for n in range(len(LEVELS)):
            half = dot_nn(inv.astype(BF16), erase_tiled * level_ref[n])
            yield
            inv = inv - dot_nn(half.astype(BF16), bd(inv))
            yield
        inv_b = inv.astype(BF16)
        recalled, carried_map = paired(
            dot_nn, 1, inv_b, by_value[0:C], before_unit * grow_mid
        )
        yield
        recalled_b = recalled.astype(BF16)
        carried_b = carried_map.astype(BF16)
        local_less, start_less = paired(dot_nn, 1, erase_read, recalled_b, carried_b)
        local = by_value[C:] - local_less
        from_start = (read_fwd * grow_mid - start_less).astype(BF16)
        key_end = (key_back * grow_rest).astype(BF16)
        erase_end = (erase_back * grow_rest).astype(BF16)
        gain = dot_tn(
            jnp.concatenate([vb, -recalled_b], axis=0),
            jnp.concatenate([key_end, erase_end], axis=0),
        )
        loss = dot_tn(carried_b, erase_end)
        yield
        result.append(
            (rows, local, from_start, diagonal_of(gain), loss.astype(BF16) * mask_ref[...], grow_end)
        )

    def group(g, _):
        for n in (1, 3, 4, 5):

            @pl.when(g == n)
            def _():
                if n == 1:
                    weight_loads[0].wait()
                    all_moved(gate_up_ref.at[own_rows], weight_load_sem.at[1])
                    pl.semaphore_wait(barrier, n_y - 1 + n_z - 1 + 3)
                gather.step(n)

        added = dot_tn_exact(afl_ref[:, pl.ds(pl.multiple_of(g * C * TOGETHER, 128), C * TOGETHER)], pick)
        results = [[] for _ in range(TOGETHER)]
        running = [
            chunk(g * TOGETHER + n, added[n * C : (n + 1) * C], results[n]) for n in range(TOGETHER)
        ]
        while running:
            left_over = []
            for one in running:
                try:
                    next(one)
                    left_over.append(one)
                except StopIteration:
                    pass
            running = left_over
        sm = sm_ref[...]
        for n in range(TOGETHER):
            rows, local, from_start, gain, loss, grow_end = results[n][0]
            sm_b = sm.astype(BF16)
            from_state, coef = paired(dot_nt, 0, from_start, sm_b[0:C], sm_b[C:])
            local_ref[rows, :] = local + from_state
            coef_ref[rows, :] = coef.astype(BF16)
            sm = sm * grow_end - dot_nn(sm_b, loss)
            sm = jnp.concatenate([sm[0:C] + gain, sm[C:]], axis=0)
        sm_ref[...] = sm
        return 0

    for load in loads[:9]:
        load.wait()
    lax.fori_loop(0, length // (C * TOGETHER), group, 0)

    low = lax.broadcasted_iota(jnp.int32, (C, 2 * C), 1) < C

    def swapped(x):
        return jnp.concatenate([x[:, C:], x[:, :C]], axis=1)

    def map_of(packet):
        wide = packet.astype(F32)
        return jnp.concatenate(
            [jnp.where(low, swapped(wide), 0.0), jnp.where(low, 0.0, wide)], axis=0
        ).astype(BF16)

    def followed_by(before, packet):
        return dot_nn(before.astype(BF16), map_of(packet)) + jnp.where(low, packet.astype(F32), 0.0)

    sm = sm_ref[...]
    for h in range(heads):
        cols = slice(h * C, (h + 1) * C)
        packet_y[h] = jnp.concatenate([sm[0:C, cols], sm[C:, cols]], axis=1).astype(BF16)
    recv_y[place_y] = packet_y[place_y]

    def copy_y(to, slot):
        return pltpu.make_async_remote_copy(
            src_ref=packet_y.at[to],
            dst_ref=recv_y.at[slot],
            send_sem=send_y_sem.at[to],
            recv_sem=recv_y_sem.at[slot],
            device_id={"sp_1": to},
            device_id_type=MESH,
        )

    for d in range(1, n_y):
        copy_y(lax.rem(place_y + d, n_y), place_y).start()
    gather.step(6)
    for d in range(1, n_y):
        peer = lax.rem(place_y + n_y - d, n_y)
        copy_y(peer, peer).wait_recv()
    small_eye = jnp.where(
        lax.broadcasted_iota(jnp.int32, (C, 2 * C), 1)
        == lax.broadcasted_iota(jnp.int32, (C, 2 * C), 0) + C,
        1.0,
        0.0,
    ).astype(F32)
    insides = [small_eye, recv_y[0].astype(F32)]
    for m in range(1, n_y):
        insides.append(followed_by(insides[m], recv_y[m]))
    packet_z[...] = insides[n_y].astype(BF16)

    def copy_z(to, slot):
        return pltpu.make_async_remote_copy(
            src_ref=packet_z,
            dst_ref=recv_z.at[slot],
            send_sem=send_z_sem.at[to],
            recv_sem=recv_z_sem.at[slot],
            device_id={"sp_0": to},
            device_id_type=MESH,
        )

    for d in range(1, n_z):

        @pl.when(place_z + d < n_z)
        def _():
            copy_z(place_z + d, place_z).start()

    gather.step(7)
    gather.step(8)
    for m in range(n_z - 1):

        @pl.when(m < place_z)
        def _():
            copy_z(m, m).wait_recv()

        @pl.when(m >= place_z)
        def _():
            recv_z[m] = small_eye.astype(BF16)

    runs = [recv_z[m] for m in range(n_z - 1)]
    while len(runs) > 1:
        runs = [
            followed_by(runs[m], runs[m + 1]) if m + 1 < len(runs) else runs[m]
            for m in range(0, len(runs), 2)
        ]
    before = jnp.where(low, runs[0].astype(F32), 0.0).astype(BF16)
    for m in range(n_y):
        inside = insides[m]
        packet_in[m] = (dot_nn(before, map_of(inside)) + jnp.where(low, inside, 0.0)).astype(BF16)
    recv_in[place_y] = packet_in[place_y]

    def copy_in(to, slot):
        return pltpu.make_async_remote_copy(
            src_ref=packet_in.at[to],
            dst_ref=recv_in.at[slot],
            send_sem=send_in_sem.at[to],
            recv_sem=recv_in_sem.at[slot],
            device_id={"sp_1": to},
            device_id_type=MESH,
        )

    for d in range(1, n_y):
        copy_in(lax.rem(place_y + d, n_y), place_y).start()
    gather.step(15)
    for d in range(1, n_y):
        peer = lax.rem(place_y + n_y - d, n_y)
        copy_in(peer, peer).wait_recv()
    blocks = []
    for h in range(heads):
        state = recv_in[h].astype(F32)
        state = jnp.where(low, state, 0.0) if h % 2 == 0 else jnp.where(low, 0.0, swapped(state))
        empty = jnp.zeros((C, 2 * C), F32)
        blocks.append(
            jnp.concatenate([state if p == h // 2 else empty for p in range(heads // 2)], axis=1)
        )
    incoming_bd = jnp.concatenate(blocks, axis=0).astype(BF16)
    for load in loads[9:]:
        load.wait()

    span = 2 * PIECE
    rings = [RingSum(*ring_refs[9 * n : 9 * n + 5], ring_refs[9 * n + 5 : 9 * n + 9]) for n in range(2 * BATCHES)]
    chip, core, right, left, sibling = ring_places()
    here = pl.ds(pl.multiple_of(core * PIECE, PIECE), PIECE)
    there = pl.ds(pl.multiple_of((1 - core) * PIECE, PIECE), PIECE)

    def chip_at(d):
        return lax.rem(chip + d, 4)

    def produce(b, d):
        def taken(ref):
            first = chip_at(d) * (2 * ROWS) + b * PIECE
            return jnp.concatenate(
                [
                    ref[pl.ds(pl.multiple_of(first + n * ROWS, PIECE), PIECE), :].astype(F32)
                    for n in range(2)
                ],
                axis=0,
            )

        outcome = taken(local_ref) + dot_nt(taken(coef_ref).astype(BF16), incoming_bd)
        o_hi, o_lo = two_parts(outcome)
        centre = dot_nn(jnp.concatenate([o_hi, o_lo], axis=0), mask_ref[...])
        away = outcome - (centre[0:span] + centre[span:]) * (1.0 / C)
        a_hi, a_lo = two_parts(away * away)
        spread = dot_nn(jnp.concatenate([a_hi, a_lo], axis=0), mask_ref[...])
        spread = (spread[0:span] + spread[span:]) * (1.0 / C)
        normed = away * lax.rsqrt(spread + group_eps)
        mixed = ((normed + taken(extra_ref)) * taken(gate_ref)).astype(BF16)
        for h in range(2):
            for n in range(HALF // 256):
                rings[b].part[d, h, :, pl.ds(256 * n, 256)] = dot_nn(
                    mixed, matrix_ref[:, pl.ds(h * HALF + 256 * n, 256)]
                ).astype(BF16)
        rings[b].produced(d)

    def normed_rows(b):
        rows = pl.ds(b * PIECE, PIECE)
        squares = jnp.zeros((PIECE, 1), F32)
        for h in range(2):
            cols = pl.ds(h * HALF, HALF)
            stream = skip_ref[rows, cols].astype(F32) + rings[b].result(h)
            stream_ref[rows, cols] = stream
            squares = squares + jnp.sum(stream * stream, axis=1, keepdims=True)
        scale_rows = lax.rsqrt(squares * (1.0 / (2 * HALF)) + norm_eps)
        for h in range(2):
            cols = pl.ds(h * HALF, HALF)
            rows_ref[b, chip, h, here, :] = (
                stream_ref[rows, cols] * scale_rows * gain_ref[:, cols]
            ).astype(BF16)
        for n in range(4):
            hop(b, n).start()
        side(b, 0).start()
        side(b, 1).start()

    def hop(b, n):
        d, h, to = (
            (0, 0, right),
            (0, 1, left),
            (0, 1, right),
            (0, 0, left),
            (3, 0, right),
            (1, 1, left),
        )[n]
        block = rows_ref.at[b, chip_at(d), h, here, :]
        return remote(block, block, row_send.at[b], row_recv.at[b, n], to)

    def arrival(b, n):
        d, h = ((3, 0), (1, 1), (3, 1), (1, 0), (2, 0), (2, 1))[n]
        block = rows_ref.at[b, chip_at(d), h, here, :]
        return remote(block, block, row_send.at[b], row_recv.at[b, n], sibling)

    sides = ((0, 0), (0, 1), (1, 0), (1, 1), (3, 0), (3, 1), (2, 0), (2, 1))

    def side(b, n):
        d, h = sides[n]
        block = rows_ref.at[b, chip_at(d), h, here, :]
        return remote(block, block, side_send.at[b], side_recv.at[b, n // 2], sibling)

    def relay_rows(b):
        arrival(b, 0).wait_recv()
        hop(b, 4).start()
        side(b, 4).start()
        arrival(b, 1).wait_recv()
        hop(b, 5).start()
        side(b, 3).start()

    def share_near(b):
        arrival(b, 2).wait_recv()
        side(b, 5).start()
        arrival(b, 3).wait_recv()
        side(b, 2).start()

    def share_far(b):
        arrival(b, 4).wait_recv()
        side(b, 6).start()
        arrival(b, 5).wait_recv()
        side(b, 7).start()

    def feed(*blocks):
        for b, d in blocks:
            all_moved(rows_ref.at[b, chip_at(d), :, there, :], side_recv.at[b, (0, 1, 3, 2)[d]])
        x = [
            jnp.concatenate([rows_ref[b, chip_at(d), h] for b, d in blocks], axis=0)
            for h in range(2)
        ]
        filled = pl.ds(0, len(blocks) * span)
        for n in range(hidden_ref.shape[1] // 128):
            cols = pl.ds(256 * n, 256)
            both = dot_nn(x[0], gate_up_ref[0:HALF, cols]) + dot_nn(x[1], gate_up_ref[HALF:, cols])
            gate_act, up_act = both[:, :128], both[:, 128:]
            hidden_ref[filled, pl.ds(128 * n, 128)] = (
                gate_act * jax.nn.sigmoid(gate_act) * up_act
            ).astype(BF16)
        if blocks == ((0, 0),):
            gather.down_here()
        hidden = hidden_ref[filled, :]
        for h in range(2):
            for n in range(HALF // 256):
                product = dot_nt(hidden, down_ref[pl.ds(h * HALF + 256 * n, 256), :]).astype(BF16)
                for m, (b, d) in enumerate(blocks):
                    rings[BATCHES + b].part[d, h, :, pl.ds(256 * n, 256)] = product[
                        m * span : (m + 1) * span
                    ]
        for b, d in blocks:
            rings[BATCHES + b].produced(d)

    def finish(b):
        ring = rings[BATCHES + b]
        rows = pl.ds(b * PIECE, PIECE)
        ring.to_sibling(0).wait_recv()
        ring.arrive()
        for h in range(2):
            cols = pl.ds(h * HALF, HALF)
            out_ref[rows, cols] = (stream_ref[rows, cols] + half_step * ring.result(h)).astype(BF16)

    gather.step(9)
    produce(0, 2)
    produce(0, 1)
    produce(0, 3)
    rings[0].pass_on(2)
    gather.step(10)
    rings[0].pass_on(1)
    produce(0, 0)
    rings[0].pass_on(3)
    produce(1, 2)
    gather.step(11)
    produce(1, 1)
    rings[1].pass_on(2)
    produce(1, 3)
    gather.step(14)
    rings[0].pass_relayed()
    rings[1].pass_on(1)
    produce(1, 0)
    rings[1].pass_on(3)
    rings[1].pass_relayed()
    rings[0].to_sibling(0).wait_recv()
    rings[0].arrive()
    normed_rows(0)
    gather.step(12)
    gather.step(13)
    rings[1].to_sibling(0).wait_recv()
    rings[1].arrive()
    normed_rows(1)
    gather.gate_up_here()
    feed((0, 0))
    relay_rows(0)
    share_near(0)
    feed((1, 0))
    relay_rows(1)
    feed((0, 3), (0, 1))
    share_far(0)
    share_near(1)
    rings[2].pass_on(3)
    rings[2].pass_on(1)
    feed((0, 2))
    share_far(1)
    rings[2].pass_on(2)
    feed((1, 2))
    rings[3].pass_on(2)
    rings[2].pass_relayed()
    feed((1, 3), (1, 1))
    rings[3].pass_on(3)
    rings[3].pass_on(1)
    rings[3].pass_relayed()
    finish(0)
    finish(1)
    for ring in rings:
        ring.drain()
    for b in range(BATCHES):
        all_moved(rows_ref.at[b, 0:3, :, 0:PIECE, :], row_send.at[b])
        all_moved(rows_ref.at[b, :, :, 0:PIECE, :], side_send.at[b])
    gather.drain()
    for d in range(1, n_y):
        to = lax.rem(place_y + d, n_y)
        copy_y(to, to).wait_send()
        copy_in(to, to).wait_send()
    for d in range(1, n_z):

        @pl.when(place_z + d < n_z)
        def _():
            copy_z(place_z + d, place_z).wait_send()


def layer(r, k, v, gate, fd, afl, foff, sd, soff, scale, skip, matrix, gain, switch, expand, contract):
    n_z, n_y = lax.axis_size("sp_0"), lax.axis_size("sp_1")
    length, width = r.shape
    ff = switch.shape[1]
    depth = switch.shape[0] * n_z * n_y
    vmem = pl.BlockSpec(memory_space=pltpu.VMEM)
    hbm = pl.BlockSpec(memory_space=pl.ANY)
    dma = pltpu.SemaphoreType.DMA
    return pl.pallas_call(
        functools.partial(layer_kernel, n_z, n_y),
        out_shape=jax.ShapeDtypeStruct((ROWS, 2 * HALF), BF16),
        in_specs=[hbm] * 16,
        out_specs=vmem,
        scratch_shapes=[pltpu.VMEM((ROWS, 2 * HALF), F32)]
        + [pltpu.VMEM((length, width), BF16)] * 6
        + [
            pltpu.VMEM((width, 2 * HALF), BF16),
            pltpu.VMEM((width // C, length), F32),
            pltpu.VMEM((1, width), F32),
            pltpu.VMEM((1, width), F32),
            pltpu.VMEM((1, width), F32),
            pltpu.VMEM((ROWS, 2 * HALF), BF16),
            pltpu.VMEM((1, 2 * HALF), F32),
            dma((13,)),
            pltpu.VMEM((width, width), BF16),
            pltpu.VMEM((len(LEVELS), width, width), BF16),
            pltpu.VMEM((length, width), F32),
            pltpu.VMEM((length, width), BF16),
            pltpu.VMEM((length, width), F32),
            pltpu.VMEM((2 * C, width), F32),
            pltpu.VMEM((n_y, C, 2 * C), BF16),
            pltpu.VMEM((n_y, C, 2 * C), BF16),
            pltpu.VMEM((C, 2 * C), BF16),
            pltpu.VMEM((n_z, C, 2 * C), BF16),
            pltpu.VMEM((n_y, C, 2 * C), BF16),
            pltpu.VMEM((n_y, C, 2 * C), BF16),
            dma((n_y,)),
            dma((n_y,)),
            dma((n_y,)),
            dma((n_y,)),
            dma((n_z,)),
            dma((n_z,)),
            pltpu.VMEM((depth, 2 * ff), BF16),
            pltpu.VMEM((depth, ff), BF16),
            pltpu.VMEM((BATCHES, 4, 2, 2 * PIECE, HALF), BF16),
            pltpu.VMEM((4 * PIECE, ff), BF16),
            dma((2,)),
            dma((2,)),
            dma((WEIGHT_ARRIVALS,)),
            dma((BATCHES,)),
            dma((BATCHES, 6)),
            dma((BATCHES,)),
            dma((BATCHES, 4)),
        ]
        + RING_SUM_SCRATCH * (2 * BATCHES),
        compiler_params=pltpu.CompilerParams(
            collective_id=0, has_side_effects=True, vmem_limit_bytes=60 * 1024 * 1024
        ),
        cost_estimate=pl.CostEstimate(
            flops=40_000_000_000, bytes_accessed=8_000_000, transcendentals=0
        ),
        name="layer",
    )(
        r, k, v, gate, fd, afl.T, foff[None, :], sd, soff[None, :], scale[None, :], skip, matrix,
        gain[None, :], switch, expand, contract,
    )


def per_device(
    skip_stream,
    acceptance_signal,
    lookup_mapped,
    payload_mapped,
    result_switch,
    forget_dynamic_share,
    additive_forget_logarithm,
    forget_feature_offset,
    substitution_dynamic_share,
    substitution_feature_offset,
    diagonal_reward_scales,
    result_matrix,
    mlp_rescaler,
    switch_matrix,
    expand_matrix,
    contract_matrix,
):
    return layer(
        acceptance_signal,
        lookup_mapped,
        payload_mapped,
        result_switch,
        forget_dynamic_share,
        additive_forget_logarithm,
        forget_feature_offset,
        substitution_dynamic_share,
        substitution_feature_offset,
        diagonal_reward_scales,
        skip_stream,
        result_matrix,
        mlp_rescaler,
        switch_matrix,
        expand_matrix,
        contract_matrix,
    )


def solution(mesh):
    torus = Mesh(mesh.devices.reshape(8, 4, mesh.shape["tp"]), ("sp_0", "sp_1", "tp"))
    in_specs = (
        P(SP_TP, None),
        P(SP, "tp"),
        P(SP, "tp"),
        P(SP, "tp"),
        P(SP, "tp"),
        P(SP, "tp"),
        P(SP, "tp"),
        P("tp"),
        P(SP, "tp"),
        P("tp"),
        P("tp"),
        P("tp", None),
        P(),
        P(SP, "tp"),
        P(SP, "tp"),
        P(SP, "tp"),
    )
    out_specs = P(SP_TP, None)
    return jax.shard_map(
        per_device, mesh=torus, in_specs=in_specs, out_specs=out_specs, check_vma=False
    )
```
